256 devices in a mesh: fs: 32 (over z, x), tp: 8 (over y, core).
Axes of the slice: x: 4, y: 4, z: 8, core: 2. Of those that a mesh axis runs over, the one named last changes fastest.
Arguments:
- later_rows: bfloat16 [32768, 2048], P(('fs', 'tp')), may hold values from -6 to 6
- earlier_rows: bfloat16 [32768, 2048], P(('fs', 'tp')), may hold values from -6 to 6
- cotangent: bfloat16 [32768, 2048], P(('fs', 'tp')), may hold values from -24 to 24
- up_weight: bfloat16 [2048, 4096], P('fs', 'tp'), may hold values from -0.125 to 0.125
- down_weight: bfloat16 [2048, 4096], P('fs', 'tp'), may hold values from -0.09375 to 0.09375
- up_total: float32 [2048, 4096], P('fs', 'tp'), may hold values from -6 to 6
- down_total: float32 [2048, 4096], P('fs', 'tp'), may hold values from -6 to 6
Outputs:
- later_out: bfloat16 [32768, 2048], P(('fs', 'tp'))
- earlier_grad: bfloat16 [32768, 2048], P(('fs', 'tp'))
- up_updated: float32 [2048, 4096], P('fs', 'tp')
- down_updated: float32 [2048, 4096], P('fs', 'tp')
The draws below stay inside these ranges and needn't reach their ends.
All inputs are finite; a program needn't handle non-finite values.
Results may differ from the reference program's by a relative error of at most 0.015.
Values may be sent and summed in bfloat16 or wider, within the bound.
A program may use at most 128 MiB of HBM per device.

```python
import math
import jax
import jax.numpy as jnp
from jax import lax

D = 2048
FF = 4096
TOKENS = 32768
FF_TP = 512
N_TP = 8


def spiked(drawn, rng, source, target, shards_of, factor):
    def block_of(position):
        return (jnp.arange(drawn.shape[position]) // (drawn.shape[position] // shards_of)).reshape((-1,) + (1,) * (drawn.ndim - 1 - position))

    one_side = jax.random.permutation(rng, shards_of)[block_of(target)]
    far = (block_of(target) + shards_of // 2) % shards_of
    return jnp.where((block_of(source) == one_side) | (block_of(source) == far), factor * drawn, drawn)


def steps_of(rng, dims, split, low, largest):
    def one(axis_at, parts):
        steps = jax.random.uniform(jax.random.fold_in(jax.random.fold_in(rng, 6), axis_at), (parts,), jnp.float32, low / len(split), largest / len(split))
        return jnp.repeat(jnp.exp(steps), dims[axis_at] // parts).reshape((-1,) + (1,) * (len(dims) - axis_at - 1))

    level = one(*split[0])
    for cut in split[1:]:
        level = level * one(*cut)
    return level


def scatter_about(key, extent, width, reach, shards=(), kind=jnp.bfloat16):
    loudness = steps_of(key, extent, shards, -0.22, 0.18) if shards else 1.0
    array = jax.random.normal(key, extent, jnp.float32) * width * loudness
    return jnp.minimum(jnp.maximum(array, -reach), reach).astype(kind)


def noise_with(stream_key, dims, width, reach, shards, heavy, kind=jnp.bfloat16):
    entries = width * jax.random.normal(stream_key, dims, jnp.float32)
    if shards:
        entries = entries * steps_of(stream_key, dims, shards, -0.22, 0.18)
    return jnp.clip(spiked(entries, jax.random.fold_in(stream_key, 3), *heavy), -reach, reach).astype(kind)


def setup_inputs(seed: int = 0) -> dict:
    keys = jax.random.split(jax.random.key(seed), 8)
    return {
        "later_rows": scatter_about(keys[0], (TOKENS, D), 1.0, 6.0, ((0, 256),)),
        "earlier_rows": scatter_about(keys[1], (TOKENS, D), 1.0, 6.0, ((0, 256),)),
        "cotangent": noise_with(keys[2], (TOKENS, D), 1.0, 24.0, ((0, 256),), (0, 1, 256, 6.0)),
        "up_weight": scatter_about(keys[3], (D, FF), D ** -0.5, 0.125, ((0, 32), (1, 8))),
        "down_weight": scatter_about(keys[4], (D, FF), FF ** -0.5, 0.09375, ((0, 32), (1, 8))),
        "up_total": scatter_about(keys[5], (D, FF), 1.0, 6.0, ((0, 32), (1, 8)), jnp.float32),
        "down_total": scatter_about(keys[6], (D, FF), 1.0, 6.0, ((0, 32), (1, 8)), jnp.float32),
    }


def blocked_sum(left, right):

    def one_block(carry, index):
        start = (index * FF_TP).astype(jnp.int32)
        left_block = lax.dynamic_slice_in_dim(left, start, FF_TP, 1)
        right_block = lax.dynamic_slice_in_dim(right, start, FF_TP, 1)
        partial_value = lax.dot_general(left_block, right_block, (((1,), (1,)), ((), ())), preferred_element_type=jnp.float32)
        rounded = lax.optimization_barrier(partial_value.astype(jnp.bfloat16))
        return (carry + rounded.astype(jnp.float32), None)
    init = jnp.zeros((left.shape[0], right.shape[0]), jnp.float32)
    total, _ = lax.scan(one_block, init, jnp.arange(N_TP, dtype=jnp.int32))
    return total

def reference(later_rows, earlier_rows, cotangent, up_weight, down_weight, up_total, down_total):
    later_pre = jnp.dot(later_rows, up_weight, preferred_element_type=jnp.float32)
    later_relu = jnp.maximum(later_pre, 0.0)
    later_hidden = (later_relu * later_relu).astype(jnp.bfloat16)
    later_out = blocked_sum(later_hidden, down_weight).astype(jnp.bfloat16)
    earlier_pre = jnp.dot(earlier_rows, up_weight, preferred_element_type=jnp.float32)
    earlier_relu = jnp.maximum(earlier_pre, 0.0)
    earlier_hidden = (earlier_relu * earlier_relu).astype(jnp.bfloat16)
    hidden_grad = jnp.dot(cotangent, down_weight, preferred_element_type=jnp.float32)
    pre_grad = (2.0 * earlier_relu * hidden_grad).astype(jnp.bfloat16)
    earlier_grad = blocked_sum(pre_grad, up_weight).astype(jnp.bfloat16)
    factor = 1.0 / math.sqrt(TOKENS)
    up_term = jnp.dot(earlier_rows.T, pre_grad, preferred_element_type=jnp.float32)
    down_term = jnp.dot(cotangent.T, earlier_hidden, preferred_element_type=jnp.float32)
    up_updated = up_total + up_term * factor
    down_updated = down_total + down_term * factor
    return (later_out, earlier_grad, up_updated, down_updated)
```

```python
import math
from types import SimpleNamespace

import jax
import jax.numpy as jnp
from jax import lax
from jax.experimental import pallas as pl
from jax.experimental.pallas import tpu as pltpu
from jax.sharding import PartitionSpec as P

NZ, NX, NY = 8, 4, 4
BF = jnp.bfloat16
F32 = jnp.float32
N_COPIES = 160


def scratch_of(tok, d, ff, rows):
    per_z = NX * rows
    vm = pltpu.VMEM
    return dict(
        ye=vm((4 * tok, d), BF),
        yc=vm((4 * tok, d), BF),
        yl=vm((4 * tok, d), BF),
        wu=vm((2, NZ, per_z, ff), BF),
        wd=vm((2, NZ, per_z, ff), BF),
        hid=vm((4 * tok, 2 * ff), BF),
        pg=vm((4 * tok, 2 * ff), BF),
        pe=vm((4 * tok, d), BF),
        po=vm((4 * tok, d), BF),
        se=vm((2, tok // 2, d), BF),
        so=vm((2, tok // 2, d), BF),
        re=vm((2, tok, d), BF),
        ro=vm((2, tok, d), BF),
        gou=vm((NZ, per_z, ff), BF),
        god=vm((NZ, per_z, ff), BF),
        xu=vm((NZ, per_z, ff), BF),
        xd=vm((NZ, per_z, ff), BF),
        su=vm((NZ, per_z, ff), BF),
        sd=vm((NZ, per_z, ff), BF),
        sx=vm((2, NZ // 2, rows, ff), BF),
        rx=vm((2, NZ, rows, ff), BF),
        tu=vm((NZ, rows, ff), BF),
        rz=vm((NZ - 1, rows, ff), BF),
        ra=vm((4, per_z, ff), BF),
        rb=vm((4, per_z, ff), BF),
        td=vm((NX, rows, ff), BF),
        rxd=vm((NX - 1, rows, ff), BF),
        tot_u=vm((rows, ff), F32),
        tot_d=vm((rows, ff), F32),
        send=pltpu.SemaphoreType.DMA((N_COPIES,)),
        recv=pltpu.SemaphoreType.DMA((N_COPIES,)),
        local=pltpu.SemaphoreType.DMA((16,)),
    )


def dot_tt(a, b):
    return lax.dot_general(a, b, (((1,), (1,)), ((), ())), preferred_element_type=F32)


def dot_ta(a, b):
    return lax.dot_general(a, b, (((0,), (0,)), ((), ())), preferred_element_type=F32)


def kernel(names, factor, *refs):
    later, earlier, cot, up, down, up_total, down_total = refs[:7]
    o_later, o_earlier, o_up, o_down = refs[7:11]
    r = SimpleNamespace(**dict(zip(names, refs[11:])))
    tok, d = later.shape
    rows, ff = up.shape
    half = tok // 2
    per_z = NX * rows
    hz = per_z // 2

    f, t = lax.axis_index("fs"), lax.axis_index("tp")
    z, x = f // NX, f % NX
    y, c = t // 2, t % 2

    def zi(k):
        return (z + k + NZ) % NZ

    def xi(k):
        return (x + k + NX) % NX

    def dev(dz=0, dx=0, dy=0, dc=0):
        fs = zi(dz) * NX + xi(dx)
        tp = ((y + dy + NY) % NY) * 2 + (c + dc) % 2
        return {"fs": fs, "tp": tp}

    sent = []

    def send(src, dst, to):
        i = len(sent)
        copy = pltpu.make_async_remote_copy(
            src_ref=src,
            dst_ref=dst,
            send_sem=r.send.at[i],
            recv_sem=r.recv.at[i],
            device_id=to,
            device_id_type=pl.DeviceIdType.MESH,
        )
        copy.start()
        sent.append(copy)
        return copy

    def got(*copies):
        for copy in copies:
            copy.wait_recv()

    local = []

    def fetch(src, dst):
        copy = pltpu.make_async_copy(src, dst, r.local.at[len(local)])
        copy.start()
        local.append(copy)
        return copy

    def xs(k):
        return pl.ds(pl.multiple_of(xi(k) * rows, rows), rows)

    first = [
        fetch(earlier, r.ye.at[pl.ds(0, tok)]),
        fetch(cot, r.yc.at[pl.ds(0, tok)]),
        fetch(up, r.wu.at[0, z, xs(0)]),
        fetch(down, r.wd.at[0, z, xs(0)]),
        fetch(later, r.yl.at[pl.ds(0, tok)]),
    ]
    totals = [fetch(up_total, r.tot_u), fetch(down_total, r.tot_d)]

    barrier = pltpu.get_barrier_semaphore()
    partners = [dev(dy=1), dev(dy=-1), dev(dc=1), dev(dx=1), dev(dx=2), dev(dx=3)]
    partners += [dev(dz=k) for k in range(1, NZ)]
    for p in partners:
        pl.semaphore_signal(barrier, inc=1, device_id=p, device_id_type=pl.DeviceIdType.MESH)
    pl.semaphore_wait(barrier, len(partners))
    for copy in first:
        copy.wait()

    def rows_of(slot, h):
        return pl.ds(slot * tok + h * half, half)

    def own_tokens(buf, h):
        plus = send(buf.at[rows_of(0, h)], buf.at[rows_of(1, h)], dev(dy=1))
        minus = send(buf.at[rows_of(0, 1 - h)], buf.at[rows_of(2, 1 - h)], dev(dy=-1))
        return plus, minus

    def pass_tokens(buf, pair):
        got(*pair)
        plus = send(buf.at[rows_of(1, 0)], buf.at[rows_of(3, 0)], dev(dy=1))
        minus = send(buf.at[rows_of(2, 1)], buf.at[rows_of(3, 1)], dev(dy=-1))
        return plus, minus

    wu, wd = r.wu, r.wd

    def up_block(dz, dx):
        return wu.at[0, zi(dz), xs(dx)]

    def up_z(dz, step, h=None):
        ref = up_block(dz, 0)
        if h is not None:
            ref = ref.at[pl.ds(h * (rows // 2), rows // 2)]
        return send(ref, ref, dev(dz=step))

    up_x = {}

    def up_to_x(dz):
        ref = up_block(dz, 0)
        up_x[dz] = (send(ref, ref, dev(dx=1)), send(ref, ref, dev(dx=-1)))

    def up_pass_x(dz):
        plus, minus = up_x[dz]
        if 0 <= dz <= 3:
            got(plus)
            ref = up_block(dz, -1)
            return send(ref, ref, dev(dx=1)), minus
        got(minus)
        ref = up_block(dz, 1)
        return send(ref, ref, dev(dx=-1)), plus

    def up_column(dx):
        src = wu.at[0, :, xs(dx)]
        return send(src, wu.at[1, :, xs(dx)], dev(dc=1))

    def down_half(dz, h):
        return wd.at[0, zi(dz), pl.ds(h * hz, hz)]

    def down_z(dz, step, h):
        ref = down_half(dz, h)
        return send(ref, ref, dev(dz=step))

    def down_chunk(dz):
        return send(wd.at[0, zi(dz)], wd.at[1, zi(dz)], dev(dc=1))

    e_a = own_tokens(r.ye, 0)
    c_a = own_tokens(r.yc, 0)
    e_b = own_tokens(r.ye, 1)
    c_b = own_tokens(r.yc, 1)
    own_down = wd.at[0, z, xs(0)]
    down_x = [send(own_down, own_down, dev(dx=k)) for k in (1, -1, 2)]
    zp, zm = [up_z(0, 1)], [up_z(0, -1)]
    up_to_x(0)

    across = []
    got(zp[0], zm[0])
    zp.append(up_z(-1, 1))
    zm.append(up_z(1, -1))
    got(*down_x)
    dp = [(down_z(0, 1, 0), down_z(0, 1, 1))]
    dm = [(down_z(0, -1, 1), down_z(0, -1, 0))]
    across.append(down_chunk(0))
    up_to_x(-1)
    up_to_x(1)
    got(zp[1], zm[1])
    zp.append(up_z(-2, 1))
    zm.append(up_z(2, -1))
    up_to_x(-2)
    up_to_x(2)
    last_up = [up_pass_x(0)]

    def down_pass(k):
        dp_new, dm_new = [], []
        for i in range(2):
            got(dp[k - 1][i])
            if k < 3 or i == 0:
                dp_new.append(down_z(-k, 1, i))
            got(dm[k - 1][i])
            if k < 3 or i == 0:
                dm_new.append(down_z(k, -1, 1 - i))
        dp.append(dp_new)
        dm.append(dm_new)
        across.append(down_chunk(-k))
        across.append(down_chunk(k))

    got(zp[2], zm[2])
    zp.append(up_z(-3, 1, 0))
    zm.append(up_z(3, -1, 1))
    up_to_x(-3)
    up_to_x(3)
    down_pass(1)
    last_up += [up_pass_x(-1), up_pass_x(1)]
    e_f = pass_tokens(r.ye, e_a)
    c_f = pass_tokens(r.yc, c_a)
    l_a = own_tokens(r.yl, 0)
    l_b = own_tokens(r.yl, 1)
    got(zp[3], zm[3])
    up_to_x(4)
    across.append(up_column(0))
    last_up += [up_pass_x(-2), up_pass_x(2)]
    down_pass(2)
    last_up += [up_pass_x(-3), up_pass_x(3)]
    last_up += [up_pass_x(4)]
    for passed, other in last_up:
        got(other)
    across.append(up_column(-1))
    across.append(up_column(1))
    down_pass(3)
    for passed, other in last_up:
        got(passed)
    across.append(up_column(2))
    got(dp[3][0], dm[3][0])
    across.append(down_chunk(4))
    got(*across)
    got(*e_b, *c_b, *e_f, *c_f)

    tile = 256
    for core in range(2):

        @pl.loop(0, ff // tile)
        def _(n):
            at = pl.multiple_of(n * tile, tile)
            w_up = wu[core, :, :, pl.ds(at, tile)].reshape(d, tile)
            w_down = wd[core, :, :, pl.ds(at, tile)].reshape(d, tile)
            relu = jnp.maximum(jnp.dot(r.ye[...], w_up, preferred_element_type=F32), 0.0)
            grad = jnp.dot(r.yc[...], w_down, preferred_element_type=F32)
            out = pl.ds(pl.multiple_of(core * ff + at, tile), tile)
            r.hid[:, out] = (relu * relu).astype(BF)
            r.pg[:, out] = (2.0 * relu * grad).astype(BF)

    def cross_grad(left, right, out, into):
        copies = []
        for part in range(2):

            @pl.loop(part * NZ // 2, (part + 1) * NZ // 2)
            def _(k):
                cols = pl.ds(pl.multiple_of(k * per_z, per_z), per_z)
                out[k] = dot_ta(left[:, cols], right[:, ff:]).astype(BF)

            piece = pl.ds(part * NZ // 2, NZ // 2)
            copies.append(send(out.at[piece], into.at[piece], dev(dc=1)))
        return copies

    def own_grad(left, right, other, out):
        @pl.loop(0, NZ)
        def _(k):
            cols = pl.ds(pl.multiple_of(k * per_z, per_z), per_z)
            mine = dot_ta(left[:, cols], right[:, :ff])
            out[k] = (mine + other[k].astype(F32)).astype(BF)

    c_up = cross_grad(r.ye, r.pg, r.gou, r.xu)
    c_down = cross_grad(r.yc, r.hid, r.god, r.xd)
    l_f = pass_tokens(r.yl, l_a)
    got(*c_up)
    own_grad(r.ye, r.pg, r.xu, r.su)

    su, sd = r.su, r.sd
    nh = NZ // 2
    lo, hi = pl.ds(0, nh), pl.ds(nh, nh)
    ux_a = send(su.at[lo, xs(2)], r.sx.at[0], dev(dx=1))
    ux_b = send(su.at[hi, xs(2)], r.sx.at[1], dev(dx=-1))
    ur_a = [send(su.at[hi, xs(1)], r.rx.at[0, hi], dev(dx=1))]
    ur_b = [send(su.at[lo, xs(-1)], r.rx.at[1, lo], dev(dx=-1))]

    got(*c_down)
    own_grad(r.yc, r.hid, r.xd, r.sd)

    h0, h1 = pl.ds(0, hz), pl.ds(hz, hz)
    da = {(0, 0): send(sd.at[zi(4), h0], r.ra.at[0, h0], dev(dz=1))}
    db = {(0, 1): send(sd.at[zi(-4), h1], r.rb.at[0, h1], dev(dz=-1))}
    da[1, 1] = send(sd.at[zi(3), h1], r.ra.at[1, h1], dev(dz=1))
    db[1, 0] = send(sd.at[zi(-3), h0], r.rb.at[1, h0], dev(dz=-1))

    def hop(s, h, plus):
        part = pl.ds(h * hz, hz)
        arrived, buf, to = (da, r.ra, 1) if plus else (db, r.rb, -1)
        k = zi(4 - s) if plus else zi(s - 4)
        got(arrived[s - 1, h])
        total = sd[k, part].astype(F32) + buf[s - 1, part].astype(F32)
        sd[k, part] = total.astype(BF)
        arrived[s, h] = send(sd.at[k, part], buf.at[s, part], dev(dz=to))

    def back(left, weight, out):
        @pl.loop(0, NZ)
        def _(k):
            acc = dot_tt(left[:, :ff], weight[0, k]) + dot_tt(left[:, ff:], weight[1, k])
            out[:, pl.ds(pl.multiple_of(k * per_z, per_z), per_z)] = acc.astype(BF)

    def start_sum(p, s, m):
        a = send(p.at[rows_of(3, 0)], s.at[0], dev(dy=1))
        b = send(p.at[rows_of(3, 1)], s.at[1], dev(dy=-1))
        ra = send(p.at[rows_of(2, 1)], m.at[0, pl.ds(half, half)], dev(dy=1))
        rb = send(p.at[rows_of(1, 0)], m.at[1, pl.ds(0, half)], dev(dy=-1))
        return a, b, ra, rb

    def pass_sum(p, s, m, pieces):
        a, b, ra, rb = pieces
        got(a)
        at = rows_of(2, 0)
        p[at] = (p[at].astype(F32) + s[0].astype(F32)).astype(BF)
        ra2 = send(p.at[at], m.at[0, pl.ds(0, half)], dev(dy=1))
        got(b)
        at = rows_of(1, 1)
        p[at] = (p[at].astype(F32) + s[1].astype(F32)).astype(BF)
        rb2 = send(p.at[at], m.at[1, pl.ds(half, half)], dev(dy=-1))
        return ra, rb, ra2, rb2

    def end_sum(p, m, pieces, out):
        got(*pieces)
        own = pl.ds(0, tok)
        total = p[own].astype(F32) + m[0].astype(F32) + m[1].astype(F32)
        p[own] = total.astype(BF)
        return fetch(p.at[own], out)

    back(r.pg, wu, r.pe)
    y_e = start_sum(r.pe, r.se, r.re)

    got(ux_a)
    su[lo, xs(1)] = (su[lo, xs(1)].astype(F32) + r.sx[0].astype(F32)).astype(BF)
    ur_a.append(send(su.at[lo, xs(1)], r.rx.at[0, lo], dev(dx=1)))
    got(ux_b)
    su[hi, xs(-1)] = (su[hi, xs(-1)].astype(F32) + r.sx[1].astype(F32)).astype(BF)
    ur_b.append(send(su.at[hi, xs(-1)], r.rx.at[1, hi], dev(dx=-1)))
    hop(1, 0, True)
    hop(1, 1, False)

    got(*l_b, *l_f)
    for core in range(2):

        @pl.loop(0, ff // tile)
        def _(n):
            at = pl.multiple_of(n * tile, tile)
            w_up = wu[core, :, :, pl.ds(at, tile)].reshape(d, tile)
            relu = jnp.maximum(jnp.dot(r.yl[...], w_up, preferred_element_type=F32), 0.0)
            out = pl.ds(pl.multiple_of(core * ff + at, tile), tile)
            r.hid[:, out] = (relu * relu).astype(BF)

    hop(2, 1, True)
    hop(2, 0, False)
    y_e = pass_sum(r.pe, r.se, r.re, y_e)
    back(r.hid, wd, r.po)
    y_o = start_sum(r.po, r.so, r.ro)

    hop(2, 0, True)
    hop(2, 1, False)
    hop(3, 1, True)
    hop(3, 0, False)
    got(*ur_a, *ur_b)
    tu = r.tu
    tu[...] = (
        su[:, xs(0)].astype(F32) + r.rx[0].astype(F32) + r.rx[1].astype(F32)
    ).astype(BF)
    uz = [send(tu.at[zi(k)], r.rz.at[k - 1], dev(dz=k)) for k in (1, 7, 2, 6, 3, 5, 4)]
    hop(3, 0, True)
    hop(3, 1, False)

    out_e = end_sum(r.pe, r.re, y_e, o_earlier)
    y_o = pass_sum(r.po, r.so, r.ro, y_o)

    got(da[3, 0], da[3, 1], db[3, 0], db[3, 1])
    down_sum = sd[z].astype(F32) + r.ra[3].astype(F32) + r.rb[3].astype(F32)
    r.td[...] = down_sum.astype(BF).reshape(NX, rows, ff)
    dx = [send(r.td.at[xi(k)], r.rxd.at[k - 1], dev(dx=k)) for k in (1, 3, 2)]

    for copy in totals:
        copy.wait()
    got(*uz)
    total = tu[z].astype(F32)
    for k in range(NZ - 1):
        total = total + r.rz[k].astype(F32)
    r.tot_u[...] = r.tot_u[...] + total * factor
    out_u = fetch(r.tot_u, o_up)
    got(*dx)
    total = r.td[x].astype(F32)
    for k in range(NX - 1):
        total = total + r.rxd[k].astype(F32)
    r.tot_d[...] = r.tot_d[...] + total * factor
    out_d = fetch(r.tot_d, o_down)

    out_l = end_sum(r.po, r.ro, y_o, o_later)
    for copy in sent:
        copy.wait_send()
    for copy in (out_e, out_u, out_d, out_l):
        copy.wait()


def body(later_rows, earlier_rows, cotangent, up_weight, down_weight, up_total, down_total):
    tok, d = later_rows.shape
    rows, ff = up_weight.shape
    total_rows = tok * lax.axis_size("fs") * lax.axis_size("tp")
    factor = 1.0 / math.sqrt(total_rows)
    scratch = scratch_of(tok, d, ff, rows)

    def run(*refs):
        kernel(list(scratch), factor, *refs)

    return pl.pallas_call(
        run,
        out_shape=(
            jax.ShapeDtypeStruct((tok, d), BF),
            jax.ShapeDtypeStruct((tok, d), BF),
            jax.ShapeDtypeStruct((rows, ff), F32),
            jax.ShapeDtypeStruct((rows, ff), F32),
        ),
        in_specs=[pl.BlockSpec(memory_space=pl.ANY)] * 7,
        out_specs=(pl.BlockSpec(memory_space=pl.ANY),) * 4,
        scratch_shapes=list(scratch.values()),
        compiler_params=pltpu.CompilerParams(
            collective_id=0, has_side_effects=True, vmem_limit_bytes=67_000_000
        ),
        name="ffn_step",
    )(later_rows, earlier_rows, cotangent, up_weight, down_weight, up_total, down_total)


def solution(mesh):
    tokens = P(("fs", "tp"), None)
    weight = P("fs", "tp")
    return jax.shard_map(
        body,
        mesh=mesh,
        in_specs=(tokens, tokens, tokens, weight, weight, weight, weight),
        out_specs=(tokens, tokens, weight, weight),
        check_vma=False,
    )
```

```python
import math
from types import SimpleNamespace

import jax
import jax.numpy as jnp
from jax import lax
from jax.experimental import pallas as pl
from jax.experimental.pallas import tpu as pltpu
from jax.sharding import PartitionSpec as P

NZ, NX, NY = 8, 4, 4
BF = jnp.bfloat16
F32 = jnp.float32
N_SENT = 13
N_GOT = 68


def scratch_of(tok, d, ff, rows):
    per_z = NX * rows
    vm = pltpu.VMEM
    return dict(
        ye=vm((4 * tok, d), BF),
        yc=vm((4 * tok, d), BF),
        yl=vm((4 * tok, d), BF),
        wu=vm((2, NZ, per_z, ff), BF),
        wd=vm((2, NZ, per_z, ff), BF),
        hid=vm((4 * tok, 2 * ff), BF),
        rel=vm((tok, 2 * ff), F32),
        pg=vm((4 * tok, 2 * ff), BF),
        pe=vm((4 * tok, d), BF),
        po=vm((4 * tok, d), BF),
        se=vm((2, tok // 2, d), BF),
        so=vm((2, tok // 2, d), BF),
        re=vm((2, tok, d), BF),
        ro=vm((2, tok, d), BF),
        gou=vm((NZ, per_z, ff), BF),
        god=vm((NZ, per_z, ff), BF),
        xu=vm((NZ, per_z, ff), BF),
        xd=vm((NZ, per_z, ff), BF),
        su=vm((NZ, per_z, ff), BF),
        sd=vm((NZ, per_z, ff), BF),
        sx=vm((2, NZ // 2, rows, ff), BF),
        rx=vm((2, NZ, rows, ff), BF),
        tu=vm((NZ, rows, ff), BF),
        ua=vm((4, rows, ff), BF),
        ub=vm((4, rows, ff), BF),
        ra=vm((4, per_z, ff), BF),
        rb=vm((4, per_z, ff), BF),
        td=vm((NX, rows, ff), BF),
        xa=vm((2, rows, ff), BF),
        xb=vm((2, rows, ff), BF),
        et=vm((d, 4 * tok), BF),
        ct=vm((d, 4 * tok), BF),
        tot_u=vm((rows, ff), F32),
        tot_d=vm((rows, ff), F32),
        send=pltpu.SemaphoreType.DMA((N_SENT,)),
        recv=pltpu.SemaphoreType.DMA((N_GOT,)),
        local=pltpu.SemaphoreType.DMA((7,)),
    )


def dot_tt(a, b):
    return lax.dot_general(a, b, (((1,), (1,)), ((), ())), preferred_element_type=F32)


def kernel(names, factor, *refs):
    later, earlier, cot, up, down, up_total, down_total = refs[:7]
    o_later, o_earlier, o_up, o_down = refs[7:11]
    r = SimpleNamespace(**dict(zip(names, refs[11:])))
    tok, d = later.shape
    rows, ff = up.shape
    half = tok // 2
    per_z = NX * rows
    hz = per_z // 2

    f, t = lax.axis_index("fs"), lax.axis_index("tp")
    z, x = f // NX, f % NX
    y, c = t // 2, t % 2

    def zi(k):
        return (z + k + NZ) % NZ

    def xi(k):
        return (x + k + NX) % NX

    def dev(dz=0, dx=0, dy=0, dc=0):
        fs = zi(dz) * NX + xi(dx)
        tp = ((y + dy + NY) % NY) * 2 + (c + dc) % 2
        return {"fs": fs, "tp": tp}

    row_bytes = d * 2
    limit = r.ye.shape[0] * row_bytes
    leaving, arriving = [], []

    def group():
        g = SimpleNamespace(at=len(arriving), bytes=0)
        arriving.append(g)
        return g

    def wait(sem, g):
        ref = r.ye.at[pl.ds(0, g.bytes // row_bytes)]
        pltpu.make_async_copy(ref, ref, sem).wait()

    def send(src, dst, to, g=None):
        size = math.prod(src.shape) * 2
        g = group() if g is None else g
        g.bytes += size
        if not leaving or leaving[-1].done or leaving[-1].bytes + size > limit:
            leaving.append(SimpleNamespace(bytes=0, done=False))
        leaving[-1].bytes += size
        pltpu.make_async_remote_copy(
            src_ref=src,
            dst_ref=dst,
            send_sem=r.send.at[len(leaving) - 1],
            recv_sem=r.recv.at[g.at],
            device_id=to,
            device_id_type=pl.DeviceIdType.MESH,
        ).start()
        return g

    @jax.named_scope("sent")
    def settle():
        for i, g in enumerate(leaving):
            if not g.done:
                wait(r.send.at[i], g)
                g.done = True

    def got(name, *groups):
        with jax.named_scope(name):
            for g in {g.at: g for g in groups}.values():
                wait(r.recv.at[g.at], g)

    local = []

    def fetch(src, dst):
        copy = pltpu.make_async_copy(src, dst, r.local.at[len(local)])
        copy.start()
        local.append(copy)
        return copy

    def xs(k):
        return pl.ds(pl.multiple_of(xi(k) * rows, rows), rows)

    first = [
        fetch(earlier, r.ye.at[pl.ds(0, tok)]),
        fetch(cot, r.yc.at[pl.ds(0, tok)]),
        fetch(up, r.wu.at[0, z, xs(0)]),
        fetch(down, r.wd.at[0, z, xs(0)]),
        fetch(later, r.yl.at[pl.ds(0, tok)]),
    ]
    totals = [fetch(up_total, r.tot_u), fetch(down_total, r.tot_d)]

    barrier = pltpu.get_barrier_semaphore()
    partners = [dev(dy=1), dev(dy=-1), dev(dx=1), dev(dx=-1), dev(dz=1), dev(dz=-1), dev(dc=1)]
    for p in partners:
        pl.semaphore_signal(barrier, inc=1, device_id=p, device_id_type=pl.DeviceIdType.MESH)
    with jax.named_scope("barrier"):
        pl.semaphore_wait(barrier, len(partners))
        for copy in first:
            copy.wait()

    def rows_of(slot, h):
        return pl.ds(slot * tok + h * half, half)

    def own_tokens(buf, h, g=None):
        g = g or group()
        send(buf.at[rows_of(0, h)], buf.at[rows_of(1, h)], dev(dy=1), g)
        send(buf.at[rows_of(0, 1 - h)], buf.at[rows_of(2, 1 - h)], dev(dy=-1), g)
        return g

    def pass_tokens(buf, first, g=None):
        g = g or group()
        got("tok_first", first)
        send(buf.at[rows_of(1, 0)], buf.at[rows_of(3, 0)], dev(dy=1), g)
        send(buf.at[rows_of(2, 1)], buf.at[rows_of(3, 1)], dev(dy=-1), g)
        return g

    wu, wd = r.wu, r.wd

    def up_block(dz, dx):
        return wu.at[0, zi(dz), xs(dx)]

    def up_z(k):
        g = group()
        for step in (1, -1):
            ref = up_block(-k * step, 0)
            if k == 3:
                ref = ref.at[pl.ds(0 if step == 1 else rows // 2, rows // 2)]
            send(ref, ref, dev(dz=step), g)
        return g

    up_first, up_rest, up_last = {}, group(), group()

    def up_to_x(dz):
        ref = up_block(dz, 0)
        up_first[dz] = group()
        plus, minus = (up_first[dz], up_rest) if 0 <= dz <= 3 else (up_rest, up_first[dz])
        send(ref, ref, dev(dx=1), plus)
        send(ref, ref, dev(dx=-1), minus)

    def up_pass_x(*dzs):
        for dz in dzs:
            got("up_x", up_first[dz])
            step = 1 if 0 <= dz <= 3 else -1
            ref = up_block(dz, -step)
            send(ref, ref, dev(dx=step), up_last)

    across_up, across_down = group(), group()

    def up_column(dx):
        src = wu.at[0, :, xs(dx)]
        send(src, wu.at[1, :, xs(dx)], dev(dc=1), across_up)

    def down_block(dz, dx):
        return wd.at[0, zi(dz), xs(dx)]

    down_far = group()
    down_at = {}

    def down_z(k, *dxs):
        for dx in dxs:
            g = down_far if k == 3 else group()
            down_at[k + 1, dx] = g
            if k < 3 or dx in (0, -1):
                ref = down_block(-k, dx)
                send(ref, ref, dev(dz=1), g)
            if k < 3 or dx in (1, 2):
                ref = down_block(k, dx)
                send(ref, ref, dev(dz=-1), g)

    def down_pass(k, *dxs):
        for dx in dxs:
            got(f"down_z{k}", down_at[k, dx])
            down_z(k, dx)

    def down_chunk(*dzs):
        for dz in dzs:
            send(wd.at[0, zi(dz)], wd.at[1, zi(dz)], dev(dc=1), across_down)

    @jax.named_scope("turn")
    def turn(slot, src, dst):
        @pl.loop(0, NZ)
        def _(k):
            cols = pl.ds(pl.multiple_of(k * per_z, per_z), per_z)
            dst[cols, pl.ds(slot * tok, tok)] = src[pl.ds(slot * tok, tok), cols].T

    e_a = own_tokens(r.ye, 0)
    up_1 = up_z(0)
    own_down = down_block(0, 0)
    down_x1, down_x2 = group(), group()
    send(own_down, own_down, dev(dx=1), down_x1)
    send(own_down, own_down, dev(dx=-1), down_x1)
    down_z(0, 0)
    up_to_x(0)
    c_a = own_tokens(r.yc, 0)
    tok_own = own_tokens(r.ye, 1)
    own_tokens(r.yc, 1, tok_own)
    turn(0, r.ye, r.et)

    got("up_z1", up_1)
    up_2 = up_z(1)
    got("down_x", down_x1)
    part = down_block(0, -1).at[pl.ds(0, rows // 2)]
    send(part, part, dev(dx=1), down_x2)
    part = down_block(0, 1).at[pl.ds(rows // 2, rows // 2)]
    send(part, part, dev(dx=-1), down_x2)
    down_z(0, -1, 1)
    up_to_x(-1)
    up_to_x(1)
    down_pass(1, 0)
    turn(0, r.yc, r.ct)
    got("up_z2", up_2)
    up_3 = up_z(2)
    up_to_x(-2)
    up_to_x(2)
    got("down_x2", down_x2)
    down_z(0, 2)
    down_chunk(0)
    up_pass_x(0)
    down_pass(1, -1, 1)
    got("up_z3", up_3)
    up_4 = up_z(3)
    up_to_x(-3)
    up_to_x(3)
    down_pass(2, 0)
    up_pass_x(-1, 1)
    down_pass(1, 2)
    down_chunk(-1, 1)
    e_f = pass_tokens(r.ye, e_a)
    down_pass(2, -1, 1)
    got("up_z4", up_4)
    up_to_x(4)
    up_column(0)
    c_f = pass_tokens(r.yc, c_a)
    l_a = own_tokens(r.yl, 0)
    tok_l = own_tokens(r.yl, 1)
    up_pass_x(-2, 2)
    down_pass(3, 0)
    down_pass(2, 2)
    down_chunk(-2, 2)
    down_pass(3, -1, 1)
    up_pass_x(-3, 3, 4)
    got("up_x_rest", up_rest)
    up_column(-1)
    up_column(1)
    down_pass(3, 2)
    down_chunk(-3, 3)
    got("up_x_last", up_last)
    up_column(2)
    got("down_z4", down_far)
    down_chunk(4)
    got("tok_own", tok_own)
    for slot in (1, 2):
        turn(slot, r.ye, r.et)
        turn(slot, r.yc, r.ct)
    got("across", across_up, across_down)

    tile = 256
    many, last = pl.ds(0, 3 * tok), pl.ds(3 * tok, tok)

    @jax.named_scope("pre_earlier")
    def pre_earlier():
        for core in range(2):

            @pl.loop(0, ff // tile)
            def _(n):
                at = pl.multiple_of(n * tile, tile)
                w_up = wu[core, :, :, pl.ds(at, tile)].reshape(d, tile)
                w_down = wd[core, :, :, pl.ds(at, tile)].reshape(d, tile)
                relu = jnp.maximum(jnp.dot(r.ye[many], w_up, preferred_element_type=F32), 0.0)
                grad = jnp.dot(r.yc[many], w_down, preferred_element_type=F32)
                out = pl.ds(pl.multiple_of(core * ff + at, tile), tile)
                r.hid[many, out] = (relu * relu).astype(BF)
                r.pg[many, out] = (2.0 * relu * grad).astype(BF)

    @jax.named_scope("pre_last_e")
    def pre_last_e():
        for core in range(2):

            @pl.loop(0, ff // tile)
            def _(n):
                at = pl.multiple_of(n * tile, tile)
                w_up = wu[core, :, :, pl.ds(at, tile)].reshape(d, tile)
                relu = jnp.maximum(jnp.dot(r.ye[last], w_up, preferred_element_type=F32), 0.0)
                out = pl.ds(pl.multiple_of(core * ff + at, tile), tile)
                r.hid[last, out] = (relu * relu).astype(BF)
                r.rel[:, out] = relu

    @jax.named_scope("pre_last_c")
    def pre_last_c():
        for core in range(2):

            @pl.loop(0, ff // tile)
            def _(n):
                at = pl.multiple_of(n * tile, tile)
                w_down = wd[core, :, :, pl.ds(at, tile)].reshape(d, tile)
                grad = jnp.dot(r.yc[last], w_down, preferred_element_type=F32)
                out = pl.ds(pl.multiple_of(core * ff + at, tile), tile)
                r.pg[last, out] = (2.0 * r.rel[:, out] * grad).astype(BF)

    @jax.named_scope("pre_later")
    def pre_later(core):
        @pl.loop(0, ff // tile)
        def _(n):
            at = pl.multiple_of(n * tile, tile)
            w_up = wu[core, :, :, pl.ds(at, tile)].reshape(d, tile)
            relu = jnp.maximum(jnp.dot(r.yl[...], w_up, preferred_element_type=F32), 0.0)
            out = pl.ds(pl.multiple_of(core * ff + at, tile), tile)
            r.hid[:, out] = (relu * relu).astype(BF)

    pre_earlier()
    got("tok_last_e", e_f)
    turn(3, r.ye, r.et)
    pre_last_e()
    got("tok_last_c", c_f)
    turn(3, r.yc, r.ct)
    pre_last_c()

    def gradient(left, right, ks, core):
        rows_at = [left[pl.ds(pl.multiple_of(k * per_z, per_z), per_z)] for k in ks]
        both = jnp.concatenate(rows_at, axis=0)
        cols = right[:, core * ff : (core + 1) * ff]
        both = jnp.dot(both, cols, preferred_element_type=F32)
        return both[:per_z], both[per_z:]

    def farthest(j):
        return zi(4 + (1 - 2 * (j % 2)) * ((j + 1) // 2))

    @jax.named_scope("cross_grad")
    def cross_grad(left, right, out, into, order):
        copies = []
        for part in range(4):
            ks = order(2 * part), order(2 * part + 1)
            for k, total in zip(ks, gradient(left, right, ks, 1)):
                out[k] = total.astype(BF)
            g = group()
            for k in ks:
                send(out.at[k], into.at[k], dev(dc=1), g)
            copies.append(g)
        return copies

    @jax.named_scope("own_grad")
    def own_grad(left, right, other, out, order, part):
        ks = order(2 * part), order(2 * part + 1)
        for k, total in zip(ks, gradient(left, right, ks, 0)):
            out[k] = (total + other[k].astype(F32)).astype(BF)

    su, sd = r.su, r.sd
    c_down = cross_grad(r.ct, r.hid, r.god, r.xd, farthest)

    arrived = {(s, first): group() for s in range(3) for first in (True, False)}
    z_last = group()
    for first in (True, False):
        arrived[3, first] = z_last

    def z_send(s, first):
        g = arrived[s, first]
        for k, buf, step in ((zi(4 - s), r.ra, 1), (zi(s - 4), r.rb, -1)):
            part = pl.ds(0 if first == (step == 1) else hz, hz)
            send(sd.at[k, part], buf.at[s, part], dev(dz=step), g)

    def hop(s, first):
        got(f"hop{s}", arrived[s - 1, first])
        for k, buf, step in ((zi(4 - s), r.ra, 1), (zi(s - 4), r.rb, -1)):
            part = pl.ds(0 if first == (step == 1) else hz, hz)
            total = sd[k, part].astype(F32) + buf[s - 1, part].astype(F32)
            sd[k, part] = total.astype(BF)
        z_send(s, first)

    c_up = cross_grad(r.et, r.pg, r.gou, r.xu, lambda j: j)
    for part in range(4):
        got("c_down", c_down[part])
        own_grad(r.ct, r.hid, r.xd, sd, farthest, part)
        if part == 0:
            z_send(0, True)
        if part == 1:
            z_send(1, False)
        if part == 2:
            pass_tokens(r.yl, l_a, tok_l)

    nh = NZ // 2
    lo, hi = pl.ds(0, nh), pl.ds(nh, nh)
    ux_a, ux_b, ur = group(), group(), group()
    for part in range(4):
        got("c_up", c_up[part])
        own_grad(r.et, r.pg, r.xu, su, lambda j: j, part)
        if part == 1:
            send(su.at[lo, xs(2)], r.sx.at[0], dev(dx=1), ux_a)
    send(su.at[hi, xs(2)], r.sx.at[1], dev(dx=-1), ux_b)
    send(su.at[hi, xs(1)], r.rx.at[0, hi], dev(dx=1), ur)
    send(su.at[lo, xs(-1)], r.rx.at[1, lo], dev(dx=-1), ur)

    @jax.named_scope("back")
    def back(left, weight, out):
        @pl.loop(0, NZ // 2)
        def _(k):
            for core in range(2):
                w = weight[core, pl.ds(2 * k, 2)].reshape(2 * per_z, ff)
                acc = dot_tt(left[:, core * ff : (core + 1) * ff], w)
                total = acc if core == 0 else total + acc
            out[:, pl.ds(pl.multiple_of(k * 2 * per_z, per_z), 2 * per_z)] = total.astype(BF)

    def start_sum(p, s, m):
        g, g0, g1 = group(), group(), group()
        send(p.at[rows_of(3, 0)], s.at[0], dev(dy=1), g)
        send(p.at[rows_of(3, 1)], s.at[1], dev(dy=-1), g)
        send(p.at[rows_of(2, 1)], m.at[0, pl.ds(half, half)], dev(dy=1), g1)
        send(p.at[rows_of(1, 0)], m.at[1, pl.ds(0, half)], dev(dy=-1), g0)
        return g, g0, g1

    def pass_sum(p, s, m, groups):
        g, g0, g1 = groups
        got("sum_first", g)
        at = rows_of(2, 0)
        p[at] = (p[at].astype(F32) + s[0].astype(F32)).astype(BF)
        send(p.at[at], m.at[0, pl.ds(0, half)], dev(dy=1), g0)
        at = rows_of(1, 1)
        p[at] = (p[at].astype(F32) + s[1].astype(F32)).astype(BF)
        send(p.at[at], m.at[1, pl.ds(half, half)], dev(dy=-1), g1)

    def end_sum(p, m, groups, out):
        for h in range(2):
            got("sum_end", groups[1 + h])
            own = rows_of(0, h)
            total = p[own].astype(F32) + m[0, own].astype(F32) + m[1, own].astype(F32)
            out[own] = total.astype(BF)

    back(r.pg, wu, r.pe)
    y_e = start_sum(r.pe, r.se, r.re)
    hop(1, True)
    hop(2, False)

    got("tok_l", tok_l)
    pre_later(0)
    got("ux", ux_a)
    su[lo, xs(1)] = (su[lo, xs(1)].astype(F32) + r.sx[0].astype(F32)).astype(BF)
    send(su.at[lo, xs(1)], r.rx.at[0, lo], dev(dx=1), ur)
    hop(2, True)
    pre_later(1)
    got("ux", ux_b)
    su[hi, xs(-1)] = (su[hi, xs(-1)].astype(F32) + r.sx[1].astype(F32)).astype(BF)
    send(su.at[hi, xs(-1)], r.rx.at[1, hi], dev(dx=-1), ur)
    hop(3, False)
    back(r.hid, wd, r.po)
    pass_sum(r.pe, r.se, r.re, y_e)
    y_o = start_sum(r.po, r.so, r.ro)
    hop(3, True)

    got("hop4", z_last)
    down_sum = sd[z].astype(F32) + r.ra[3].astype(F32) + r.rb[3].astype(F32)
    td = r.td
    td[...] = down_sum.astype(BF).reshape(NX, rows, ff)
    q0, q1 = pl.ds(0, rows // 2), pl.ds(rows // 2, rows // 2)
    dx1, dx2 = group(), group()
    send(td.at[xi(2), q0], r.xa.at[0, q0], dev(dx=1), dx1)
    send(td.at[xi(2), q1], r.xb.at[0, q1], dev(dx=-1), dx1)

    got("ur", ur)
    tu = r.tu
    tu[...] = (
        su[:, xs(0)].astype(F32) + r.rx[0].astype(F32) + r.rx[1].astype(F32)
    ).astype(BF)
    uz = [group() for _ in range(4)]
    send(tu.at[zi(4), q0], r.ua.at[0, q0], dev(dz=1), uz[0])
    send(tu.at[zi(4), q1], r.ub.at[0, q1], dev(dz=-1), uz[0])

    def add_on(acc, k, buf, s, part):
        acc[k, part] = (acc[k, part].astype(F32) + buf[s, part].astype(F32)).astype(BF)

    def up_hop(s):
        got(f"uz{s}", uz[s - 1])
        whole = pl.ds(0, rows)
        add_on(tu, zi(4 - s), r.ua, s - 1, q0 if s == 1 else whole)
        send(tu.at[zi(4 - s)], r.ua.at[s], dev(dz=1), uz[s])
        add_on(tu, zi(s - 4), r.ub, s - 1, q1 if s == 1 else whole)
        send(tu.at[zi(s - 4)], r.ub.at[s], dev(dz=-1), uz[s])

    got("dx1", dx1)
    add_on(td, xi(1), r.xa, 0, q0)
    send(td.at[xi(1)], r.xa.at[1], dev(dx=1), dx2)
    add_on(td, xi(-1), r.xb, 0, q1)
    send(td.at[xi(-1)], r.xb.at[1], dev(dx=-1), dx2)
    up_hop(1)
    for copy in totals:
        copy.wait()
    got("dx2", dx2)
    total = td[x].astype(F32) + r.xa[1].astype(F32) + r.xb[1].astype(F32)
    o_down[...] = r.tot_d[...] + total * factor
    up_hop(2)
    pass_sum(r.po, r.so, r.ro, y_o)
    up_hop(3)
    end_sum(r.pe, r.re, y_e, o_earlier)
    got("uz4", uz[3])
    total = tu[z].astype(F32) + r.ua[3].astype(F32) + r.ub[3].astype(F32)
    o_up[...] = r.tot_u[...] + total * factor
    settle()
    end_sum(r.po, r.ro, y_o, o_later)
    assert len(leaving) == N_SENT and len(arriving) == N_GOT, (len(leaving), len(arriving))


def body(later_rows, earlier_rows, cotangent, up_weight, down_weight, up_total, down_total):
    given = later_rows, earlier_rows, cotangent, up_weight, down_weight, up_total, down_total
    tok, d = later_rows.shape
    rows, ff = up_weight.shape
    total_rows = tok * lax.axis_size("fs") * lax.axis_size("tp")
    factor = 1.0 / math.sqrt(total_rows)
    scratch = scratch_of(tok, d, ff, rows)

    def run(*refs):
        kernel(list(scratch), factor, *refs)

    shapes = (
        jax.ShapeDtypeStruct((tok, d), BF),
        jax.ShapeDtypeStruct((tok, d), BF),
        jax.ShapeDtypeStruct((rows, ff), F32),
        jax.ShapeDtypeStruct((rows, ff), F32),
    )
    results = pl.pallas_call(
        run,
        out_shape=shapes,
        in_specs=[pl.BlockSpec(memory_space=pltpu.HBM)] * 7,
        out_specs=(pl.BlockSpec(memory_space=pltpu.VMEM),) * 4,
        scratch_shapes=list(scratch.values()),
        compiler_params=pltpu.CompilerParams(
            collective_id=0, has_side_effects=True, vmem_limit_bytes=50 * 2**20
        ),
        name="ffn_step",
    )(*(pltpu.with_memory_space_constraint(a, pltpu.HBM) for a in given))
    return pl.pallas_call(
        store,
        out_shape=shapes,
        in_specs=[pl.BlockSpec(memory_space=pltpu.VMEM)] * 4,
        out_specs=(pl.BlockSpec(memory_space=pl.ANY),) * 4,
        scratch_shapes=[pltpu.SemaphoreType.DMA((4,))],
        compiler_params=pltpu.CompilerParams(vmem_limit_bytes=4 * 2**20),
        name="ffn_store",
    )(*results)


def store(*refs):
    copies = [pltpu.make_async_copy(refs[i], refs[4 + i], refs[8].at[i]) for i in range(4)]
    for copy in copies:
        copy.start()
    for copy in copies:
        copy.wait()


def solution(mesh):
    tokens = P(("fs", "tp"), None)
    weight = P("fs", "tp")
    return jax.shard_map(
        body,
        mesh=mesh,
        in_specs=(tokens, tokens, tokens, weight, weight, weight, weight),
        out_specs=(tokens, tokens, weight, weight),
        check_vma=False,
    )
```

```python
import math
from types import SimpleNamespace

import jax
import jax.numpy as jnp
from jax import lax
from jax.experimental import pallas as pl
from jax.experimental.pallas import tpu as pltpu
from jax.sharding import PartitionSpec as P

NZ, NX, NY = 8, 4, 4
BF = jnp.bfloat16
F32 = jnp.float32
N_SENT = 13
N_GOT = 71


def scratch_of(tok, d, ff, rows):
    per_z = NX * rows
    vm = pltpu.VMEM
    return dict(
        ye=vm((4 * tok, d), BF),
        yc=vm((4 * tok, d), BF),
        yl=vm((4 * tok, d), BF),
        wu=vm((2, NZ, per_z, ff), BF),
        wd=vm((2, NZ, per_z, ff), BF),
        hid=vm((4 * tok, 2 * ff), BF),
        rel=vm((tok, 2 * ff), F32),
        pg=vm((4 * tok, 2 * ff), BF),
        pe=vm((4 * tok, d), BF),
        po=vm((4 * tok, d), BF),
        se=vm((2, tok // 2, d), BF),
        so=vm((2, tok // 2, d), BF),
        re=vm((2, tok, d), BF),
        ro=vm((2, tok, d), BF),
        gou=vm((NZ, per_z, ff), BF),
        god=vm((NZ, per_z, ff), BF),
        xu=vm((NZ, per_z, ff), BF),
        xd=vm((NZ, per_z, ff), BF),
        su=vm((NZ, per_z, ff), BF),
        sd=vm((NZ, per_z, ff), BF),
        sx=vm((2, NZ // 2, rows, ff), BF),
        rx=vm((2, NZ, rows, ff), BF),
        tu=vm((NZ, rows, ff), BF),
        ua=vm((4, rows, ff), BF),
        ub=vm((4, rows, ff), BF),
        ra=vm((4, per_z, ff), BF),
        rb=vm((4, per_z, ff), BF),
        td=vm((NX, rows, ff), BF),
        xa=vm((2, rows, ff), BF),
        xb=vm((2, rows, ff), BF),
        et=vm((d, 4 * tok), BF),
        ct=vm((d, 4 * tok), BF),
        tot_u=vm((rows, ff), F32),
        tot_d=vm((rows, ff), F32),
        send=pltpu.SemaphoreType.DMA((N_SENT,)),
        recv=pltpu.SemaphoreType.DMA((N_GOT,)),
        local=pltpu.SemaphoreType.DMA((7,)),
    )


def dot_tt(a, b):
    return lax.dot_general(a, b, (((1,), (1,)), ((), ())), preferred_element_type=F32)


def kernel(names, factor, *refs):
    later, earlier, cot, up, down, up_total, down_total = refs[:7]
    o_later, o_earlier, o_up, o_down = refs[7:11]
    r = SimpleNamespace(**dict(zip(names, refs[11:])))
    tok, d = later.shape
    rows, ff = up.shape
    half = tok // 2
    per_z = NX * rows
    hz = per_z // 2

    f, t = lax.axis_index("fs"), lax.axis_index("tp")
    z, x = f // NX, f % NX
    y, c = t // 2, t % 2

    def zi(k):
        return (z + k + NZ) % NZ

    def xi(k):
        return (x + k + NX) % NX

    def dev(dz=0, dx=0, dy=0, dc=0):
        fs = zi(dz) * NX + xi(dx)
        tp = ((y + dy + NY) % NY) * 2 + (c + dc) % 2
        return {"fs": fs, "tp": tp}

    row_bytes = d * 2
    limit = r.ye.shape[0] * row_bytes
    leaving, arriving = [], []

    def group():
        g = SimpleNamespace(at=len(arriving), bytes=0)
        arriving.append(g)
        return g

    def wait(sem, g):
        ref = r.ye.at[pl.ds(0, g.bytes // row_bytes)]
        pltpu.make_async_copy(ref, ref, sem).wait()

    def send(src, dst, to, g=None):
        size = math.prod(src.shape) * 2
        g = group() if g is None else g
        g.bytes += size
        if not leaving or leaving[-1].done or leaving[-1].bytes + size > limit:
            leaving.append(SimpleNamespace(bytes=0, done=False))
        leaving[-1].bytes += size
        pltpu.make_async_remote_copy(
            src_ref=src,
            dst_ref=dst,
            send_sem=r.send.at[len(leaving) - 1],
            recv_sem=r.recv.at[g.at],
            device_id=to,
            device_id_type=pl.DeviceIdType.MESH,
        ).start()
        return g

    @jax.named_scope("sent")
    def settle():
        for i, g in enumerate(leaving):
            if not g.done:
                wait(r.send.at[i], g)
                g.done = True

    def got(name, *groups):
        with jax.named_scope(name):
            for g in {g.at: g for g in groups}.values():
                wait(r.recv.at[g.at], g)

    local = []

    def fetch(src, dst):
        copy = pltpu.make_async_copy(src, dst, r.local.at[len(local)])
        copy.start()
        local.append(copy)
        return copy

    def xs(k):
        return pl.ds(pl.multiple_of(xi(k) * rows, rows), rows)

    first = [
        fetch(earlier, r.ye.at[pl.ds(0, tok)]),
        fetch(cot, r.yc.at[pl.ds(0, tok)]),
        fetch(up, r.wu.at[0, z, xs(0)]),
        fetch(down, r.wd.at[0, z, xs(0)]),
        fetch(later, r.yl.at[pl.ds(0, tok)]),
    ]
    totals = [fetch(up_total, r.tot_u), fetch(down_total, r.tot_d)]

    barrier = pltpu.get_barrier_semaphore()
    partners = [dev(dy=1), dev(dy=-1), dev(dx=1), dev(dx=-1), dev(dz=1), dev(dz=-1), dev(dc=1)]
    for p in partners:
        pl.semaphore_signal(barrier, inc=1, device_id=p, device_id_type=pl.DeviceIdType.MESH)
    with jax.named_scope("barrier"):
        pl.semaphore_wait(barrier, len(partners))
        for copy in first:
            copy.wait()

    def rows_of(slot, h):
        return pl.ds(slot * tok + h * half, half)

    def own_tokens(buf, h, g=None):
        g = g or group()
        send(buf.at[rows_of(0, h)], buf.at[rows_of(1, h)], dev(dy=1), g)
        send(buf.at[rows_of(0, 1 - h)], buf.at[rows_of(2, 1 - h)], dev(dy=-1), g)
        return g

    def pass_tokens(buf, first, g=None):
        g = g or group()
        got("tok_first", first)
        send(buf.at[rows_of(1, 0)], buf.at[rows_of(3, 0)], dev(dy=1), g)
        send(buf.at[rows_of(2, 1)], buf.at[rows_of(3, 1)], dev(dy=-1), g)
        return g

    wu, wd = r.wu, r.wd

    def up_block(dz, dx):
        return wu.at[0, zi(dz), xs(dx)]

    def up_z(k):
        g = group()
        for step in (1, -1):
            ref = up_block(-k * step, 0)
            if k == 3:
                ref = ref.at[pl.ds(0 if step == 1 else rows // 2, rows // 2)]
            send(ref, ref, dev(dz=step), g)
        return g

    up_first, up_rest, up_last = {}, group(), group()

    def up_to_x(dz):
        ref = up_block(dz, 0)
        up_first[dz] = group()
        plus, minus = (up_first[dz], up_rest) if 0 <= dz <= 3 else (up_rest, up_first[dz])
        send(ref, ref, dev(dx=1), plus)
        send(ref, ref, dev(dx=-1), minus)

    def up_pass_x(*dzs):
        for dz in dzs:
            got("up_x", up_first[dz])
            step = 1 if 0 <= dz <= 3 else -1
            ref = up_block(dz, -step)
            send(ref, ref, dev(dx=step), up_last)

    across_up, across_down = group(), group()

    def up_column(dx):
        src = wu.at[0, :, xs(dx)]
        send(src, wu.at[1, :, xs(dx)], dev(dc=1), across_up)

    def down_block(dz, dx):
        return wd.at[0, zi(dz), xs(dx)]

    down_far = group()
    down_at = {}

    def down_z(k, *dxs):
        for dx in dxs:
            g = down_far if k == 3 else group()
            down_at[k + 1, dx] = g
            if k < 3 or dx in (0, -1):
                ref = down_block(-k, dx)
                send(ref, ref, dev(dz=1), g)
            if k < 3 or dx in (1, 2):
                ref = down_block(k, dx)
                send(ref, ref, dev(dz=-1), g)

    def down_pass(k, *dxs):
        for dx in dxs:
            got(f"down_z{k}", down_at[k, dx])
            down_z(k, dx)

    def down_chunk(*dzs):
        for dz in dzs:
            send(wd.at[0, zi(dz)], wd.at[1, zi(dz)], dev(dc=1), across_down)

    @jax.named_scope("turn")
    def turn(slot, src, dst):
        @pl.loop(0, NZ)
        def _(k):
            cols = pl.ds(pl.multiple_of(k * per_z, per_z), per_z)
            dst[cols, pl.ds(slot * tok, tok)] = src[pl.ds(slot * tok, tok), cols].T

    e_a = own_tokens(r.ye, 0)
    up_1 = up_z(0)
    own_down = down_block(0, 0)
    down_x1, down_x2 = group(), group()
    send(own_down, own_down, dev(dx=1), down_x1)
    send(own_down, own_down, dev(dx=-1), down_x1)
    down_z(0, 0)
    up_to_x(0)
    c_a = own_tokens(r.yc, 0)
    tok_own = own_tokens(r.ye, 1)
    own_tokens(r.yc, 1, tok_own)
    turn(0, r.ye, r.et)

    got("up_z1", up_1)
    up_2 = up_z(1)
    got("down_x", down_x1)
    part = down_block(0, -1).at[pl.ds(0, rows // 2)]
    send(part, part, dev(dx=1), down_x2)
    part = down_block(0, 1).at[pl.ds(rows // 2, rows // 2)]
    send(part, part, dev(dx=-1), down_x2)
    down_z(0, -1, 1)
    up_to_x(-1)
    up_to_x(1)
    down_pass(1, 0)
    turn(0, r.yc, r.ct)
    got("up_z2", up_2)
    up_3 = up_z(2)
    up_to_x(-2)
    up_to_x(2)
    got("down_x2", down_x2)
    down_z(0, 2)
    down_chunk(0)
    up_pass_x(0)
    down_pass(1, -1, 1)
    got("up_z3", up_3)
    up_4 = up_z(3)
    up_to_x(-3)
    up_to_x(3)
    down_pass(2, 0)
    up_pass_x(-1, 1)
    down_pass(1, 2)
    down_chunk(-1, 1)
    e_f = pass_tokens(r.ye, e_a)
    down_pass(2, -1, 1)
    got("up_z4", up_4)
    up_to_x(4)
    up_column(0)
    c_f = pass_tokens(r.yc, c_a)
    l_a = own_tokens(r.yl, 0)
    tok_l = own_tokens(r.yl, 1)
    up_pass_x(-2, 2)
    down_pass(3, 0)
    down_pass(2, 2)
    down_chunk(-2, 2)
    down_pass(3, -1, 1)
    up_pass_x(-3, 3, 4)
    got("up_x_rest", up_rest)
    up_column(-1)
    up_column(1)
    down_pass(3, 2)
    down_chunk(-3, 3)
    got("up_x_last", up_last)
    up_column(2)
    got("down_z4", down_far)
    down_chunk(4)
    got("tok_own", tok_own)
    for slot in (1, 2):
        turn(slot, r.ye, r.et)
        turn(slot, r.yc, r.ct)
    got("across", across_up, across_down)

    tile = 256
    many, last = pl.ds(0, 3 * tok), pl.ds(3 * tok, tok)

    @jax.named_scope("pre_earlier")
    def pre_earlier():
        for core in range(2):

            @pl.loop(0, ff // tile)
            def _(n):
                at = pl.multiple_of(n * tile, tile)
                w_up = wu[core, :, :, pl.ds(at, tile)].reshape(d, tile)
                w_down = wd[core, :, :, pl.ds(at, tile)].reshape(d, tile)
                relu = jnp.maximum(jnp.dot(r.ye[many], w_up, preferred_element_type=F32), 0.0)
                grad = jnp.dot(r.yc[many], w_down, preferred_element_type=F32)
                out = pl.ds(pl.multiple_of(core * ff + at, tile), tile)
                r.hid[many, out] = (relu * relu).astype(BF)
                r.pg[many, out] = (2.0 * relu * grad).astype(BF)

    @jax.named_scope("pre_last_e")
    def pre_last_e():
        for core in range(2):

            @pl.loop(0, ff // tile)
            def _(n):
                at = pl.multiple_of(n * tile, tile)
                w_up = wu[core, :, :, pl.ds(at, tile)].reshape(d, tile)
                relu = jnp.maximum(jnp.dot(r.ye[last], w_up, preferred_element_type=F32), 0.0)
                out = pl.ds(pl.multiple_of(core * ff + at, tile), tile)
                r.hid[last, out] = (relu * relu).astype(BF)
                r.rel[:, out] = relu

    @jax.named_scope("pre_last_c")
    def pre_last_c():
        for core in range(2):

            @pl.loop(0, ff // tile)
            def _(n):
                at = pl.multiple_of(n * tile, tile)
                w_down = wd[core, :, :, pl.ds(at, tile)].reshape(d, tile)
                grad = jnp.dot(r.yc[last], w_down, preferred_element_type=F32)
                out = pl.ds(pl.multiple_of(core * ff + at, tile), tile)
                r.pg[last, out] = (2.0 * r.rel[:, out] * grad).astype(BF)

    @jax.named_scope("pre_later")
    def pre_later(core):
        @pl.loop(0, ff // tile)
        def _(n):
            at = pl.multiple_of(n * tile, tile)
            w_up = wu[core, :, :, pl.ds(at, tile)].reshape(d, tile)
            relu = jnp.maximum(jnp.dot(r.yl[...], w_up, preferred_element_type=F32), 0.0)
            out = pl.ds(pl.multiple_of(core * ff + at, tile), tile)
            r.hid[:, out] = (relu * relu).astype(BF)

    pre_earlier()
    got("tok_last_e", e_f)
    turn(3, r.ye, r.et)
    pre_last_e()
    got("tok_last_c", c_f)
    turn(3, r.yc, r.ct)
    pre_last_c()

    def gradient(left, right, ks, core):
        rows_at = [left[pl.ds(pl.multiple_of(k * per_z, per_z), per_z)] for k in ks]
        both = jnp.concatenate(rows_at, axis=0)
        cols = right[:, core * ff : (core + 1) * ff]
        both = jnp.dot(both, cols, preferred_element_type=F32)
        return both[:per_z], both[per_z:]

    def farthest(j):
        return zi(4 + (1 - 2 * (j % 2)) * ((j + 1) // 2))

    @jax.named_scope("cross_grad")
    def cross_grad(left, right, out, into, order):
        copies = []
        for part in range(4):
            ks = order(2 * part), order(2 * part + 1)
            for k, total in zip(ks, gradient(left, right, ks, 1)):
                out[k] = total.astype(BF)
            g = group()
            for k in ks:
                send(out.at[k], into.at[k], dev(dc=1), g)
            copies.append(g)
        return copies

    @jax.named_scope("own_grad")
    def own_grad(left, right, other, out, order, part):
        ks = order(2 * part), order(2 * part + 1)
        for k, total in zip(ks, gradient(left, right, ks, 0)):
            out[k] = (total + other[k].astype(F32)).astype(BF)

    su, sd = r.su, r.sd

    def z_sum(name, acc, plus, minus, size):
        steps = {(s, first): group() for s in range(3) for first in (True, False)}
        steps[3, True] = steps[3, False] = end = group()

        def ways(s, first):
            for k, buf, step in ((zi(4 - s), plus, 1), (zi(s - 4), minus, -1)):
                yield k, buf, step, pl.ds(0 if first == (step == 1) else size, size)

        def start(s, first):
            for k, buf, step, part in ways(s, first):
                send(acc.at[k, part], buf.at[s, part], dev(dz=step), steps[s, first])

        def hop(s, first):
            got(f"{name}{s}", steps[s - 1, first])
            for k, buf, step, part in ways(s, first):
                total = acc[k, part].astype(F32) + buf[s - 1, part].astype(F32)
                acc[k, part] = total.astype(BF)
            start(s, first)

        def finish():
            got(f"{name}4", end)
            return acc[z].astype(F32) + plus[3].astype(F32) + minus[3].astype(F32)

        return start, hop, finish

    z_send, hop, z_end = z_sum("hop", sd, r.ra, r.rb, hz)
    uz_send, uz_hop, uz_end = z_sum("uz", r.tu, r.ua, r.ub, rows // 2)

    @jax.named_scope("back")
    def back(left, weight, out, part):
        @pl.loop(0, NZ // 2)
        def _(k):
            for core in range(2):
                w = weight[core, pl.ds(2 * k, 2)].reshape(2 * per_z, ff)
                acc = dot_tt(left[part, core * ff : (core + 1) * ff], w)
                total = acc if core == 0 else total + acc
            at = pl.ds(pl.multiple_of(k * 2 * per_z, per_z), 2 * per_z)
            out[part, at] = total.astype(BF)

    def start_sum(p, s):
        g = group()
        send(p.at[rows_of(3, 0)], s.at[0], dev(dy=1), g)
        send(p.at[rows_of(3, 1)], s.at[1], dev(dy=-1), g)
        return g

    def more_sum(p, m):
        g0, g1 = group(), group()
        send(p.at[rows_of(2, 1)], m.at[0, pl.ds(half, half)], dev(dy=1), g1)
        send(p.at[rows_of(1, 0)], m.at[1, pl.ds(0, half)], dev(dy=-1), g0)
        return g0, g1

    def pass_sum(p, s, m, g, groups):
        g0, g1 = groups
        got("sum_first", g)
        at = rows_of(2, 0)
        p[at] = (p[at].astype(F32) + s[0].astype(F32)).astype(BF)
        send(p.at[at], m.at[0, pl.ds(0, half)], dev(dy=1), g0)
        at = rows_of(1, 1)
        p[at] = (p[at].astype(F32) + s[1].astype(F32)).astype(BF)
        send(p.at[at], m.at[1, pl.ds(half, half)], dev(dy=-1), g1)

    def end_sum(p, m, groups, out):
        for h in range(2):
            got("sum_end", groups[h])
            own = rows_of(0, h)
            total = p[own].astype(F32) + m[0, own].astype(F32) + m[1, own].astype(F32)
            out[own] = total.astype(BF)

    back(r.pg, wu, r.pe, last)
    c_down = cross_grad(r.ct, r.hid, r.god, r.xd, farthest)
    pass_tokens(r.yl, l_a, tok_l)
    first_e = start_sum(r.pe, r.se)
    c_up = cross_grad(r.et, r.pg, r.gou, r.xu, lambda j: j)
    for part in range(4):
        got("c_down", c_down[part])
        own_grad(r.ct, r.hid, r.xd, sd, farthest, part)
        if part == 0:
            z_send(0, True)
        if part == 1:
            z_send(1, False)

    nh = NZ // 2
    lo, hi = pl.ds(0, nh), pl.ds(nh, nh)
    ux_a, ux_b, ur = group(), group(), group()
    for part in range(4):
        got("c_up", c_up[part])
        own_grad(r.et, r.pg, r.xu, su, lambda j: j, part)
        if part == 1:
            send(su.at[lo, xs(2)], r.sx.at[0], dev(dx=1), ux_a)
    send(su.at[hi, xs(2)], r.sx.at[1], dev(dx=-1), ux_b)
    send(su.at[hi, xs(1)], r.rx.at[0, hi], dev(dx=1), ur)
    send(su.at[lo, xs(-1)], r.rx.at[1, lo], dev(dx=-1), ur)

    back(r.pg, wu, r.pe, many)
    more_e = more_sum(r.pe, r.re)
    hop(1, True)
    hop(2, False)

    got("tok_l", tok_l)
    pre_later(0)
    got("ux", ux_a)
    su[lo, xs(1)] = (su[lo, xs(1)].astype(F32) + r.sx[0].astype(F32)).astype(BF)
    send(su.at[lo, xs(1)], r.rx.at[0, lo], dev(dx=1), ur)
    hop(2, True)
    pre_later(1)
    got("ux", ux_b)
    su[hi, xs(-1)] = (su[hi, xs(-1)].astype(F32) + r.sx[1].astype(F32)).astype(BF)
    send(su.at[hi, xs(-1)], r.rx.at[1, hi], dev(dx=-1), ur)
    hop(3, False)
    pass_sum(r.pe, r.se, r.re, first_e, more_e)
    back(r.hid, wd, r.po, pl.ds(0, 4 * tok))
    first_o = start_sum(r.po, r.so)
    more_o = more_sum(r.po, r.ro)
    hop(3, True)

    down_sum = z_end()
    td = r.td
    td[...] = down_sum.astype(BF).reshape(NX, rows, ff)
    q0, q1 = pl.ds(0, rows // 2), pl.ds(rows // 2, rows // 2)
    dx1, dx2 = group(), group()
    send(td.at[xi(2), q0], r.xa.at[0, q0], dev(dx=1), dx1)
    send(td.at[xi(2), q1], r.xb.at[0, q1], dev(dx=-1), dx1)

    got("ur", ur)
    tu = r.tu
    tu[...] = (
        su[:, xs(0)].astype(F32) + r.rx[0].astype(F32) + r.rx[1].astype(F32)
    ).astype(BF)
    uz_send(0, True)
    uz_send(1, False)

    def add_on(acc, k, buf, s, part):
        acc[k, part] = (acc[k, part].astype(F32) + buf[s, part].astype(F32)).astype(BF)

    got("dx1", dx1)
    add_on(td, xi(1), r.xa, 0, q0)
    send(td.at[xi(1)], r.xa.at[1], dev(dx=1), dx2)
    add_on(td, xi(-1), r.xb, 0, q1)
    send(td.at[xi(-1)], r.xb.at[1], dev(dx=-1), dx2)
    uz_hop(1, True)
    uz_hop(2, False)
    for copy in totals:
        copy.wait()
    uz_hop(2, True)
    uz_hop(3, False)
    got("dx2", dx2)
    total = td[x].astype(F32) + r.xa[1].astype(F32) + r.xb[1].astype(F32)
    o_down[...] = r.tot_d[...] + total * factor
    uz_hop(3, True)
    pass_sum(r.po, r.so, r.ro, first_o, more_o)
    end_sum(r.pe, r.re, more_e, o_earlier)
    o_up[...] = r.tot_u[...] + uz_end() * factor
    settle()
    end_sum(r.po, r.ro, more_o, o_later)
    assert len(leaving) == N_SENT and len(arriving) == N_GOT, (len(leaving), len(arriving))


def body(later_rows, earlier_rows, cotangent, up_weight, down_weight, up_total, down_total):
    given = later_rows, earlier_rows, cotangent, up_weight, down_weight, up_total, down_total
    tok, d = later_rows.shape
    rows, ff = up_weight.shape
    total_rows = tok * lax.axis_size("fs") * lax.axis_size("tp")
    factor = 1.0 / math.sqrt(total_rows)
    scratch = scratch_of(tok, d, ff, rows)

    def run(*refs):
        kernel(list(scratch), factor, *refs)

    shapes = (
        jax.ShapeDtypeStruct((tok, d), BF),
        jax.ShapeDtypeStruct((tok, d), BF),
        jax.ShapeDtypeStruct((rows, ff), F32),
        jax.ShapeDtypeStruct((rows, ff), F32),
    )
    results = pl.pallas_call(
        run,
        out_shape=shapes,
        in_specs=[pl.BlockSpec(memory_space=pltpu.HBM)] * 7,
        out_specs=(pl.BlockSpec(memory_space=pltpu.VMEM),) * 4,
        scratch_shapes=list(scratch.values()),
        compiler_params=pltpu.CompilerParams(
            collective_id=0, has_side_effects=True, vmem_limit_bytes=50 * 2**20
        ),
        name="ffn_step",
    )(*(pltpu.with_memory_space_constraint(a, pltpu.HBM) for a in given))
    return pl.pallas_call(
        store,
        out_shape=shapes,
        in_specs=[pl.BlockSpec(memory_space=pltpu.VMEM)] * 4,
        out_specs=(pl.BlockSpec(memory_space=pl.ANY),) * 4,
        scratch_shapes=[pltpu.SemaphoreType.DMA((4,))],
        compiler_params=pltpu.CompilerParams(vmem_limit_bytes=4 * 2**20),
        name="ffn_store",
    )(*results)


def store(*refs):
    copies = [pltpu.make_async_copy(refs[i], refs[4 + i], refs[8].at[i]) for i in range(4)]
    for copy in copies:
        copy.start()
    for copy in copies:
        copy.wait()


def solution(mesh):
    tokens = P(("fs", "tp"), None)
    weight = P("fs", "tp")
    return jax.shard_map(
        body,
        mesh=mesh,
        in_specs=(tokens, tokens, tokens, weight, weight, weight, weight),
        out_specs=(tokens, tokens, weight, weight),
        check_vma=False,
    )
```

```python
import math
from types import SimpleNamespace

import jax
import jax.numpy as jnp
from jax import lax
from jax.experimental import pallas as pl
from jax.experimental.pallas import tpu as pltpu
from jax.sharding import PartitionSpec as P

NZ, NX, NY = 8, 4, 4
BF = jnp.bfloat16
F32 = jnp.float32
N_SENT = 13
N_GOT = 67


def scratch_of(tok, d, ff, rows):
    per_z = NX * rows
    vm = pltpu.VMEM
    return dict(
        ye=vm((4 * tok, d), BF),
        yc=vm((4 * tok, d), BF),
        yl=vm((4 * tok, d), BF),
        wu=vm((2, NZ, per_z, ff), BF),
        wd=vm((2, NZ, per_z, ff), BF),
        hid=vm((4 * tok, 2 * ff), BF),
        rel=vm((tok, 2 * ff), F32),
        pg=vm((4 * tok, 2 * ff), BF),
        pe=vm((4 * tok, d), BF),
        po=vm((4 * tok, d), BF),
        se=vm((2, tok // 2, d), BF),
        so=vm((2, tok // 2, d), BF),
        re=vm((2, tok, d), BF),
        ro=vm((2, tok, d), BF),
        gou=vm((NZ, per_z, ff), BF),
        god=vm((NZ, per_z, ff), BF),
        xu=vm((NZ, per_z, ff), BF),
        xd=vm((NZ, per_z, ff), BF),
        su=vm((NZ, per_z, ff), BF),
        sd=vm((NZ, per_z, ff), BF),
        sx=vm((2, NZ // 2, rows, ff), BF),
        rx=vm((2, NZ, rows, ff), BF),
        tu=vm((NZ, rows, ff), BF),
        ua=vm((4, rows, ff), BF),
        ub=vm((4, rows, ff), BF),
        ra=vm((4, per_z, ff), BF),
        rb=vm((4, per_z, ff), BF),
        td=vm((NX, rows, ff), BF),
        xa=vm((2, rows, ff), BF),
        xb=vm((2, rows, ff), BF),
        et=vm((d, 4 * tok), BF),
        ct=vm((d, 4 * tok), BF),
        tot_u=vm((rows, ff), F32),
        tot_d=vm((rows, ff), F32),
        send=pltpu.SemaphoreType.DMA((N_SENT,)),
        recv=pltpu.SemaphoreType.DMA((N_GOT,)),
        told=pltpu.SemaphoreType.REGULAR,
        local=pltpu.SemaphoreType.DMA((2,)),
    )


def dot_tt(a, b):
    return lax.dot_general(a, b, (((1,), (1,)), ((), ())), preferred_element_type=F32)


def kernel(names, factor, *refs):
    later, earlier, cot, up, down, up_total, down_total = refs[:7]
    o_later, o_earlier, o_up, o_down = refs[7:11]
    r = SimpleNamespace(**dict(zip(names, refs[11:])))
    tok, d = later.shape
    rows, ff = up.shape
    half = tok // 2
    per_z = NX * rows
    hz = per_z // 2

    f, t = lax.axis_index("fs"), lax.axis_index("tp")
    z, x = f // NX, f % NX
    y, c = t // 2, t % 2

    def zi(k):
        return (z + k + NZ) % NZ

    def xi(k):
        return (x + k + NX) % NX

    def dev(dz=0, dx=0, dy=0, dc=0):
        fs = zi(dz) * NX + xi(dx)
        tp = ((y + dy + NY) % NY) * 2 + (c + dc + 2) % 2
        return {"fs": fs, "tp": tp}

    row_bytes = d * 2
    limit = r.ye.shape[0] * row_bytes
    leaving, arriving = [], []

    def group():
        g = SimpleNamespace(at=len(arriving), bytes=0)
        arriving.append(g)
        return g

    def wait(sem, g):
        ref = r.ye.at[pl.ds(0, g.bytes // row_bytes)]
        pltpu.make_async_copy(ref, ref, sem).wait()

    def send(src, dst, to, g=None):
        size = math.prod(src.shape) * 2
        g = group() if g is None else g
        g.bytes += size
        if not leaving or leaving[-1].done or leaving[-1].bytes + size > limit:
            leaving.append(SimpleNamespace(bytes=0, done=False))
        leaving[-1].bytes += size
        pltpu.make_async_remote_copy(
            src_ref=src,
            dst_ref=dst,
            send_sem=r.send.at[len(leaving) - 1],
            recv_sem=r.recv.at[g.at],
            device_id=to,
            device_id_type=pl.DeviceIdType.MESH,
        ).start()
        return g

    @jax.named_scope("sent")
    def settle():
        for i, g in enumerate(leaving):
            if not g.done:
                wait(r.send.at[i], g)
                g.done = True

    def got(name, *groups):
        with jax.named_scope(name):
            for g in {g.at: g for g in groups}.values():
                wait(r.recv.at[g.at], g)

    def fetch(i, *pairs):
        g = SimpleNamespace(bytes=0)
        for src, dst in pairs:
            pltpu.make_async_copy(src, dst, r.local.at[i]).start()
            g.bytes += math.prod(src.shape) * src.dtype.itemsize
        return lambda: wait(r.local.at[i], g)

    def xs(k):
        return pl.ds(pl.multiple_of(xi(k) * rows, rows), rows)

    inputs = fetch(
        0,
        (earlier, r.ye.at[pl.ds(0, tok)]),
        (up, r.wu.at[0, z, xs(0)]),
        (down, r.wd.at[0, z, xs(0)]),
        (cot, r.yc.at[pl.ds(0, tok)]),
        (later, r.yl.at[pl.ds(0, tok)]),
    )
    totals = fetch(1, (up_total, r.tot_u), (down_total, r.tot_d))

    barrier = pltpu.get_barrier_semaphore()

    def enter(**to):
        pl.semaphore_signal(
            barrier, inc=1, device_id=dev(**to), device_id_type=pl.DeviceIdType.MESH
        )

    def tell():
        pl.semaphore_signal(
            r.told, inc=1, device_id=dev(dc=1), device_id_type=pl.DeviceIdType.MESH
        )

    for step in (1, -1):
        enter(dy=step, dc=-c)
        enter(dx=step, dc=-c)
        enter(dz=step, dc=1 - c)
    enter(dc=1)

    with jax.named_scope("barrier"):

        @pl.when(c == 0)
        def _():
            pl.semaphore_wait(barrier, 9)
            tell()

        @pl.when(c == 1)
        def _():
            pl.semaphore_wait(r.told, 1)

        inputs()

    def enter_z():
        with jax.named_scope("barrier_z"):

            @pl.when(c == 1)
            def _():
                pl.semaphore_wait(barrier, 5)
                tell()

            @pl.when(c == 0)
            def _():
                pl.semaphore_wait(r.told, 1)

    def rows_of(slot, h):
        return pl.ds(slot * tok + h * half, half)

    def own_tokens(buf, h, g=None):
        g = g or group()
        send(buf.at[rows_of(0, h)], buf.at[rows_of(1, h)], dev(dy=1), g)
        send(buf.at[rows_of(0, 1 - h)], buf.at[rows_of(2, 1 - h)], dev(dy=-1), g)
        return g

    def pass_tokens(buf, first, g=None):
        g = g or group()
        got("tok_first", first)
        send(buf.at[rows_of(1, 0)], buf.at[rows_of(3, 0)], dev(dy=1), g)
        send(buf.at[rows_of(2, 1)], buf.at[rows_of(3, 1)], dev(dy=-1), g)
        return g

    wu, wd = r.wu, r.wd

    def up_block(dz, dx):
        return wu.at[0, zi(dz), xs(dx)]

    def up_z(k):
        g = group()
        for step in (1, -1):
            ref = up_block(-k * step, 0)
            if k == 3:
                ref = ref.at[pl.ds(0 if step == 1 else rows // 2, rows // 2)]
            send(ref, ref, dev(dz=step), g)
        return g

    up_first, up_rest, up_last = [group() for _ in range(4)], group(), group()

    def up_to_x(dz):
        ref = up_block(dz, 0)
        first = up_first[min(abs(dz), 3)]
        plus, minus = (first, up_rest) if 0 <= dz <= 3 else (up_rest, first)
        send(ref, ref, dev(dx=1), plus)
        send(ref, ref, dev(dx=-1), minus)

    def up_pass_x(*dzs):
        got("up_x", up_first[min(abs(dzs[0]), 3)])
        for dz in dzs:
            step = 1 if 0 <= dz <= 3 else -1
            ref = up_block(dz, -step)
            send(ref, ref, dev(dx=step), up_last)

    across_up, across_down = group(), group()

    def up_column(dx):
        src = wu.at[0, :, xs(dx)]
        send(src, wu.at[1, :, xs(dx)], dev(dc=1), across_up)

    def down_block(dz, dx):
        return wd.at[0, zi(dz), xs(dx)]

    down_far = group()
    down_at = {}

    def down_z(k, *dxs):
        for dx in dxs:
            g = down_far if k == 3 else group()
            down_at[k + 1, dx] = g
            if k < 3 or dx in (0, -1):
                ref = down_block(-k, dx)
                send(ref, ref, dev(dz=1), g)
            if k < 3 or dx in (1, 2):
                ref = down_block(k, dx)
                send(ref, ref, dev(dz=-1), g)

    def down_pass(k, *dxs):
        for dx in dxs:
            got(f"down_z{k}", down_at[k, dx])
            down_z(k, dx)

    def down_chunk(*dzs):
        for dz in dzs:
            send(wd.at[0, zi(dz)], wd.at[1, zi(dz)], dev(dc=1), across_down)

    @jax.named_scope("turn")
    def turn(slot, src, dst):
        @pl.loop(0, NZ)
        def _(k):
            cols = pl.ds(pl.multiple_of(k * per_z, per_z), per_z)
            dst[cols, pl.ds(slot * tok, tok)] = src[pl.ds(slot * tok, tok), cols].T

    e_a = own_tokens(r.ye, 0)
    own_down = down_block(0, 0)
    down_x1, down_x2 = group(), group()
    send(own_down, own_down, dev(dx=1), down_x1)
    send(own_down, own_down, dev(dx=-1), down_x1)
    up_to_x(0)
    c_a = own_tokens(r.yc, 0)
    tok_own = own_tokens(r.ye, 1)
    own_tokens(r.yc, 1, tok_own)
    enter_z()
    up_1 = up_z(0)
    down_z(0, 0)
    turn(0, r.ye, r.et)

    got("up_z1", up_1)
    up_2 = up_z(1)
    got("down_x", down_x1)
    part = down_block(0, -1).at[pl.ds(0, rows // 2)]
    send(part, part, dev(dx=1), down_x2)
    part = down_block(0, 1).at[pl.ds(rows // 2, rows // 2)]
    send(part, part, dev(dx=-1), down_x2)
    down_z(0, -1, 1)
    up_to_x(-1)
    up_to_x(1)
    down_pass(1, 0)
    turn(0, r.yc, r.ct)
    got("up_z2", up_2)
    up_3 = up_z(2)
    up_to_x(-2)
    up_to_x(2)
    got("down_x2", down_x2)
    down_z(0, 2)
    down_chunk(0)
    up_pass_x(0)
    down_pass(1, -1, 1)
    got("up_z3", up_3)
    up_4 = up_z(3)
    up_to_x(-3)
    up_to_x(3)
    down_pass(2, 0)
    up_pass_x(-1, 1)
    down_pass(1, 2)
    down_chunk(-1, 1)
    e_f = pass_tokens(r.ye, e_a)
    down_pass(2, -1, 1)
    got("up_z4", up_4)
    up_to_x(4)
    up_column(0)
    c_f = pass_tokens(r.yc, c_a)
    l_a = own_tokens(r.yl, 0)
    tok_l = own_tokens(r.yl, 1)
    up_pass_x(-2, 2)
    down_pass(3, 0)
    down_pass(2, 2)
    down_chunk(-2, 2)
    down_pass(3, -1, 1)
    up_pass_x(-3, 3, 4)
    got("up_x_rest", up_rest)
    up_column(-1)
    up_column(1)
    down_pass(3, 2)
    down_chunk(-3, 3)
    got("up_x_last", up_last)
    up_column(2)
    got("down_z4", down_far)
    down_chunk(4)
    got("tok_own", tok_own)
    for slot in (1, 2):
        turn(slot, r.ye, r.et)
        turn(slot, r.yc, r.ct)
    got("across", across_up, across_down)

    tile = 256
    many, last = pl.ds(0, 3 * tok), pl.ds(3 * tok, tok)

    @jax.named_scope("pre_earlier")
    def pre_earlier():
        for core in range(2):

            @pl.loop(0, ff // tile)
            def _(n):
                at = pl.multiple_of(n * tile, tile)
                w_up = wu[core, :, :, pl.ds(at, tile)].reshape(d, tile)
                w_down = wd[core, :, :, pl.ds(at, tile)].reshape(d, tile)
                relu = jnp.maximum(jnp.dot(r.ye[many], w_up, preferred_element_type=F32), 0.0)
                grad = jnp.dot(r.yc[many], w_down, preferred_element_type=F32)
                out = pl.ds(pl.multiple_of(core * ff + at, tile), tile)
                r.hid[many, out] = (relu * relu).astype(BF)
                r.pg[many, out] = (2.0 * relu * grad).astype(BF)

    @jax.named_scope("pre_last_e")
    def pre_last_e():
        for core in range(2):

            @pl.loop(0, ff // tile)
            def _(n):
                at = pl.multiple_of(n * tile, tile)
                w_up = wu[core, :, :, pl.ds(at, tile)].reshape(d, tile)
                relu = jnp.maximum(jnp.dot(r.ye[last], w_up, preferred_element_type=F32), 0.0)
                out = pl.ds(pl.multiple_of(core * ff + at, tile), tile)
                r.hid[last, out] = (relu * relu).astype(BF)
                r.rel[:, out] = relu

    @jax.named_scope("pre_last_c")
    def pre_last_c():
        for core in range(2):

            @pl.loop(0, ff // tile)
            def _(n):
                at = pl.multiple_of(n * tile, tile)
                w_down = wd[core, :, :, pl.ds(at, tile)].reshape(d, tile)
                grad = jnp.dot(r.yc[last], w_down, preferred_element_type=F32)
                out = pl.ds(pl.multiple_of(core * ff + at, tile), tile)
                r.pg[last, out] = (2.0 * r.rel[:, out] * grad).astype(BF)

    @jax.named_scope("pre_later")
    def pre_later(core):
        @pl.loop(0, ff // tile)
        def _(n):
            at = pl.multiple_of(n * tile, tile)
            w_up = wu[core, :, :, pl.ds(at, tile)].reshape(d, tile)
            relu = jnp.maximum(jnp.dot(r.yl[...], w_up, preferred_element_type=F32), 0.0)
            out = pl.ds(pl.multiple_of(core * ff + at, tile), tile)
            r.hid[:, out] = (relu * relu).astype(BF)

    pre_earlier()
    got("tok_last_e", e_f)
    turn(3, r.ye, r.et)
    pre_last_e()
    got("tok_last_c", c_f)
    turn(3, r.yc, r.ct)
    pre_last_c()

    def gradient(left, right, ks, core):
        rows_at = [left[pl.ds(pl.multiple_of(k * per_z, per_z), per_z)] for k in ks]
        both = jnp.concatenate(rows_at, axis=0)
        cols = right[:, core * ff : (core + 1) * ff]
        both = jnp.dot(both, cols, preferred_element_type=F32)
        return both[:per_z], both[per_z:]

    def farthest(j):
        return zi(4 + (1 - 2 * (j % 2)) * ((j + 1) // 2))

    @jax.named_scope("cross_grad")
    def cross_grad(left, right, out, into, order):
        copies = []
        for part in range(4):
            ks = order(2 * part), order(2 * part + 1)
            for k, total in zip(ks, gradient(left, right, ks, 1)):
                out[k] = total.astype(BF)
            copies.append(group())
            for k in ks:
                send(out.at[k], into.at[k], dev(dc=1), copies[-1])
        return copies

    @jax.named_scope("own_grad")
    def own_grad(left, right, other, out, order, part):
        ks = order(2 * part), order(2 * part + 1)
        for k, total in zip(ks, gradient(left, right, ks, 0)):
            out[k] = (total + other[k].astype(F32)).astype(BF)

    su, sd = r.su, r.sd

    def z_sum(name, acc, plus, minus, size):
        steps = {(s, first): group() for s in range(3) for first in (True, False)}
        steps[3, True] = steps[3, False] = end = group()

        def ways(s, first):
            for k, buf, step in ((zi(4 - s), plus, 1), (zi(s - 4), minus, -1)):
                yield k, buf, step, pl.ds(0 if first == (step == 1) else size, size)

        def start(s, first):
            for k, buf, step, part in ways(s, first):
                send(acc.at[k, part], buf.at[s, part], dev(dz=step), steps[s, first])

        def hop(s, first):
            got(f"{name}{s}", steps[s - 1, first])
            for k, buf, step, part in ways(s, first):
                total = acc[k, part].astype(F32) + buf[s - 1, part].astype(F32)
                acc[k, part] = total.astype(BF)
            start(s, first)

        def finish():
            got(f"{name}4", end)
            return acc[z].astype(F32) + plus[3].astype(F32) + minus[3].astype(F32)

        return start, hop, finish

    z_send, hop, z_end = z_sum("hop", sd, r.ra, r.rb, hz)
    uz_send, uz_hop, uz_end = z_sum("uz", r.tu, r.ua, r.ub, rows // 2)

    @jax.named_scope("back")
    def back(left, weight, out, part):
        @pl.loop(0, NZ // 2)
        def _(k):
            for core in range(2):
                w = weight[core, pl.ds(2 * k, 2)].reshape(2 * per_z, ff)
                acc = dot_tt(left[part, core * ff : (core + 1) * ff], w)
                total = acc if core == 0 else total + acc
            at = pl.ds(pl.multiple_of(k * 2 * per_z, per_z), 2 * per_z)
            out[part, at] = total.astype(BF)

    def start_sum(p, s):
        g = group()
        send(p.at[rows_of(3, 0)], s.at[0], dev(dy=1), g)
        send(p.at[rows_of(3, 1)], s.at[1], dev(dy=-1), g)
        return g

    def more_sum(p, m):
        g0, g1 = group(), group()
        send(p.at[rows_of(2, 1)], m.at[0, pl.ds(half, half)], dev(dy=1), g1)
        send(p.at[rows_of(1, 0)], m.at[1, pl.ds(0, half)], dev(dy=-1), g0)
        return g0, g1

    def pass_sum(p, s, m, g, groups):
        g0, g1 = groups
        got("sum_first", g)
        at = rows_of(2, 0)
        p[at] = (p[at].astype(F32) + s[0].astype(F32)).astype(BF)
        send(p.at[at], m.at[0, pl.ds(0, half)], dev(dy=1), g0)
        at = rows_of(1, 1)
        p[at] = (p[at].astype(F32) + s[1].astype(F32)).astype(BF)
        send(p.at[at], m.at[1, pl.ds(half, half)], dev(dy=-1), g1)

    def end_sum(p, m, groups, out):
        for h in range(2):
            got("sum_end", groups[h])
            own = rows_of(0, h)
            total = p[own].astype(F32) + m[0, own].astype(F32) + m[1, own].astype(F32)
            out[own] = total.astype(BF)

    back(r.pg, wu, r.pe, last)
    pass_tokens(r.yl, l_a, tok_l)
    first_e = start_sum(r.pe, r.se)
    c_down = cross_grad(r.ct, r.hid, r.god, r.xd, farthest)
    c_up = cross_grad(r.et, r.pg, r.gou, r.xu, lambda j: j)
    for part in range(4):
        got("c_down", c_down[part])
        own_grad(r.ct, r.hid, r.xd, sd, farthest, part)
        if part == 0:
            z_send(0, True)
        if part == 1:
            z_send(1, False)

    nh = NZ // 2
    lo, hi = pl.ds(0, nh), pl.ds(nh, nh)
    ux_a, ux_b, ur = group(), group(), group()
    for part in range(4):
        got("c_up", c_up[part])
        own_grad(r.et, r.pg, r.xu, su, lambda j: j, part)
        if part == 1:
            send(su.at[lo, xs(2)], r.sx.at[0], dev(dx=1), ux_a)
    send(su.at[hi, xs(2)], r.sx.at[1], dev(dx=-1), ux_b)
    send(su.at[hi, xs(1)], r.rx.at[0, hi], dev(dx=1), ur)
    send(su.at[lo, xs(-1)], r.rx.at[1, lo], dev(dx=-1), ur)

    back(r.pg, wu, r.pe, many)
    more_e = more_sum(r.pe, r.re)
    hop(1, True)
    hop(2, False)

    got("tok_l", tok_l)
    pre_later(0)
    got("ux", ux_a)
    su[lo, xs(1)] = (su[lo, xs(1)].astype(F32) + r.sx[0].astype(F32)).astype(BF)
    send(su.at[lo, xs(1)], r.rx.at[0, lo], dev(dx=1), ur)
    hop(2, True)
    pass_sum(r.pe, r.se, r.re, first_e, more_e)
    pre_later(1)
    got("ux", ux_b)
    su[hi, xs(-1)] = (su[hi, xs(-1)].astype(F32) + r.sx[1].astype(F32)).astype(BF)
    send(su.at[hi, xs(-1)], r.rx.at[1, hi], dev(dx=-1), ur)
    hop(3, False)
    back(r.hid, wd, r.po, pl.ds(0, 4 * tok))
    first_o = start_sum(r.po, r.so)
    more_o = more_sum(r.po, r.ro)
    hop(3, True)

    down_sum = z_end()
    td = r.td
    td[...] = down_sum.astype(BF).reshape(NX, rows, ff)
    q0, q1 = pl.ds(0, rows // 2), pl.ds(rows // 2, rows // 2)
    dx1, dx2 = group(), group()
    send(td.at[xi(2), q0], r.xa.at[0, q0], dev(dx=1), dx1)
    send(td.at[xi(2), q1], r.xb.at[0, q1], dev(dx=-1), dx1)

    got("ur", ur)
    tu = r.tu
    tu[...] = (
        su[:, xs(0)].astype(F32) + r.rx[0].astype(F32) + r.rx[1].astype(F32)
    ).astype(BF)
    uz_send(0, True)
    uz_send(1, False)

    def add_on(acc, k, buf, s, part):
        acc[k, part] = (acc[k, part].astype(F32) + buf[s, part].astype(F32)).astype(BF)

    got("dx1", dx1)
    add_on(td, xi(1), r.xa, 0, q0)
    send(td.at[xi(1)], r.xa.at[1], dev(dx=1), dx2)
    add_on(td, xi(-1), r.xb, 0, q1)
    send(td.at[xi(-1)], r.xb.at[1], dev(dx=-1), dx2)
    uz_hop(1, True)
    uz_hop(2, False)
    totals()
    uz_hop(2, True)
    pass_sum(r.po, r.so, r.ro, first_o, more_o)
    uz_hop(3, False)
    got("dx2", dx2)
    total = td[x].astype(F32) + r.xa[1].astype(F32) + r.xb[1].astype(F32)
    o_down[...] = r.tot_d[...] + total * factor
    uz_hop(3, True)
    end_sum(r.pe, r.re, more_e, o_earlier)
    o_up[...] = r.tot_u[...] + uz_end() * factor
    settle()
    end_sum(r.po, r.ro, more_o, o_later)
    assert len(leaving) == N_SENT and len(arriving) == N_GOT, (len(leaving), len(arriving))


def body(later_rows, earlier_rows, cotangent, up_weight, down_weight, up_total, down_total):
    given = later_rows, earlier_rows, cotangent, up_weight, down_weight, up_total, down_total
    tok, d = later_rows.shape
    rows, ff = up_weight.shape
    total_rows = tok * lax.axis_size("fs") * lax.axis_size("tp")
    factor = 1.0 / math.sqrt(total_rows)
    scratch = scratch_of(tok, d, ff, rows)

    def run(*refs):
        kernel(list(scratch), factor, *refs)

    shapes = (
        jax.ShapeDtypeStruct((tok, d), BF),
        jax.ShapeDtypeStruct((tok, d), BF),
        jax.ShapeDtypeStruct((rows, ff), F32),
        jax.ShapeDtypeStruct((rows, ff), F32),
    )
    results = pl.pallas_call(
        run,
        out_shape=shapes,
        in_specs=[pl.BlockSpec(memory_space=pltpu.HBM)] * 7,
        out_specs=(pl.BlockSpec(memory_space=pltpu.VMEM),) * 4,
        scratch_shapes=list(scratch.values()),
        compiler_params=pltpu.CompilerParams(
            collective_id=0, has_side_effects=True, vmem_limit_bytes=50 * 2**20
        ),
        name="ffn_step",
    )(*(pltpu.with_memory_space_constraint(a, pltpu.HBM) for a in given))
    return pl.pallas_call(
        store,
        out_shape=shapes,
        in_specs=[pl.BlockSpec(memory_space=pltpu.VMEM)] * 4,
        out_specs=(pl.BlockSpec(memory_space=pl.ANY),) * 4,
        scratch_shapes=[pltpu.SemaphoreType.DMA((4,))],
        compiler_params=pltpu.CompilerParams(vmem_limit_bytes=4 * 2**20),
        name="ffn_store",
    )(*results)


def store(*refs):
    copies = [pltpu.make_async_copy(refs[i], refs[4 + i], refs[8].at[i]) for i in range(4)]
    for copy in copies:
        copy.start()
    for copy in copies:
        copy.wait()


def solution(mesh):
    tokens = P(("fs", "tp"), None)
    weight = P("fs", "tp")
    return jax.shard_map(
        body,
        mesh=mesh,
        in_specs=(tokens, tokens, tokens, weight, weight, weight, weight),
        out_specs=(tokens, tokens, weight, weight),
        check_vma=False,
    )
```

```python
import math
from types import SimpleNamespace

import jax
import jax.numpy as jnp
from jax import lax
from jax.experimental import pallas as pl
from jax.experimental.pallas import tpu as pltpu
from jax.sharding import PartitionSpec as P

NZ, NX, NY = 8, 4, 4
BF = jnp.bfloat16
F32 = jnp.float32
N_SENT = 13
N_GOT = 72


def scratch_of(tok, d, ff, rows):
    per_z = NX * rows
    vm = pltpu.VMEM
    return dict(
        ye=vm((4 * tok, d), BF),
        yc=vm((4 * tok, d), BF),
        yl=vm((4 * tok, d), BF),
        wu=vm((2, NZ, per_z, ff), BF),
        wd=vm((2, NZ, per_z, ff), BF),
        hid=vm((4 * tok, 2 * ff), BF),
        rel=vm((tok, 2 * ff), F32),
        pg=vm((4 * tok, 2 * ff), BF),
        pe=vm((4 * tok, d), BF),
        po=vm((4 * tok, d), BF),
        se=vm((2, tok // 2, d), BF),
        so=vm((2, tok // 2, d), BF),
        re=vm((2, tok, d), BF),
        ro=vm((2, tok, d), BF),
        gou=vm((NZ, per_z, ff), BF),
        god=vm((NZ, per_z, ff), BF),
        xu=vm((NZ, per_z, ff), BF),
        xd=vm((NZ, per_z, ff), BF),
        su=vm((NZ, per_z, ff), BF),
        sd=vm((NZ, per_z, ff), BF),
        sx=vm((NZ // 2, 2, rows, ff), BF),
        rx=vm((2, NZ, rows, ff), BF),
        tu=vm((NZ, rows, ff), BF),
        ua=vm((4, rows, ff), BF),
        ub=vm((4, rows, ff), BF),
        ra=vm((4, per_z, ff), BF),
        rb=vm((4, per_z, ff), BF),
        td=vm((NX, rows, ff), BF),
        xa=vm((2, rows, ff), BF),
        xb=vm((2, rows, ff), BF),
        et=vm((d, 4 * tok), BF),
        ct=vm((d, 4 * tok), BF),
        tot_u=vm((rows, ff), F32),
        tot_d=vm((rows, ff), F32),
        send=pltpu.SemaphoreType.DMA((N_SENT,)),
        recv=pltpu.SemaphoreType.DMA((N_GOT,)),
        told=pltpu.SemaphoreType.REGULAR,
        local=pltpu.SemaphoreType.DMA((2,)),
    )


def dot_tt(a, b):
    return lax.dot_general(a, b, (((1,), (1,)), ((), ())), preferred_element_type=F32)


def kernel(names, factor, *refs):
    later, earlier, cot, up, down, up_total, down_total = refs[:7]
    o_later, o_earlier, o_up, o_down = refs[7:11]
    r = SimpleNamespace(**dict(zip(names, refs[11:])))
    tok, d = later.shape
    rows, ff = up.shape
    half = tok // 2
    per_z = NX * rows
    hz = per_z // 2

    f, t = lax.axis_index("fs"), lax.axis_index("tp")
    z, x = f // NX, f % NX
    y, c = t // 2, t % 2

    def zi(k):
        return (z + k + NZ) % NZ

    def xi(k):
        return (x + k + NX) % NX

    def dev(dz=0, dx=0, dy=0, dc=0):
        fs = zi(dz) * NX + xi(dx)
        tp = ((y + dy + NY) % NY) * 2 + (c + dc + 2) % 2
        return {"fs": fs, "tp": tp}

    row_bytes = d * 2
    limit = r.ye.shape[0] * row_bytes
    leaving, arriving = [], []

    def group():
        g = SimpleNamespace(at=len(arriving), bytes=0)
        arriving.append(g)
        return g

    def wait(sem, g):
        ref = r.ye.at[pl.ds(0, g.bytes // row_bytes)]
        pltpu.make_async_copy(ref, ref, sem).wait()

    def send(src, dst, to, g=None):
        size = math.prod(src.shape) * 2
        g = group() if g is None else g
        g.bytes += size
        if not leaving or leaving[-1].done or leaving[-1].bytes + size > limit:
            leaving.append(SimpleNamespace(bytes=0, done=False))
        leaving[-1].bytes += size
        pltpu.make_async_remote_copy(
            src_ref=src,
            dst_ref=dst,
            send_sem=r.send.at[len(leaving) - 1],
            recv_sem=r.recv.at[g.at],
            device_id=to,
            device_id_type=pl.DeviceIdType.MESH,
        ).start()
        return g

    @jax.named_scope("sent")
    def settle():
        for i, g in enumerate(leaving):
            if not g.done:
                wait(r.send.at[i], g)
                g.done = True

    def got(name, *groups):
        with jax.named_scope(name):
            for g in {g.at: g for g in groups}.values():
                wait(r.recv.at[g.at], g)

    def fetch(i, *pairs):
        g = SimpleNamespace(bytes=0)
        for src, dst in pairs:
            pltpu.make_async_copy(src, dst, r.local.at[i]).start()
            g.bytes += math.prod(src.shape) * src.dtype.itemsize
        return lambda: wait(r.local.at[i], g)

    def xs(k):
        return pl.ds(pl.multiple_of(xi(k) * rows, rows), rows)

    inputs = fetch(
        0,
        (earlier, r.ye.at[pl.ds(0, tok)]),
        (up, r.wu.at[0, z, xs(0)]),
        (down, r.wd.at[0, z, xs(0)]),
        (cot, r.yc.at[pl.ds(0, tok)]),
        (later, r.yl.at[pl.ds(0, tok)]),
    )
    totals = fetch(1, (up_total, r.tot_u), (down_total, r.tot_d))

    barrier = pltpu.get_barrier_semaphore()

    def enter(**to):
        pl.semaphore_signal(
            barrier, inc=1, device_id=dev(**to), device_id_type=pl.DeviceIdType.MESH
        )

    def tell():
        pl.semaphore_signal(
            r.told, inc=1, device_id=dev(dc=1), device_id_type=pl.DeviceIdType.MESH
        )

    for step in (1, -1):
        enter(dy=step, dc=-c)
        enter(dx=step, dc=1 - c)
        enter(dz=step, dc=1 - c)
    enter(dc=1)

    with jax.named_scope("barrier"):

        @pl.when(c == 0)
        def _():
            pl.semaphore_wait(barrier, 5)
            tell()

        @pl.when(c == 1)
        def _():
            pl.semaphore_wait(r.told, 1)

        inputs()

    def enter_xz():
        with jax.named_scope("barrier_xz"):

            @pl.when(c == 1)
            def _():
                pl.semaphore_wait(barrier, 9)
                tell()

            @pl.when(c == 0)
            def _():
                pl.semaphore_wait(r.told, 1)

    def rows_of(slot, h):
        return pl.ds(slot * tok + h * half, half)

    def own_tokens(buf, h, g=None):
        g = g or group()
        send(buf.at[rows_of(0, h)], buf.at[rows_of(1, h)], dev(dy=1), g)
        send(buf.at[rows_of(0, 1 - h)], buf.at[rows_of(2, 1 - h)], dev(dy=-1), g)
        return g

    def pass_tokens(buf, first, g=None):
        g = g or group()
        got("tok_first", first)
        send(buf.at[rows_of(1, 0)], buf.at[rows_of(3, 0)], dev(dy=1), g)
        send(buf.at[rows_of(2, 1)], buf.at[rows_of(3, 1)], dev(dy=-1), g)
        return g

    wu, wd = r.wu, r.wd

    def up_block(dz, dx):
        return wu.at[0, zi(dz), xs(dx)]

    def up_z(k):
        g = group()
        for step in (1, -1):
            ref = up_block(-k * step, 0)
            if k == 3:
                ref = ref.at[pl.ds(0 if step == 1 else rows // 2, rows // 2)]
            send(ref, ref, dev(dz=step), g)
        return g

    up_first, up_rest, up_last = [group() for _ in range(4)], group(), group()

    def up_to_x(dz):
        ref = up_block(dz, 0)
        first = up_first[min(abs(dz), 3)]
        plus, minus = (first, up_rest) if 0 <= dz <= 3 else (up_rest, first)
        send(ref, ref, dev(dx=1), plus)
        send(ref, ref, dev(dx=-1), minus)

    def up_pass_x(*dzs):
        got("up_x", up_first[min(abs(dzs[0]), 3)])
        for dz in dzs:
            step = 1 if 0 <= dz <= 3 else -1
            ref = up_block(dz, -step)
            send(ref, ref, dev(dx=step), up_last)

    across_up, across_down = group(), group()

    def up_column(dx):
        src = wu.at[0, :, xs(dx)]
        send(src, wu.at[1, :, xs(dx)], dev(dc=1), across_up)

    def down_block(dz, dx):
        return wd.at[0, zi(dz), xs(dx)]

    down_far = group()
    down_at = {}

    def down_z(k, *dxs):
        for dx in dxs:
            g = down_far if k == 3 else group()
            down_at[k + 1, dx] = g
            if k < 3 or dx in (0, -1):
                ref = down_block(-k, dx)
                send(ref, ref, dev(dz=1), g)
            if k < 3 or dx in (1, 2):
                ref = down_block(k, dx)
                send(ref, ref, dev(dz=-1), g)

    def down_pass(k, *dxs):
        for dx in dxs:
            got(f"down_z{k}", down_at[k, dx])
            down_z(k, dx)

    def down_chunk(*dzs):
        for dz in dzs:
            send(wd.at[0, zi(dz)], wd.at[1, zi(dz)], dev(dc=1), across_down)

    @jax.named_scope("turn")
    def turn(slot, src, dst):
        @pl.loop(0, NZ)
        def _(k):
            cols = pl.ds(pl.multiple_of(k * per_z, per_z), per_z)
            dst[cols, pl.ds(slot * tok, tok)] = src[pl.ds(slot * tok, tok), cols].T

    e_a = own_tokens(r.ye, 0)
    c_a = own_tokens(r.yc, 0)
    tok_own = own_tokens(r.ye, 1)
    own_tokens(r.yc, 1, tok_own)
    enter_xz()
    own_down = down_block(0, 0)
    down_x1, down_x2 = group(), group()
    send(own_down, own_down, dev(dx=1), down_x1)
    send(own_down, own_down, dev(dx=-1), down_x1)
    up_to_x(0)
    up_1 = up_z(0)
    down_z(0, 0)
    turn(0, r.ye, r.et)

    got("up_z1", up_1)
    up_2 = up_z(1)
    got("down_x", down_x1)
    part = down_block(0, -1).at[pl.ds(0, rows // 2)]
    send(part, part, dev(dx=1), down_x2)
    part = down_block(0, 1).at[pl.ds(rows // 2, rows // 2)]
    send(part, part, dev(dx=-1), down_x2)
    down_z(0, -1, 1)
    up_to_x(-1)
    up_to_x(1)
    down_pass(1, 0)
    turn(0, r.yc, r.ct)
    got("up_z2", up_2)
    up_3 = up_z(2)
    up_to_x(-2)
    up_to_x(2)
    got("down_x2", down_x2)
    down_z(0, 2)
    down_chunk(0)
    up_pass_x(0)
    down_pass(1, -1, 1)
    got("up_z3", up_3)
    up_4 = up_z(3)
    up_to_x(-3)
    up_to_x(3)
    down_pass(2, 0)
    up_pass_x(-1, 1)
    down_pass(1, 2)
    down_chunk(-1, 1)
    e_f = pass_tokens(r.ye, e_a)
    down_pass(2, -1, 1)
    got("up_z4", up_4)
    up_to_x(4)
    up_column(0)
    c_f = pass_tokens(r.yc, c_a)
    l_a = own_tokens(r.yl, 0)
    tok_l = own_tokens(r.yl, 1)
    up_pass_x(-2, 2)
    down_pass(3, 0)
    down_pass(2, 2)
    down_chunk(-2, 2)
    down_pass(3, -1, 1)
    up_pass_x(-3, 3, 4)
    got("up_x_rest", up_rest)
    up_column(-1)
    up_column(1)
    down_pass(3, 2)
    down_chunk(-3, 3)
    got("up_x_last", up_last)
    up_column(2)
    got("down_z4", down_far)
    down_chunk(4)
    got("tok_own", tok_own)
    for slot in (1, 2):
        turn(slot, r.ye, r.et)
        turn(slot, r.yc, r.ct)
    got("across", across_up, across_down)

    tile = 256
    many, last = pl.ds(0, 3 * tok), pl.ds(3 * tok, tok)

    @jax.named_scope("pre_earlier")
    def pre_earlier():
        for core in range(2):

            @pl.loop(0, ff // tile)
            def _(n):
                at = pl.multiple_of(n * tile, tile)
                w_up = wu[core, :, :, pl.ds(at, tile)].reshape(d, tile)
                w_down = wd[core, :, :, pl.ds(at, tile)].reshape(d, tile)
                relu = jnp.maximum(jnp.dot(r.ye[many], w_up, preferred_element_type=F32), 0.0)
                grad = jnp.dot(r.yc[many], w_down, preferred_element_type=F32)
                out = pl.ds(pl.multiple_of(core * ff + at, tile), tile)
                r.hid[many, out] = (relu * relu).astype(BF)
                r.pg[many, out] = (2.0 * relu * grad).astype(BF)

    @jax.named_scope("pre_last_e")
    def pre_last_e():
        for core in range(2):

            @pl.loop(0, ff // tile)
            def _(n):
                at = pl.multiple_of(n * tile, tile)
                w_up = wu[core, :, :, pl.ds(at, tile)].reshape(d, tile)
                relu = jnp.maximum(jnp.dot(r.ye[last], w_up, preferred_element_type=F32), 0.0)
                out = pl.ds(pl.multiple_of(core * ff + at, tile), tile)
                r.hid[last, out] = (relu * relu).astype(BF)
                r.rel[:, out] = relu

    @jax.named_scope("pre_last_c")
    def pre_last_c():
        for core in range(2):

            @pl.loop(0, ff // tile)
            def _(n):
                at = pl.multiple_of(n * tile, tile)
                w_down = wd[core, :, :, pl.ds(at, tile)].reshape(d, tile)
                grad = jnp.dot(r.yc[last], w_down, preferred_element_type=F32)
                out = pl.ds(pl.multiple_of(core * ff + at, tile), tile)
                r.pg[last, out] = (2.0 * r.rel[:, out] * grad).astype(BF)

    @jax.named_scope("pre_later")
    def pre_later(core):
        @pl.loop(0, ff // tile)
        def _(n):
            at = pl.multiple_of(n * tile, tile)
            w_up = wu[core, :, :, pl.ds(at, tile)].reshape(d, tile)
            relu = jnp.maximum(jnp.dot(r.yl[...], w_up, preferred_element_type=F32), 0.0)
            out = pl.ds(pl.multiple_of(core * ff + at, tile), tile)
            r.hid[:, out] = (relu * relu).astype(BF)

    pre_earlier()
    got("tok_last_e", e_f)
    turn(3, r.ye, r.et)
    pre_last_e()
    got("tok_last_c", c_f)
    turn(3, r.yc, r.ct)
    pre_last_c()

    def gradient(left, right, ks, core):
        rows_at = [left[pl.ds(pl.multiple_of(k * per_z, per_z), per_z)] for k in ks]
        both = jnp.concatenate(rows_at, axis=0)
        cols = right[:, core * ff : (core + 1) * ff]
        both = jnp.dot(both, cols, preferred_element_type=F32)
        return both[:per_z], both[per_z:]

    def farthest(j):
        return zi(4 + (1 - 2 * (j % 2)) * ((j + 1) // 2))

    @jax.named_scope("cross_grad")
    def cross_grad(left, right, out, into, order):
        copies = []
        for part in range(4):
            ks = order(2 * part), order(2 * part + 1)
            for k, total in zip(ks, gradient(left, right, ks, 1)):
                out[k] = total.astype(BF)
            copies.append(group())
            for k in ks:
                send(out.at[k], into.at[k], dev(dc=1), copies[-1])
        return copies

    @jax.named_scope("own_grad")
    def own_grad(left, right, other, out, order, part):
        ks = order(2 * part), order(2 * part + 1)
        for k, total in zip(ks, gradient(left, right, ks, 0)):
            out[k] = (total + other[k].astype(F32)).astype(BF)

    su, sd = r.su, r.sd

    def z_sum(name, acc, plus, minus, size):
        steps = {(s, first): group() for s in range(3) for first in (True, False)}
        steps[3, True] = steps[3, False] = end = group()

        def ways(s, first):
            for k, buf, step in ((zi(4 - s), plus, 1), (zi(s - 4), minus, -1)):
                yield k, buf, step, pl.ds(0 if first == (step == 1) else size, size)

        def start(s, first):
            for k, buf, step, part in ways(s, first):
                send(acc.at[k, part], buf.at[s, part], dev(dz=step), steps[s, first])

        def hop(s, first):
            got(f"{name}{s}", steps[s - 1, first])
            for k, buf, step, part in ways(s, first):
                total = acc[k, part].astype(F32) + buf[s - 1, part].astype(F32)
                acc[k, part] = total.astype(BF)
            start(s, first)

        def finish():
            got(f"{name}4", end)
            return acc[z].astype(F32) + plus[3].astype(F32) + minus[3].astype(F32)

        return start, hop, finish

    z_send, hop, z_end = z_sum("hop", sd, r.ra, r.rb, hz)
    uz_send, uz_hop, uz_end = z_sum("uz", r.tu, r.ua, r.ub, rows // 2)

    @jax.named_scope("back")
    def back(left, weight, out, part, begin=0, end=NZ // 2):
        @pl.loop(begin, end)
        def _(k):
            for core in range(2):
                w = weight[core, pl.ds(2 * k, 2)].reshape(2 * per_z, ff)
                acc = dot_tt(left[part, core * ff : (core + 1) * ff], w)
                total = acc if core == 0 else total + acc
            at = pl.ds(pl.multiple_of(k * 2 * per_z, per_z), 2 * per_z)
            out[part, at] = total.astype(BF)

    def start_sum(p, s):
        g = group()
        send(p.at[rows_of(3, 0)], s.at[0], dev(dy=1), g)
        send(p.at[rows_of(3, 1)], s.at[1], dev(dy=-1), g)
        return g

    def more_sum(p, m):
        g0, g1 = group(), group()
        send(p.at[rows_of(2, 1)], m.at[0, pl.ds(half, half)], dev(dy=1), g1)
        send(p.at[rows_of(1, 0)], m.at[1, pl.ds(0, half)], dev(dy=-1), g0)
        return g0, g1

    def pass_sum(p, s, m, g, groups):
        g0, g1 = groups
        got("sum_first", g)
        at = rows_of(2, 0)
        p[at] = (p[at].astype(F32) + s[0].astype(F32)).astype(BF)
        send(p.at[at], m.at[0, pl.ds(0, half)], dev(dy=1), g0)
        at = rows_of(1, 1)
        p[at] = (p[at].astype(F32) + s[1].astype(F32)).astype(BF)
        send(p.at[at], m.at[1, pl.ds(half, half)], dev(dy=-1), g1)

    def end_sum(p, m, groups, out):
        for h in range(2):
            got("sum_end", groups[h])
            own = rows_of(0, h)
            total = p[own].astype(F32) + m[0, own].astype(F32) + m[1, own].astype(F32)
            out[own] = total.astype(BF)

    back(r.pg, wu, r.pe, last, end=NZ // 4)
    pass_tokens(r.yl, l_a, tok_l)
    back(r.pg, wu, r.pe, last, begin=NZ // 4)
    first_e = start_sum(r.pe, r.se)
    c_down = cross_grad(r.ct, r.hid, r.god, r.xd, farthest)
    pairs = ((4, 0), (3, 5), (2, 6), (1, 7))
    c_up = cross_grad(r.et, r.pg, r.gou, r.xu, lambda j: zi(pairs[j // 2][j % 2]))
    for part in range(4):
        got("c_down", c_down[part])
        own_grad(r.ct, r.hid, r.xd, sd, farthest, part)
        if part == 0:
            z_send(0, True)
        if part == 1:
            z_send(1, False)

    x_first, x_last = [group() for _ in pairs], [group() for _ in pairs]

    def x_send(p):
        for i, step in ((0, 1), (1, -1)):
            k = zi(pairs[p][i])
            send(su.at[k, xs(2)], r.sx.at[p, i], dev(dx=step), x_first[p])

    def x_hop(p):
        got(f"x_hop{p}", x_first[p])
        for i, step in ((0, 1), (1, -1)):
            k = zi(pairs[p][i])
            total = su[k, xs(step)].astype(F32) + r.sx[p, i].astype(F32)
            su[k, xs(step)] = total.astype(BF)
            send(su.at[k, xs(step)], r.rx.at[i, 2 * p + i], dev(dx=step), x_last[p])
        for i, step in ((0, 1), (1, -1)):
            k = zi(pairs[p][1 - i])
            send(su.at[k, xs(step)], r.rx.at[i, 2 * p + 1 - i], dev(dx=step), x_last[p])

    def x_end(p):
        got(f"x_end{p}", x_last[p])
        for i in range(2):
            k, j = zi(pairs[p][i]), 2 * p + i
            total = su[k, xs(0)].astype(F32) + r.rx[0, j].astype(F32) + r.rx[1, j].astype(F32)
            r.tu[k] = total.astype(BF)

    for part in range(4):
        got("c_up", c_up[part])
        own_grad(r.et, r.pg, r.xu, su, lambda j: zi(pairs[j // 2][j % 2]), part)
        x_send(part)

    back(r.pg, wu, r.pe, many)
    more_e = more_sum(r.pe, r.re)
    hop(1, True)
    x_hop(0)
    hop(2, False)

    got("tok_l", tok_l)
    pre_later(0)
    x_hop(1)
    x_hop(2)
    x_hop(3)
    pass_sum(r.pe, r.se, r.re, first_e, more_e)
    pre_later(1)
    hop(2, True)
    back(r.hid, wd, r.po, pl.ds(0, 4 * tok))
    first_o = start_sum(r.po, r.so)
    more_o = more_sum(r.po, r.ro)
    x_end(0)
    uz_send(0, True)
    hop(3, False)
    x_end(1)
    uz_send(1, False)
    uz_hop(1, True)
    hop(3, True)
    x_end(2)
    uz_hop(2, False)
    x_end(3)
    uz_hop(2, True)
    uz_hop(3, False)

    down_sum = z_end()
    td = r.td
    td[...] = down_sum.astype(BF).reshape(NX, rows, ff)
    q0, q1 = pl.ds(0, rows // 2), pl.ds(rows // 2, rows // 2)
    dx1, dx2 = group(), group()
    send(td.at[xi(2), q0], r.xa.at[0, q0], dev(dx=1), dx1)
    send(td.at[xi(2), q1], r.xb.at[0, q1], dev(dx=-1), dx1)
    uz_hop(3, True)

    def add_on(acc, k, buf, s, part):
        acc[k, part] = (acc[k, part].astype(F32) + buf[s, part].astype(F32)).astype(BF)

    pass_sum(r.po, r.so, r.ro, first_o, more_o)
    got("dx1", dx1)
    add_on(td, xi(1), r.xa, 0, q0)
    send(td.at[xi(1)], r.xa.at[1], dev(dx=1), dx2)
    add_on(td, xi(-1), r.xb, 0, q1)
    send(td.at[xi(-1)], r.xb.at[1], dev(dx=-1), dx2)
    totals()
    o_up[...] = r.tot_u[...] + uz_end() * factor
    got("dx2", dx2)
    total = td[x].astype(F32) + r.xa[1].astype(F32) + r.xb[1].astype(F32)
    o_down[...] = r.tot_d[...] + total * factor
    end_sum(r.pe, r.re, more_e, o_earlier)
    settle()
    end_sum(r.po, r.ro, more_o, o_later)
    assert len(leaving) == N_SENT and len(arriving) == N_GOT, (len(leaving), len(arriving))


def body(later_rows, earlier_rows, cotangent, up_weight, down_weight, up_total, down_total):
    given = later_rows, earlier_rows, cotangent, up_weight, down_weight, up_total, down_total
    tok, d = later_rows.shape
    rows, ff = up_weight.shape
    total_rows = tok * lax.axis_size("fs") * lax.axis_size("tp")
    factor = 1.0 / math.sqrt(total_rows)
    scratch = scratch_of(tok, d, ff, rows)

    def run(*refs):
        kernel(list(scratch), factor, *refs)

    shapes = (
        jax.ShapeDtypeStruct((tok, d), BF),
        jax.ShapeDtypeStruct((tok, d), BF),
        jax.ShapeDtypeStruct((rows, ff), F32),
        jax.ShapeDtypeStruct((rows, ff), F32),
    )
    results = pl.pallas_call(
        run,
        out_shape=shapes,
        in_specs=[pl.BlockSpec(memory_space=pltpu.HBM)] * 7,
        out_specs=(pl.BlockSpec(memory_space=pltpu.VMEM),) * 4,
        scratch_shapes=list(scratch.values()),
        compiler_params=pltpu.CompilerParams(
            collective_id=0, has_side_effects=True, vmem_limit_bytes=50 * 2**20
        ),
        name="ffn_step",
    )(*(pltpu.with_memory_space_constraint(a, pltpu.HBM) for a in given))
    return pl.pallas_call(
        store,
        out_shape=shapes,
        in_specs=[pl.BlockSpec(memory_space=pltpu.VMEM)] * 4,
        out_specs=(pl.BlockSpec(memory_space=pl.ANY),) * 4,
        scratch_shapes=[pltpu.SemaphoreType.DMA((4,))],
        compiler_params=pltpu.CompilerParams(vmem_limit_bytes=4 * 2**20),
        name="ffn_store",
    )(*results)


def store(*refs):
    copies = [pltpu.make_async_copy(refs[i], refs[4 + i], refs[8].at[i]) for i in range(4)]
    for copy in copies:
        copy.start()
    for copy in copies:
        copy.wait()


def solution(mesh):
    tokens = P(("fs", "tp"), None)
    weight = P("fs", "tp")
    return jax.shard_map(
        body,
        mesh=mesh,
        in_specs=(tokens, tokens, tokens, weight, weight, weight, weight),
        out_specs=(tokens, tokens, weight, weight),
        check_vma=False,
    )
```

```python
import math
from types import SimpleNamespace

import jax
import jax.numpy as jnp
from jax import lax
from jax.experimental import pallas as pl
from jax.experimental.pallas import tpu as pltpu
from jax.sharding import PartitionSpec as P

NZ, NX, NY = 8, 4, 4
BF = jnp.bfloat16
F32 = jnp.float32
N_SENT = 13
N_GOT = 72


def scratch_of(tok, d, ff, rows):
    per_z = NX * rows
    vm = pltpu.VMEM
    return dict(
        ye=vm((4 * tok, d), BF),
        yc=vm((4 * tok, d), BF),
        yl=vm((4 * tok, d), BF),
        wu=vm((2, NZ, per_z, ff), BF),
        wd=vm((2, NZ, per_z, ff), BF),
        hid=vm((4 * tok, 2 * ff), BF),
        rel=vm((tok, 2 * ff), F32),
        pg=vm((4 * tok, 2 * ff), BF),
        pe=vm((4 * tok, d), BF),
        po=vm((4 * tok, d), BF),
        se=vm((2, tok // 2, d), BF),
        so=vm((2, tok // 2, d), BF),
        re=vm((2, tok, d), BF),
        ro=vm((2, tok, d), BF),
        gou=vm((NZ, per_z, ff), BF),
        god=vm((NZ, per_z, ff), BF),
        xu=vm((NZ, per_z, ff), BF),
        xd=vm((NZ, per_z, ff), BF),
        su=vm((NZ, per_z, ff), BF),
        sd=vm((NZ, per_z, ff), BF),
        sx=vm((NZ // 2, 2, rows, ff), BF),
        rx=vm((2, NZ, rows, ff), BF),
        tu=vm((NZ, rows, ff), BF),
        ua=vm((4, rows, ff), BF),
        ub=vm((4, rows, ff), BF),
        ra=vm((4, per_z, ff), BF),
        rb=vm((4, per_z, ff), BF),
        td=vm((NX, rows, ff), BF),
        xa=vm((2, rows, ff), BF),
        xb=vm((2, rows, ff), BF),
        et=vm((d, 4 * tok), BF),
        ct=vm((d, 4 * tok), BF),
        tot_u=vm((rows, ff), F32),
        tot_d=vm((rows, ff), F32),
        send=pltpu.SemaphoreType.DMA((N_SENT,)),
        recv=pltpu.SemaphoreType.DMA((N_GOT,)),
        told=pltpu.SemaphoreType.REGULAR,
        local=pltpu.SemaphoreType.DMA((4,)),
    )


def dot_tt(a, b):
    return lax.dot_general(a, b, (((1,), (1,)), ((), ())), preferred_element_type=F32)


def kernel(names, factor, *refs):
    later, earlier, cot, up, down, up_total, down_total = refs[:7]
    o_later, o_earlier, o_up, o_down = refs[7:11]
    r = SimpleNamespace(**dict(zip(names, refs[11:])))
    tok, d = later.shape
    rows, ff = up.shape
    half = tok // 2
    per_z = NX * rows
    hz = per_z // 2

    f, t = lax.axis_index("fs"), lax.axis_index("tp")
    z, x = f // NX, f % NX
    y, c = t // 2, t % 2

    def zi(k):
        return (z + k + NZ) % NZ

    def xi(k):
        return (x + k + NX) % NX

    def dev(dz=0, dx=0, dy=0, dc=0):
        fs = zi(dz) * NX + xi(dx)
        tp = ((y + dy + NY) % NY) * 2 + (c + dc + 2) % 2
        return {"fs": fs, "tp": tp}

    row_bytes = d * 2
    limit = r.ye.shape[0] * row_bytes
    leaving, arriving = [], []

    def group():
        g = SimpleNamespace(at=len(arriving), bytes=0)
        arriving.append(g)
        return g

    def wait(sem, g):
        ref = r.ye.at[pl.ds(0, g.bytes // row_bytes)]
        pltpu.make_async_copy(ref, ref, sem).wait()

    def send(src, dst, to, g=None):
        size = math.prod(src.shape) * 2
        g = group() if g is None else g
        g.bytes += size
        if not leaving or leaving[-1].done or leaving[-1].bytes + size > limit:
            leaving.append(SimpleNamespace(bytes=0, done=False))
        leaving[-1].bytes += size
        pltpu.make_async_remote_copy(
            src_ref=src,
            dst_ref=dst,
            send_sem=r.send.at[len(leaving) - 1],
            recv_sem=r.recv.at[g.at],
            device_id=to,
            device_id_type=pl.DeviceIdType.MESH,
        ).start()
        return g

    @jax.named_scope("sent")
    def settle():
        for i, g in enumerate(leaving):
            if not g.done:
                wait(r.send.at[i], g)
                g.done = True

    def got(name, *groups):
        with jax.named_scope(name):
            for g in {g.at: g for g in groups}.values():
                wait(r.recv.at[g.at], g)

    def fetch(i, *pairs):
        g = SimpleNamespace(bytes=0)
        for src, dst in pairs:
            pltpu.make_async_copy(src, dst, r.local.at[i]).start()
            g.bytes += math.prod(src.shape) * src.dtype.itemsize
        return lambda: wait(r.local.at[i], g)

    def xs(k):
        return pl.ds(pl.multiple_of(xi(k) * rows, rows), rows)

    barrier = pltpu.get_barrier_semaphore()

    def enter(**to):
        pl.semaphore_signal(
            barrier, inc=1, device_id=dev(**to), device_id_type=pl.DeviceIdType.MESH
        )

    def tell():
        pl.semaphore_signal(
            r.told, inc=1, device_id=dev(dc=1), device_id_type=pl.DeviceIdType.MESH
        )

    for step in (1, -1):
        enter(dy=step, dc=-c)
        enter(dx=step, dc=1 - c)
        enter(dz=step, dc=1 - c)
    enter(dc=1)

    first = fetch(0, (earlier, r.ye.at[pl.ds(0, tok)]))
    second = fetch(1, (cot, r.yc.at[pl.ds(0, tok)]))
    inputs = fetch(
        2,
        (up, r.wu.at[0, z, xs(0)]),
        (down, r.wd.at[0, z, xs(0)]),
        (later, r.yl.at[pl.ds(0, tok)]),
    )
    totals = fetch(3, (up_total, r.tot_u), (down_total, r.tot_d))

    with jax.named_scope("barrier"):

        @pl.when(c == 0)
        def _():
            pl.semaphore_wait(barrier, 5)
            tell()

        @pl.when(c == 1)
        def _():
            pl.semaphore_wait(r.told, 1)

    def enter_xz():
        with jax.named_scope("barrier_xz"):

            @pl.when(c == 1)
            def _():
                pl.semaphore_wait(barrier, 9)
                tell()

            @pl.when(c == 0)
            def _():
                pl.semaphore_wait(r.told, 1)

    def rows_of(slot, h):
        return pl.ds(slot * tok + h * half, half)

    def own_tokens(buf, h, g=None):
        g = g or group()
        send(buf.at[rows_of(0, h)], buf.at[rows_of(1, h)], dev(dy=1), g)
        send(buf.at[rows_of(0, 1 - h)], buf.at[rows_of(2, 1 - h)], dev(dy=-1), g)
        return g

    def pass_tokens(buf, first, g=None):
        g = g or group()
        got("tok_first", first)
        send(buf.at[rows_of(1, 0)], buf.at[rows_of(3, 0)], dev(dy=1), g)
        send(buf.at[rows_of(2, 1)], buf.at[rows_of(3, 1)], dev(dy=-1), g)
        return g

    wu, wd = r.wu, r.wd

    def up_block(dz, dx):
        return wu.at[0, zi(dz), xs(dx)]

    def up_z(k):
        g = group()
        for step in (1, -1):
            ref = up_block(-k * step, 0)
            if k == 3:
                ref = ref.at[pl.ds(0 if step == 1 else rows // 2, rows // 2)]
            send(ref, ref, dev(dz=step), g)
        return g

    up_first, up_rest, up_last = [group() for _ in range(4)], group(), group()

    def up_to_x(dz):
        ref = up_block(dz, 0)
        first = up_first[min(abs(dz), 3)]
        plus, minus = (first, up_rest) if 0 <= dz <= 3 else (up_rest, first)
        send(ref, ref, dev(dx=1), plus)
        send(ref, ref, dev(dx=-1), minus)

    def up_pass_x(*dzs):
        got("up_x", up_first[min(abs(dzs[0]), 3)])
        for dz in dzs:
            step = 1 if 0 <= dz <= 3 else -1
            ref = up_block(dz, -step)
            send(ref, ref, dev(dx=step), up_last)

    across_up, across_down = group(), group()

    def up_column(dx):
        src = wu.at[0, :, xs(dx)]
        send(src, wu.at[1, :, xs(dx)], dev(dc=1), across_up)

    def down_block(dz, dx):
        return wd.at[0, zi(dz), xs(dx)]

    down_far = group()
    down_at = {}

    def down_z(k, *dxs):
        for dx in dxs:
            g = down_far if k == 3 else group()
            down_at[k + 1, dx] = g
            if k < 3 or dx in (0, -1):
                ref = down_block(-k, dx)
                send(ref, ref, dev(dz=1), g)
            if k < 3 or dx in (1, 2):
                ref = down_block(k, dx)
                send(ref, ref, dev(dz=-1), g)

    def down_pass(k, *dxs):
        for dx in dxs:
            got(f"down_z{k}", down_at[k, dx])
            down_z(k, dx)

    def down_chunk(*dzs):
        for dz in dzs:
            send(wd.at[0, zi(dz)], wd.at[1, zi(dz)], dev(dc=1), across_down)

    @jax.named_scope("turn")
    def turn(slot, src, dst):
        @pl.loop(0, NZ)
        def _(k):
            cols = pl.ds(pl.multiple_of(k * per_z, per_z), per_z)
            dst[cols, pl.ds(slot * tok, tok)] = src[pl.ds(slot * tok, tok), cols].T

    first()
    e_a = own_tokens(r.ye, 0)
    second()
    c_a = own_tokens(r.yc, 0)
    tok_own = own_tokens(r.ye, 1)
    own_tokens(r.yc, 1, tok_own)
    inputs()
    enter_xz()
    own_down = down_block(0, 0)
    down_x1, down_x2 = group(), group()
    send(own_down, own_down, dev(dx=1), down_x1)
    send(own_down, own_down, dev(dx=-1), down_x1)
    up_to_x(0)
    up_1 = up_z(0)
    down_z(0, 0)
    turn(0, r.ye, r.et)

    got("up_z1", up_1)
    up_2 = up_z(1)
    got("down_x", down_x1)
    part = down_block(0, -1).at[pl.ds(0, rows // 2)]
    send(part, part, dev(dx=1), down_x2)
    part = down_block(0, 1).at[pl.ds(rows // 2, rows // 2)]
    send(part, part, dev(dx=-1), down_x2)
    down_z(0, -1, 1)
    up_to_x(-1)
    up_to_x(1)
    down_pass(1, 0)
    turn(0, r.yc, r.ct)
    got("up_z2", up_2)
    up_3 = up_z(2)
    up_to_x(-2)
    up_to_x(2)
    got("down_x2", down_x2)
    down_z(0, 2)
    down_chunk(0)
    up_pass_x(0)
    down_pass(1, -1, 1)
    got("up_z3", up_3)
    up_4 = up_z(3)
    up_to_x(-3)
    up_to_x(3)
    down_pass(2, 0)
    up_pass_x(-1, 1)
    down_pass(1, 2)
    down_chunk(-1, 1)
    e_f = pass_tokens(r.ye, e_a)
    down_pass(2, -1, 1)
    got("up_z4", up_4)
    up_to_x(4)
    up_column(0)
    c_f = pass_tokens(r.yc, c_a)
    l_a = own_tokens(r.yl, 0)
    tok_l = own_tokens(r.yl, 1)
    up_pass_x(-2, 2)
    down_pass(3, 0)
    down_pass(2, 2)
    down_chunk(-2, 2)
    down_pass(3, -1, 1)
    up_pass_x(-3, 3, 4)
    got("up_x_rest", up_rest)
    up_column(-1)
    up_column(1)
    down_pass(3, 2)
    down_chunk(-3, 3)
    got("up_x_last", up_last)
    up_column(2)
    got("down_z4", down_far)
    down_chunk(4)
    got("tok_own", tok_own)
    for slot in (1, 2):
        turn(slot, r.ye, r.et)
        turn(slot, r.yc, r.ct)
    got("across", across_up, across_down)

    tile = 256
    many, last = pl.ds(0, 3 * tok), pl.ds(3 * tok, tok)

    @jax.named_scope("pre_earlier")
    def pre_earlier():
        for core in range(2):

            @pl.loop(0, ff // tile)
            def _(n):
                at = pl.multiple_of(n * tile, tile)
                w_up = wu[core, :, :, pl.ds(at, tile)].reshape(d, tile)
                w_down = wd[core, :, :, pl.ds(at, tile)].reshape(d, tile)
                relu = jnp.maximum(jnp.dot(r.ye[many], w_up, preferred_element_type=F32), 0.0)
                grad = jnp.dot(r.yc[many], w_down, preferred_element_type=F32)
                out = pl.ds(pl.multiple_of(core * ff + at, tile), tile)
                r.hid[many, out] = (relu * relu).astype(BF)
                r.pg[many, out] = (2.0 * relu * grad).astype(BF)

    @jax.named_scope("pre_last_e")
    def pre_last_e():
        for core in range(2):

            @pl.loop(0, ff // tile)
            def _(n):
                at = pl.multiple_of(n * tile, tile)
                w_up = wu[core, :, :, pl.ds(at, tile)].reshape(d, tile)
                relu = jnp.maximum(jnp.dot(r.ye[last], w_up, preferred_element_type=F32), 0.0)
                out = pl.ds(pl.multiple_of(core * ff + at, tile), tile)
                r.hid[last, out] = (relu * relu).astype(BF)
                r.rel[:, out] = relu

    @jax.named_scope("pre_last_c")
    def pre_last_c():
        for core in range(2):

            @pl.loop(0, ff // tile)
            def _(n):
                at = pl.multiple_of(n * tile, tile)
                w_down = wd[core, :, :, pl.ds(at, tile)].reshape(d, tile)
                grad = jnp.dot(r.yc[last], w_down, preferred_element_type=F32)
                out = pl.ds(pl.multiple_of(core * ff + at, tile), tile)
                r.pg[last, out] = (2.0 * r.rel[:, out] * grad).astype(BF)

    @jax.named_scope("pre_later")
    def pre_later(core):
        @pl.loop(0, ff // tile)
        def _(n):
            at = pl.multiple_of(n * tile, tile)
            w_up = wu[core, :, :, pl.ds(at, tile)].reshape(d, tile)
            relu = jnp.maximum(jnp.dot(r.yl[...], w_up, preferred_element_type=F32), 0.0)
            out = pl.ds(pl.multiple_of(core * ff + at, tile), tile)
            r.hid[:, out] = (relu * relu).astype(BF)

    pre_earlier()
    got("tok_last_e", e_f)
    turn(3, r.ye, r.et)
    pre_last_e()
    got("tok_last_c", c_f)
    turn(3, r.yc, r.ct)
    pre_last_c()

    def gradient(left, right, ks, core):
        rows_at = [left[pl.ds(pl.multiple_of(k * per_z, per_z), per_z)] for k in ks]
        both = jnp.concatenate(rows_at, axis=0)
        cols = right[:, core * ff : (core + 1) * ff]
        both = jnp.dot(both, cols, preferred_element_type=F32)
        return both[:per_z], both[per_z:]

    def farthest(j):
        return zi(4 + (1 - 2 * (j % 2)) * ((j + 1) // 2))

    @jax.named_scope("cross_grad")
    def cross_grad(left, right, out, into, order):
        copies = []
        for part in range(4):
            ks = order(2 * part), order(2 * part + 1)
            for k, total in zip(ks, gradient(left, right, ks, 1)):
                out[k] = total.astype(BF)
            copies.append(group())
            for k in ks:
                send(out.at[k], into.at[k], dev(dc=1), copies[-1])
        return copies

    @jax.named_scope("own_grad")
    def own_grad(left, right, other, out, order, part):
        ks = order(2 * part), order(2 * part + 1)
        for k, total in zip(ks, gradient(left, right, ks, 0)):
            out[k] = (total + other[k].astype(F32)).astype(BF)

    su, sd = r.su, r.sd

    def z_sum(name, acc, plus, minus, size):
        steps = {(s, first): group() for s in range(3) for first in (True, False)}
        steps[3, True] = steps[3, False] = end = group()

        def ways(s, first):
            for k, buf, step in ((zi(4 - s), plus, 1), (zi(s - 4), minus, -1)):
                yield k, buf, step, pl.ds(0 if first == (step == 1) else size, size)

        def start(s, first):
            for k, buf, step, part in ways(s, first):
                send(acc.at[k, part], buf.at[s, part], dev(dz=step), steps[s, first])

        def hop(s, first):
            got(f"{name}{s}", steps[s - 1, first])
            for k, buf, step, part in ways(s, first):
                total = acc[k, part].astype(F32) + buf[s - 1, part].astype(F32)
                acc[k, part] = total.astype(BF)
            start(s, first)

        def finish():
            got(f"{name}4", end)
            return acc[z].astype(F32) + plus[3].astype(F32) + minus[3].astype(F32)

        return start, hop, finish

    z_send, hop, z_end = z_sum("hop", sd, r.ra, r.rb, hz)
    uz_send, uz_hop, uz_end = z_sum("uz", r.tu, r.ua, r.ub, rows // 2)

    @jax.named_scope("back")
    def back(left, weight, out, part, begin=0, end=NZ // 2):
        @pl.loop(begin, end)
        def _(k):
            for core in range(2):
                w = weight[core, pl.ds(2 * k, 2)].reshape(2 * per_z, ff)
                acc = dot_tt(left[part, core * ff : (core + 1) * ff], w)
                total = acc if core == 0 else total + acc
            at = pl.ds(pl.multiple_of(k * 2 * per_z, per_z), 2 * per_z)
            out[part, at] = total.astype(BF)

    def start_sum(p, s):
        g = group()
        send(p.at[rows_of(3, 0)], s.at[0], dev(dy=1), g)
        send(p.at[rows_of(3, 1)], s.at[1], dev(dy=-1), g)
        return g

    def more_sum(p, m):
        g0, g1 = group(), group()
        send(p.at[rows_of(2, 1)], m.at[0, pl.ds(half, half)], dev(dy=1), g1)
        send(p.at[rows_of(1, 0)], m.at[1, pl.ds(0, half)], dev(dy=-1), g0)
        return g0, g1

    def pass_sum(p, s, m, g, groups):
        g0, g1 = groups
        got("sum_first", g)
        at = rows_of(2, 0)
        p[at] = (p[at].astype(F32) + s[0].astype(F32)).astype(BF)
        send(p.at[at], m.at[0, pl.ds(0, half)], dev(dy=1), g0)
        at = rows_of(1, 1)
        p[at] = (p[at].astype(F32) + s[1].astype(F32)).astype(BF)
        send(p.at[at], m.at[1, pl.ds(half, half)], dev(dy=-1), g1)

    def end_sum(p, m, groups, out):
        for h in range(2):
            got("sum_end", groups[h])
            own = rows_of(0, h)
            total = p[own].astype(F32) + m[0, own].astype(F32) + m[1, own].astype(F32)
            out[own] = total.astype(BF)

    pass_tokens(r.yl, l_a, tok_l)
    back(r.pg, wu, r.pe, last)
    first_e = start_sum(r.pe, r.se)
    c_down = cross_grad(r.ct, r.hid, r.god, r.xd, farthest)
    pairs = ((4, 0), (3, 5), (2, 6), (1, 7))
    c_up = cross_grad(r.et, r.pg, r.gou, r.xu, lambda j: zi(pairs[j // 2][j % 2]))
    for part in range(4):
        got("c_down", c_down[part])
        own_grad(r.ct, r.hid, r.xd, sd, farthest, part)
        if part == 0:
            z_send(0, True)
        if part == 1:
            z_send(1, False)

    x_first, x_last = [group() for _ in pairs], [group() for _ in pairs]

    def x_send(p):
        for i, step in ((0, 1), (1, -1)):
            k = zi(pairs[p][i])
            send(su.at[k, xs(2)], r.sx.at[p, i], dev(dx=step), x_first[p])

    def x_hop(p):
        got(f"x_hop{p}", x_first[p])
        for i, step in ((0, 1), (1, -1)):
            k = zi(pairs[p][i])
            total = su[k, xs(step)].astype(F32) + r.sx[p, i].astype(F32)
            su[k, xs(step)] = total.astype(BF)
            send(su.at[k, xs(step)], r.rx.at[i, 2 * p + i], dev(dx=step), x_last[p])
        for i, step in ((0, 1), (1, -1)):
            k = zi(pairs[p][1 - i])
            send(su.at[k, xs(step)], r.rx.at[i, 2 * p + 1 - i], dev(dx=step), x_last[p])

    def x_end(p):
        got(f"x_end{p}", x_last[p])
        for i in range(2):
            k, j = zi(pairs[p][i]), 2 * p + i
            total = su[k, xs(0)].astype(F32) + r.rx[0, j].astype(F32) + r.rx[1, j].astype(F32)
            r.tu[k] = total.astype(BF)

    for part in range(4):
        got("c_up", c_up[part])
        own_grad(r.et, r.pg, r.xu, su, lambda j: zi(pairs[j // 2][j % 2]), part)
        x_send(part)

    back(r.pg, wu, r.pe, many)
    more_e = more_sum(r.pe, r.re)
    hop(1, True)
    x_hop(0)
    hop(2, False)

    got("tok_l", tok_l)
    pre_later(0)
    x_hop(1)
    x_hop(2)
    x_hop(3)
    pass_sum(r.pe, r.se, r.re, first_e, more_e)
    pre_later(1)
    hop(2, True)
    back(r.hid, wd, r.po, pl.ds(0, 4 * tok))
    first_o = start_sum(r.po, r.so)
    more_o = more_sum(r.po, r.ro)
    x_end(0)
    uz_send(0, True)
    hop(3, False)
    x_end(1)
    uz_send(1, False)
    uz_hop(1, True)
    hop(3, True)
    x_end(2)
    uz_hop(2, False)
    x_end(3)
    uz_hop(2, True)
    uz_hop(3, False)

    down_sum = z_end()
    td = r.td
    td[...] = down_sum.astype(BF).reshape(NX, rows, ff)
    q0, q1 = pl.ds(0, rows // 2), pl.ds(rows // 2, rows // 2)
    dx1, dx2 = group(), group()
    send(td.at[xi(2), q0], r.xa.at[0, q0], dev(dx=1), dx1)
    send(td.at[xi(2), q1], r.xb.at[0, q1], dev(dx=-1), dx1)
    uz_hop(3, True)

    def add_on(acc, k, buf, s, part):
        acc[k, part] = (acc[k, part].astype(F32) + buf[s, part].astype(F32)).astype(BF)

    pass_sum(r.po, r.so, r.ro, first_o, more_o)
    got("dx1", dx1)
    add_on(td, xi(1), r.xa, 0, q0)
    send(td.at[xi(1)], r.xa.at[1], dev(dx=1), dx2)
    add_on(td, xi(-1), r.xb, 0, q1)
    send(td.at[xi(-1)], r.xb.at[1], dev(dx=-1), dx2)
    totals()
    o_up[...] = r.tot_u[...] + uz_end() * factor
    got("dx2", dx2)
    total = td[x].astype(F32) + r.xa[1].astype(F32) + r.xb[1].astype(F32)
    o_down[...] = r.tot_d[...] + total * factor
    end_sum(r.pe, r.re, more_e, o_earlier)
    settle()
    end_sum(r.po, r.ro, more_o, o_later)
    assert len(leaving) == N_SENT and len(arriving) == N_GOT, (len(leaving), len(arriving))


def body(later_rows, earlier_rows, cotangent, up_weight, down_weight, up_total, down_total):
    given = later_rows, earlier_rows, cotangent, up_weight, down_weight, up_total, down_total
    tok, d = later_rows.shape
    rows, ff = up_weight.shape
    total_rows = tok * lax.axis_size("fs") * lax.axis_size("tp")
    factor = 1.0 / math.sqrt(total_rows)
    scratch = scratch_of(tok, d, ff, rows)

    def run(*refs):
        kernel(list(scratch), factor, *refs)

    shapes = (
        jax.ShapeDtypeStruct((tok, d), BF),
        jax.ShapeDtypeStruct((tok, d), BF),
        jax.ShapeDtypeStruct((rows, ff), F32),
        jax.ShapeDtypeStruct((rows, ff), F32),
    )
    results = pl.pallas_call(
        run,
        out_shape=shapes,
        in_specs=[pl.BlockSpec(memory_space=pltpu.HBM)] * 7,
        out_specs=(pl.BlockSpec(memory_space=pltpu.VMEM),) * 4,
        scratch_shapes=list(scratch.values()),
        compiler_params=pltpu.CompilerParams(
            collective_id=0, has_side_effects=True, vmem_limit_bytes=50 * 2**20
        ),
        name="ffn_step",
    )(*(pltpu.with_memory_space_constraint(a, pltpu.HBM) for a in given))
    return pl.pallas_call(
        store,
        out_shape=shapes,
        in_specs=[pl.BlockSpec(memory_space=pltpu.VMEM)] * 4,
        out_specs=(pl.BlockSpec(memory_space=pl.ANY),) * 4,
        scratch_shapes=[pltpu.SemaphoreType.DMA((4,))],
        compiler_params=pltpu.CompilerParams(vmem_limit_bytes=4 * 2**20),
        name="ffn_store",
    )(*results)


def store(*refs):
    copies = [pltpu.make_async_copy(refs[i], refs[4 + i], refs[8].at[i]) for i in range(4)]
    for copy in copies:
        copy.start()
    for copy in copies:
        copy.wait()


def solution(mesh):
    tokens = P(("fs", "tp"), None)
    weight = P("fs", "tp")
    return jax.shard_map(
        body,
        mesh=mesh,
        in_specs=(tokens, tokens, tokens, weight, weight, weight, weight),
        out_specs=(tokens, tokens, weight, weight),
        check_vma=False,
    )
```

```python
import math
from types import SimpleNamespace

import jax
import jax.numpy as jnp
from jax import lax
from jax.experimental import pallas as pl
from jax.experimental.pallas import tpu as pltpu
from jax.sharding import PartitionSpec as P

NZ, NX, NY = 8, 4, 4
BF = jnp.bfloat16
F32 = jnp.float32
N_SENT = 4
N_GOT = 52


def scratch_of(tok, d, ff, rows):
    per_z = NX * rows
    vm = pltpu.VMEM
    return dict(
        tok=vm((12 * tok, d), BF),
        wu=vm((2, NZ, per_z, ff), BF),
        wd=vm((2, NZ, per_z, ff), BF),
        hid=vm((4 * tok, 2 * ff), BF),
        rel=vm((tok, 2 * ff), F32),
        pg=vm((4 * tok, 2 * ff), BF),
        pe=vm((4 * tok, d), BF),
        po=vm((4 * tok, d), BF),
        se=vm((2, tok // 2, d), BF),
        so=vm((2, tok // 2, d), BF),
        re=vm((2, tok, d), BF),
        ro=vm((2, tok, d), BF),
        gou=vm((NZ, per_z, ff), BF),
        god=vm((NZ, per_z, ff), BF),
        xu=vm((NZ, per_z, ff), BF),
        xd=vm((NZ, per_z, ff), BF),
        su=vm((NZ, per_z, ff), BF),
        sd=vm((NZ, per_z, ff), BF),
        sx=vm((NZ // 2, 2, rows, ff), BF),
        rx=vm((2, NZ, rows, ff), BF),
        tu=vm((NZ, rows, ff), BF),
        ua=vm((4, rows, ff), BF),
        ub=vm((4, rows, ff), BF),
        ra=vm((4, per_z, ff), BF),
        rb=vm((4, per_z, ff), BF),
        td=vm((NX, rows, ff), BF),
        xa=vm((2, rows, ff), BF),
        xb=vm((2, rows, ff), BF),
        et=vm((d, 4 * tok), BF),
        ct=vm((d, 4 * tok), BF),
        tot_u=vm((rows, ff), F32),
        tot_d=vm((rows, ff), F32),
        send=pltpu.SemaphoreType.DMA((N_SENT,)),
        recv=pltpu.SemaphoreType.DMA((N_GOT,)),
        told=pltpu.SemaphoreType.REGULAR,
        local=pltpu.SemaphoreType.DMA((4,)),
    )


def dot_tt(a, b):
    return lax.dot_general(a, b, (((1,), (1,)), ((), ())), preferred_element_type=F32)


def kernel(names, factor, *refs):
    later, earlier, cot, up, down, up_total, down_total = refs[:7]
    o_later, o_earlier, o_up, o_down = refs[7:11]
    r = SimpleNamespace(**dict(zip(names, refs[11:])))
    tok, d = later.shape
    rows, ff = up.shape
    r.ye, r.yc, r.yl = (r.tok.at[pl.ds(i * 4 * tok, 4 * tok)] for i in range(3))
    half = tok // 2
    per_z = NX * rows
    hz = per_z // 2

    f, t = lax.axis_index("fs"), lax.axis_index("tp")
    z, x = f // NX, f % NX
    y, c = t // 2, t % 2

    def zi(k):
        return (z + k + NZ) % NZ

    def xi(k):
        return (x + k + NX) % NX

    def dev(dz=0, dx=0, dy=0, dc=0):
        fs = zi(dz) * NX + xi(dx)
        tp = ((y + dy + NY) % NY) * 2 + (c + dc + 2) % 2
        return {"fs": fs, "tp": tp}

    row_bytes = d * 2
    limit = r.tok.shape[0] * row_bytes
    leaving, arriving, spent = [], [], []

    def group():
        if spent:
            return SimpleNamespace(at=spent.pop(), bytes=0)
        g = SimpleNamespace(at=len(arriving), bytes=0)
        arriving.append(g)
        return g

    def wait(sem, g):
        ref = r.tok.at[pl.ds(0, g.bytes // row_bytes)]
        pltpu.make_async_copy(ref, ref, sem).wait()

    def send(src, dst, to, g=None):
        size = math.prod(src.shape) * 2
        g = group() if g is None else g
        g.bytes += size
        if not leaving or leaving[-1].done or leaving[-1].bytes + size > limit:
            leaving.append(SimpleNamespace(bytes=0, done=False))
        leaving[-1].bytes += size
        pltpu.make_async_remote_copy(
            src_ref=src,
            dst_ref=dst,
            send_sem=r.send.at[len(leaving) - 1],
            recv_sem=r.recv.at[g.at],
            device_id=to,
            device_id_type=pl.DeviceIdType.MESH,
        ).start()
        return g

    @jax.named_scope("sent")
    def settle():
        for i, g in enumerate(leaving):
            if not g.done:
                wait(r.send.at[i], g)
                g.done = True

    done = []

    def got(name, *groups):
        with jax.named_scope(name):
            for g in {g.at: g for g in groups}.values():
                wait(r.recv.at[g.at], g)
                done.append(g.at)

    def fetch(i, *pairs):
        g = SimpleNamespace(bytes=0)
        for src, dst in pairs:
            pltpu.make_async_copy(src, dst, r.local.at[i]).start()
            g.bytes += math.prod(src.shape) * src.dtype.itemsize
        return lambda: wait(r.local.at[i], g)

    def xs(k):
        return pl.ds(pl.multiple_of(xi(k) * rows, rows), rows)

    barrier = pltpu.get_barrier_semaphore()

    def enter(**to):
        pl.semaphore_signal(
            barrier, inc=1, device_id=dev(**to), device_id_type=pl.DeviceIdType.MESH
        )

    def tell():
        pl.semaphore_signal(
            r.told, inc=1, device_id=dev(dc=1), device_id_type=pl.DeviceIdType.MESH
        )

    for step in (1, -1):
        enter(dy=step, dc=-c)
        enter(dx=step, dc=1 - c)
        enter(dz=step, dc=1 - c)
    enter(dc=1)

    first = fetch(0, (earlier, r.ye.at[pl.ds(0, tok)]))
    second = fetch(1, (cot, r.yc.at[pl.ds(0, tok)]))
    inputs = fetch(
        2,
        (up, r.wu.at[0, z, xs(0)]),
        (down, r.wd.at[0, z, xs(0)]),
        (later, r.yl.at[pl.ds(0, tok)]),
    )
    totals = fetch(3, (up_total, r.tot_u), (down_total, r.tot_d))

    with jax.named_scope("barrier"):

        @pl.when(c == 0)
        def _():
            pl.semaphore_wait(barrier, 5)
            tell()

        @pl.when(c == 1)
        def _():
            pl.semaphore_wait(r.told, 1)

    def enter_xz():
        with jax.named_scope("barrier_xz"):

            @pl.when(c == 1)
            def _():
                pl.semaphore_wait(barrier, 9)
                tell()

            @pl.when(c == 0)
            def _():
                pl.semaphore_wait(r.told, 1)

    def rows_of(slot, h):
        return pl.ds(slot * tok + h * half, half)

    def own_tokens(buf, h, g=None):
        g = g or group()
        send(buf.at[rows_of(0, h)], buf.at[rows_of(1, h)], dev(dy=1), g)
        send(buf.at[rows_of(0, 1 - h)], buf.at[rows_of(2, 1 - h)], dev(dy=-1), g)
        return g

    def pass_tokens(buf, first, g=None):
        g = g or group()
        got("tok_first", first)
        send(buf.at[rows_of(1, 0)], buf.at[rows_of(3, 0)], dev(dy=1), g)
        send(buf.at[rows_of(2, 1)], buf.at[rows_of(3, 1)], dev(dy=-1), g)
        return g

    wu, wd = r.wu, r.wd

    def up_block(dz, dx):
        return wu.at[0, zi(dz), xs(dx)]

    def up_z(k):
        g = group()
        for step in (1, -1):
            ref = up_block(-k * step, 0)
            if k == 3:
                ref = ref.at[pl.ds(0 if step == 1 else rows // 2, rows // 2)]
            send(ref, ref, dev(dz=step), g)
        return g

    up_first, up_rest, up_last = [group() for _ in range(4)], group(), group()

    def up_to_x(dz):
        ref = up_block(dz, 0)
        first = up_first[min(abs(dz), 3)]
        plus, minus = (first, up_rest) if 0 <= dz <= 3 else (up_rest, first)
        send(ref, ref, dev(dx=1), plus)
        send(ref, ref, dev(dx=-1), minus)

    def up_pass_x(*dzs):
        got("up_x", up_first[min(abs(dzs[0]), 3)])
        for dz in dzs:
            step = 1 if 0 <= dz <= 3 else -1
            ref = up_block(dz, -step)
            send(ref, ref, dev(dx=step), up_last)

    across = group()

    def up_column(dx):
        src = wu.at[0, :, xs(dx)]
        send(src, wu.at[1, :, xs(dx)], dev(dc=1), across)

    def down_block(dz, dx):
        return wd.at[0, zi(dz), xs(dx)]

    down_far = group()
    down_at = {}

    def down_z(k, *dxs):
        for dx in dxs:
            g = down_far if k == 3 else group()
            down_at[k + 1, dx] = g
            if k < 3 or dx in (0, -1):
                ref = down_block(-k, dx)
                send(ref, ref, dev(dz=1), g)
            if k < 3 or dx in (1, 2):
                ref = down_block(k, dx)
                send(ref, ref, dev(dz=-1), g)

    def down_pass(k, *dxs):
        for dx in dxs:
            got(f"down_z{k}", down_at[k, dx])
            down_z(k, dx)

    def down_chunk(*dzs):
        for dz in dzs:
            send(wd.at[0, zi(dz)], wd.at[1, zi(dz)], dev(dc=1), across)

    @jax.named_scope("turn")
    def turn(slot, src, dst):
        @pl.loop(0, NZ)
        def _(k):
            cols = pl.ds(pl.multiple_of(k * per_z, per_z), per_z)
            dst[cols, pl.ds(slot * tok, tok)] = src[pl.ds(slot * tok, tok), cols].T

    first()
    e_a = own_tokens(r.ye, 0)
    second()
    c_a = own_tokens(r.yc, 0)
    tok_own = own_tokens(r.ye, 1)
    own_tokens(r.yc, 1, tok_own)
    inputs()
    enter_xz()
    own_down = down_block(0, 0)
    down_x1, down_x2 = group(), group()
    send(own_down, own_down, dev(dx=1), down_x1)
    send(own_down, own_down, dev(dx=-1), down_x1)
    up_to_x(0)
    up_1 = up_z(0)
    down_z(0, 0)
    turn(0, r.ye, r.et)

    got("up_z1", up_1)
    up_2 = up_z(1)
    got("down_x", down_x1)
    part = down_block(0, -1).at[pl.ds(0, rows // 2)]
    send(part, part, dev(dx=1), down_x2)
    part = down_block(0, 1).at[pl.ds(rows // 2, rows // 2)]
    send(part, part, dev(dx=-1), down_x2)
    down_z(0, -1, 1)
    up_to_x(-1)
    up_to_x(1)
    down_pass(1, 0)
    turn(0, r.yc, r.ct)
    got("up_z2", up_2)
    up_3 = up_z(2)
    up_to_x(-2)
    up_to_x(2)
    got("down_x2", down_x2)
    down_z(0, 2)
    down_chunk(0)
    up_pass_x(0)
    down_pass(1, -1, 1)
    got("up_z3", up_3)
    up_4 = up_z(3)
    up_to_x(-3)
    up_to_x(3)
    down_pass(2, 0)
    up_pass_x(-1, 1)
    down_pass(1, 2)
    down_chunk(-1, 1)
    e_f = pass_tokens(r.ye, e_a)
    down_pass(2, -1, 1)
    got("up_z4", up_4)
    up_to_x(4)
    up_column(0)
    c_f = pass_tokens(r.yc, c_a)
    free = list(done)
    l_a = own_tokens(r.yl, 0)
    tok_l = own_tokens(r.yl, 1)
    up_pass_x(-2, 2)
    down_pass(3, 0)
    down_pass(2, 2)
    down_chunk(-2, 2)
    down_pass(3, -1, 1)
    up_pass_x(-3, 3, 4)
    got("up_x_rest", up_rest)
    up_column(-1)
    up_column(1)
    down_pass(3, 2)
    down_chunk(-3, 3)
    got("up_x_last", up_last)
    up_column(2)
    got("down_z4", down_far)
    down_chunk(4)
    got("tok_own", tok_own)
    for slot in (1, 2):
        turn(slot, r.ye, r.et)
        turn(slot, r.yc, r.ct)
    got("across", across)
    spent += free

    tile = 256
    many, last = pl.ds(0, 3 * tok), pl.ds(3 * tok, tok)

    @jax.named_scope("pre_earlier")
    def pre_earlier():
        for core in range(2):

            @pl.loop(0, ff // tile)
            def _(n):
                at = pl.multiple_of(n * tile, tile)
                w_up = wu[core, :, :, pl.ds(at, tile)].reshape(d, tile)
                w_down = wd[core, :, :, pl.ds(at, tile)].reshape(d, tile)
                relu = jnp.maximum(jnp.dot(r.ye[many], w_up, preferred_element_type=F32), 0.0)
                grad = jnp.dot(r.yc[many], w_down, preferred_element_type=F32)
                out = pl.ds(pl.multiple_of(core * ff + at, tile), tile)
                r.hid[many, out] = (relu * relu).astype(BF)
                r.pg[many, out] = (2.0 * relu * grad).astype(BF)

    @jax.named_scope("pre_last_e")
    def pre_last_e():
        for core in range(2):

            @pl.loop(0, ff // tile)
            def _(n):
                at = pl.multiple_of(n * tile, tile)
                w_up = wu[core, :, :, pl.ds(at, tile)].reshape(d, tile)
                relu = jnp.maximum(jnp.dot(r.ye[last], w_up, preferred_element_type=F32), 0.0)
                out = pl.ds(pl.multiple_of(core * ff + at, tile), tile)
                r.hid[last, out] = (relu * relu).astype(BF)
                r.rel[:, out] = relu

    @jax.named_scope("pre_last_c")
    def pre_last_c():
        for core in range(2):

            @pl.loop(0, ff // tile)
            def _(n):
                at = pl.multiple_of(n * tile, tile)
                w_down = wd[core, :, :, pl.ds(at, tile)].reshape(d, tile)
                grad = jnp.dot(r.yc[last], w_down, preferred_element_type=F32)
                out = pl.ds(pl.multiple_of(core * ff + at, tile), tile)
                r.pg[last, out] = (2.0 * r.rel[:, out] * grad).astype(BF)

    @jax.named_scope("pre_later")
    def pre_later(core):
        @pl.loop(0, ff // tile)
        def _(n):
            at = pl.multiple_of(n * tile, tile)
            w_up = wu[core, :, :, pl.ds(at, tile)].reshape(d, tile)
            relu = jnp.maximum(jnp.dot(r.yl[...], w_up, preferred_element_type=F32), 0.0)
            out = pl.ds(pl.multiple_of(core * ff + at, tile), tile)
            r.hid[:, out] = (relu * relu).astype(BF)

    pre_earlier()
    got("tok_last_e", e_f)
    turn(3, r.ye, r.et)
    pre_last_e()
    got("tok_last_c", c_f)
    turn(3, r.yc, r.ct)
    pre_last_c()

    def gradient(left, right, ks, core):
        rows_at = [left[pl.ds(pl.multiple_of(k * per_z, per_z), per_z)] for k in ks]
        both = jnp.concatenate(rows_at, axis=0)
        cols = right[:, core * ff : (core + 1) * ff]
        both = jnp.dot(both, cols, preferred_element_type=F32)
        return both[:per_z], both[per_z:]

    def farthest(j):
        return zi(4 + (1 - 2 * (j % 2)) * ((j + 1) // 2))

    @jax.named_scope("cross_grad")
    def cross_grad(left, right, out, into, order):
        copies = []
        for part in range(4):
            ks = order(2 * part), order(2 * part + 1)
            for k, total in zip(ks, gradient(left, right, ks, 1)):
                out[k] = total.astype(BF)
            copies.append(group())
            for k in ks:
                send(out.at[k], into.at[k], dev(dc=1), copies[-1])
        return copies

    @jax.named_scope("own_grad")
    def own_grad(left, right, other, out, order, part):
        ks = order(2 * part), order(2 * part + 1)
        for k, total in zip(ks, gradient(left, right, ks, 0)):
            out[k] = (total + other[k].astype(F32)).astype(BF)

    su, sd = r.su, r.sd

    def z_sum(name, acc, plus, minus, size):
        order = (0, True), (1, True), (1, False), (2, True), (2, False)
        steps = {key: group() for key in order}
        steps[3, True] = steps[3, False] = end = group()

        def ways(s, first):
            for k, buf, step in ((zi(4 - s), plus, 1), (zi(s - 4), minus, -1)):
                yield k, buf, step, pl.ds(0 if first == (step == 1) else size, size)

        def start(s, first):
            for k, buf, step, part in ways(s, first):
                send(acc.at[k, part], buf.at[s, part], dev(dz=step), steps[s, first])

        def hop(s, first):
            got(f"{name}{s}", steps[s - 1, first])
            for k, buf, step, part in ways(s, first):
                total = acc[k, part].astype(F32) + buf[s - 1, part].astype(F32)
                acc[k, part] = total.astype(BF)
            start(s, first)

        def finish():
            got(f"{name}4", end)
            return acc[z].astype(F32) + plus[3].astype(F32) + minus[3].astype(F32)

        return start, hop, finish

    z_send, hop, z_end = z_sum("hop", sd, r.ra, r.rb, hz)
    uz_send, uz_hop, uz_end = z_sum("uz", r.tu, r.ua, r.ub, rows // 2)

    @jax.named_scope("back")
    def back(left, weight, out, part, begin=0, end=NZ // 2):
        @pl.loop(begin, end)
        def _(k):
            for core in range(2):
                w = weight[core, pl.ds(2 * k, 2)].reshape(2 * per_z, ff)
                acc = dot_tt(left[part, core * ff : (core + 1) * ff], w)
                total = acc if core == 0 else total + acc
            at = pl.ds(pl.multiple_of(k * 2 * per_z, per_z), 2 * per_z)
            out[part, at] = total.astype(BF)

    def start_sum(p, s):
        g = group()
        send(p.at[rows_of(3, 0)], s.at[0], dev(dy=1), g)
        send(p.at[rows_of(3, 1)], s.at[1], dev(dy=-1), g)
        return g

    def more_sum(p, m):
        g0, g1 = group(), group()
        send(p.at[rows_of(2, 1)], m.at[0, pl.ds(half, half)], dev(dy=1), g1)
        send(p.at[rows_of(1, 0)], m.at[1, pl.ds(0, half)], dev(dy=-1), g0)
        return g0, g1

    def pass_sum(p, s, m, g, groups):
        g0, g1 = groups
        got("sum_first", g)
        at = rows_of(2, 0)
        p[at] = (p[at].astype(F32) + s[0].astype(F32)).astype(BF)
        send(p.at[at], m.at[0, pl.ds(0, half)], dev(dy=1), g0)
        at = rows_of(1, 1)
        p[at] = (p[at].astype(F32) + s[1].astype(F32)).astype(BF)
        send(p.at[at], m.at[1, pl.ds(half, half)], dev(dy=-1), g1)

    def end_sum(p, m, groups, out):
        for h in range(2):
            got("sum_end", groups[h])
            own = rows_of(0, h)
            total = p[own].astype(F32) + m[0, own].astype(F32) + m[1, own].astype(F32)
            out[own] = total.astype(BF)

    pass_tokens(r.yl, l_a, tok_l)
    back(r.pg, wu, r.pe, last)
    first_e = start_sum(r.pe, r.se)
    c_down = cross_grad(r.ct, r.hid, r.god, r.xd, farthest)
    pairs = ((4, 0), (3, 5), (2, 6), (1, 7))
    c_up = cross_grad(r.et, r.pg, r.gou, r.xu, lambda j: zi(pairs[j // 2][j % 2]))
    for part in range(4):
        got("c_down", c_down[part])
        own_grad(r.ct, r.hid, r.xd, sd, farthest, part)
        if part == 0:
            z_send(0, True)
        if part == 1:
            z_send(1, False)

    x_first, x_last = [group() for _ in pairs], [group() for _ in pairs]

    def x_send(p):
        for i, step in ((0, 1), (1, -1)):
            k = zi(pairs[p][i])
            send(su.at[k, xs(2)], r.sx.at[p, i], dev(dx=step), x_first[p])

    def x_hop(p):
        got(f"x_hop{p}", x_first[p])
        for i, step in ((0, 1), (1, -1)):
            k = zi(pairs[p][i])
            total = su[k, xs(step)].astype(F32) + r.sx[p, i].astype(F32)
            su[k, xs(step)] = total.astype(BF)
            send(su.at[k, xs(step)], r.rx.at[i, 2 * p + i], dev(dx=step), x_last[p])
        for i, step in ((0, 1), (1, -1)):
            k = zi(pairs[p][1 - i])
            send(su.at[k, xs(step)], r.rx.at[i, 2 * p + 1 - i], dev(dx=step), x_last[p])

    def x_end(p):
        got(f"x_end{p}", x_last[p])
        for i in range(2):
            k, j = zi(pairs[p][i]), 2 * p + i
            total = su[k, xs(0)].astype(F32) + r.rx[0, j].astype(F32) + r.rx[1, j].astype(F32)
            r.tu[k] = total.astype(BF)

    for part in range(4):
        got("c_up", c_up[part])
        own_grad(r.et, r.pg, r.xu, su, lambda j: zi(pairs[j // 2][j % 2]), part)
        x_send(part)

    back(r.pg, wu, r.pe, many)
    more_e = more_sum(r.pe, r.re)
    hop(1, True)
    x_hop(0)
    hop(2, False)

    got("tok_l", tok_l)
    pre_later(0)
    x_hop(1)
    x_hop(2)
    x_hop(3)
    pass_sum(r.pe, r.se, r.re, first_e, more_e)
    pre_later(1)
    hop(2, True)
    back(r.hid, wd, r.po, pl.ds(0, 4 * tok))
    first_o = start_sum(r.po, r.so)
    more_o = more_sum(r.po, r.ro)
    x_end(0)
    uz_send(0, True)
    hop(3, False)
    x_end(1)
    uz_send(1, False)
    uz_hop(1, True)
    hop(3, True)
    x_end(2)
    uz_hop(2, False)
    x_end(3)
    uz_hop(2, True)
    uz_hop(3, False)

    down_sum = z_end()
    td = r.td
    td[...] = down_sum.astype(BF).reshape(NX, rows, ff)
    q0, q1 = pl.ds(0, rows // 2), pl.ds(rows // 2, rows // 2)
    dx1, dx2 = group(), group()
    send(td.at[xi(2), q0], r.xa.at[0, q0], dev(dx=1), dx1)
    send(td.at[xi(2), q1], r.xb.at[0, q1], dev(dx=-1), dx1)
    uz_hop(3, True)

    def add_on(acc, k, buf, s, part):
        acc[k, part] = (acc[k, part].astype(F32) + buf[s, part].astype(F32)).astype(BF)

    pass_sum(r.po, r.so, r.ro, first_o, more_o)
    got("dx1", dx1)
    add_on(td, xi(1), r.xa, 0, q0)
    send(td.at[xi(1)], r.xa.at[1], dev(dx=1), dx2)
    add_on(td, xi(-1), r.xb, 0, q1)
    send(td.at[xi(-1)], r.xb.at[1], dev(dx=-1), dx2)
    totals()
    o_up[...] = r.tot_u[...] + uz_end() * factor
    got("dx2", dx2)
    total = td[x].astype(F32) + r.xa[1].astype(F32) + r.xb[1].astype(F32)
    o_down[...] = r.tot_d[...] + total * factor
    end_sum(r.pe, r.re, more_e, o_earlier)
    settle()
    end_sum(r.po, r.ro, more_o, o_later)
    assert len(leaving) == N_SENT and len(arriving) == N_GOT, (len(leaving), len(arriving))


def body(later_rows, earlier_rows, cotangent, up_weight, down_weight, up_total, down_total):
    given = later_rows, earlier_rows, cotangent, up_weight, down_weight, up_total, down_total
    tok, d = later_rows.shape
    rows, ff = up_weight.shape
    total_rows = tok * lax.axis_size("fs") * lax.axis_size("tp")
    factor = 1.0 / math.sqrt(total_rows)
    scratch = scratch_of(tok, d, ff, rows)

    def run(*refs):
        kernel(list(scratch), factor, *refs)

    shapes = (
        jax.ShapeDtypeStruct((tok, d), BF),
        jax.ShapeDtypeStruct((tok, d), BF),
        jax.ShapeDtypeStruct((rows, ff), F32),
        jax.ShapeDtypeStruct((rows, ff), F32),
    )
    results = pl.pallas_call(
        run,
        out_shape=shapes,
        in_specs=[pl.BlockSpec(memory_space=pltpu.HBM)] * 7,
        out_specs=(pl.BlockSpec(memory_space=pltpu.VMEM),) * 4,
        scratch_shapes=list(scratch.values()),
        compiler_params=pltpu.CompilerParams(
            collective_id=0, has_side_effects=True, vmem_limit_bytes=50 * 2**20
        ),
        name="ffn_step",
    )(*(pltpu.with_memory_space_constraint(a, pltpu.HBM) for a in given))
    return pl.pallas_call(
        store,
        out_shape=shapes,
        in_specs=[pl.BlockSpec(memory_space=pltpu.VMEM)] * 4,
        out_specs=(pl.BlockSpec(memory_space=pl.ANY),) * 4,
        scratch_shapes=[pltpu.SemaphoreType.DMA((4,))],
        compiler_params=pltpu.CompilerParams(vmem_limit_bytes=4 * 2**20),
        name="ffn_store",
    )(*results)


def store(*refs):
    copies = [pltpu.make_async_copy(refs[i], refs[4 + i], refs[8].at[i]) for i in range(4)]
    for copy in copies:
        copy.start()
    for copy in copies:
        copy.wait()


def solution(mesh):
    tokens = P(("fs", "tp"), None)
    weight = P("fs", "tp")
    return jax.shard_map(
        body,
        mesh=mesh,
        in_specs=(tokens, tokens, tokens, weight, weight, weight, weight),
        out_specs=(tokens, tokens, weight, weight),
        check_vma=False,
    )
```

```python
import math
from types import SimpleNamespace

import jax
import jax.numpy as jnp
from jax import lax
from jax.experimental import pallas as pl
from jax.experimental.pallas import tpu as pltpu
from jax.sharding import PartitionSpec as P

NZ, NX, NY = 8, 4, 4
BF = jnp.bfloat16
F32 = jnp.float32
N_SENT = 4
N_GOT = 52


def scratch_of(tok, d, ff, rows):
    per_z = NX * rows
    vm = pltpu.VMEM
    return dict(
        tok=vm((12 * tok, d), BF),
        wu=vm((2, NZ, per_z, ff), BF),
        wd=vm((2, NZ, per_z, ff), BF),
        hid=vm((4 * tok, 2 * ff), BF),
        rel=vm((tok, 2 * ff), F32),
        pg=vm((4 * tok, 2 * ff), BF),
        pe=vm((4 * tok, d), BF),
        po=vm((4 * tok, d), BF),
        se=vm((2, tok // 2, d), BF),
        so=vm((2, tok // 2, d), BF),
        re=vm((2, tok, d), BF),
        ro=vm((2, tok, d), BF),
        gou=vm((NZ, per_z, ff), BF),
        god=vm((NZ, per_z, ff), BF),
        xu=vm((NZ, per_z, ff), BF),
        xd=vm((NZ, per_z, ff), BF),
        su=vm((NZ, per_z, ff), BF),
        sd=vm((NZ, per_z, ff), BF),
        sx=vm((NZ // 2, 2, rows, ff), BF),
        rx=vm((2, NZ, rows, ff), BF),
        tu=vm((NZ, rows, ff), BF),
        ua=vm((4, rows, ff), BF),
        ub=vm((4, rows, ff), BF),
        ra=vm((4, per_z, ff), BF),
        rb=vm((4, per_z, ff), BF),
        td=vm((NX, rows, ff), BF),
        xa=vm((2, rows, ff), BF),
        xb=vm((2, rows, ff), BF),
        et=vm((d, 4 * tok), BF),
        ct=vm((d, 4 * tok), BF),
        tot_u=vm((rows, ff), F32),
        tot_d=vm((rows, ff), F32),
        send=pltpu.SemaphoreType.DMA((N_SENT,)),
        recv=pltpu.SemaphoreType.DMA((N_GOT,)),
        told=pltpu.SemaphoreType.REGULAR,
        local=pltpu.SemaphoreType.DMA((3,)),
    )


def dot_tt(a, b):
    return lax.dot_general(a, b, (((1,), (1,)), ((), ())), preferred_element_type=F32)


def kernel(names, factor, *refs):
    later, earlier, cot, up, down, up_total, down_total = refs[:7]
    o_later, o_earlier, o_up, o_down = refs[7:11]
    r = SimpleNamespace(**dict(zip(names, refs[11:])))
    tok, d = later.shape
    rows, ff = up.shape
    r.ye, r.yc, r.yl = (r.tok.at[pl.ds(i * 4 * tok, 4 * tok)] for i in range(3))
    half = tok // 2
    per_z = NX * rows
    hz = per_z // 2

    f, t = lax.axis_index("fs"), lax.axis_index("tp")
    z, x = f // NX, f % NX
    y, c = t // 2, t % 2

    def zi(k):
        return (z + k + NZ) % NZ

    def xi(k):
        return (x + k + NX) % NX

    def dev(dz=0, dx=0, dy=0, dc=0):
        fs = zi(dz) * NX + xi(dx)
        tp = ((y + dy + NY) % NY) * 2 + (c + dc + 2) % 2
        return {"fs": fs, "tp": tp}

    row_bytes = d * 2
    limit = r.tok.shape[0] * row_bytes
    leaving, arriving, spent = [], [], []

    def group():
        if spent:
            return SimpleNamespace(at=spent.pop(), bytes=0)
        g = SimpleNamespace(at=len(arriving), bytes=0)
        arriving.append(g)
        return g

    def wait(sem, g):
        ref = r.tok.at[pl.ds(0, g.bytes // row_bytes)]
        pltpu.make_async_copy(ref, ref, sem).wait()

    def send(src, dst, to, g=None):
        size = math.prod(src.shape) * 2
        g = group() if g is None else g
        g.bytes += size
        if not leaving or leaving[-1].done or leaving[-1].bytes + size > limit:
            leaving.append(SimpleNamespace(bytes=0, done=False))
        leaving[-1].bytes += size
        pltpu.make_async_remote_copy(
            src_ref=src,
            dst_ref=dst,
            send_sem=r.send.at[len(leaving) - 1],
            recv_sem=r.recv.at[g.at],
            device_id=to,
            device_id_type=pl.DeviceIdType.MESH,
        ).start()
        return g

    @jax.named_scope("sent")
    def settle():
        for i, g in enumerate(leaving):
            if not g.done:
                wait(r.send.at[i], g)
                g.done = True

    done = []

    def got(name, *groups):
        with jax.named_scope(name):
            for g in {g.at: g for g in groups}.values():
                wait(r.recv.at[g.at], g)
                done.append(g.at)

    def fetch(i, *pairs):
        g = SimpleNamespace(bytes=0)
        for src, dst in pairs:
            pltpu.make_async_copy(src, dst, r.local.at[i]).start()
            g.bytes += math.prod(src.shape) * src.dtype.itemsize
        return lambda: wait(r.local.at[i], g)

    def xs(k):
        return pl.ds(pl.multiple_of(xi(k) * rows, rows), rows)

    barrier = pltpu.get_barrier_semaphore()

    def enter(**to):
        pl.semaphore_signal(
            barrier, inc=1, device_id=dev(**to), device_id_type=pl.DeviceIdType.MESH
        )

    def tell():
        pl.semaphore_signal(
            r.told, inc=1, device_id=dev(dc=1), device_id_type=pl.DeviceIdType.MESH
        )

    for step in (1, -1):
        enter(dy=step, dc=-c)
        enter(dx=step, dc=1 - c)
        enter(dz=step, dc=1 - c)
    enter(dc=1)

    first = fetch(0, (earlier, r.ye.at[pl.ds(0, tok)]))
    inputs = fetch(
        1,
        (cot, r.yc.at[pl.ds(0, tok)]),
        (up, r.wu.at[0, z, xs(0)]),
        (down, r.wd.at[0, z, xs(0)]),
        (later, r.yl.at[pl.ds(0, tok)]),
    )
    totals = fetch(2, (up_total, r.tot_u), (down_total, r.tot_d))

    with jax.named_scope("barrier"):

        @pl.when(c == 0)
        def _():
            pl.semaphore_wait(barrier, 5)
            tell()

        @pl.when(c == 1)
        def _():
            pl.semaphore_wait(r.told, 1)

    def enter_xz():
        with jax.named_scope("barrier_xz"):

            @pl.when(c == 1)
            def _():
                pl.semaphore_wait(barrier, 9)
                tell()

            @pl.when(c == 0)
            def _():
                pl.semaphore_wait(r.told, 1)

    def rows_of(slot, h):
        return pl.ds(slot * tok + h * half, half)

    def own_tokens(buf, h, g=None):
        g = g or group()
        send(buf.at[rows_of(0, h)], buf.at[rows_of(1, h)], dev(dy=1), g)
        send(buf.at[rows_of(0, 1 - h)], buf.at[rows_of(2, 1 - h)], dev(dy=-1), g)
        return g

    def pass_tokens(buf, first, g=None):
        g = g or group()
        got("tok_first", first)
        send(buf.at[rows_of(1, 0)], buf.at[rows_of(3, 0)], dev(dy=1), g)
        send(buf.at[rows_of(2, 1)], buf.at[rows_of(3, 1)], dev(dy=-1), g)
        return g

    wu, wd = r.wu, r.wd

    def up_block(dz, dx):
        return wu.at[0, zi(dz), xs(dx)]

    def up_z(k):
        g = group()
        for step in (1, -1):
            ref = up_block(-k * step, 0)
            if k == 3:
                ref = ref.at[pl.ds(0 if step == 1 else rows // 2, rows // 2)]
            send(ref, ref, dev(dz=step), g)
        return g

    up_first, up_rest, up_last = [group() for _ in range(4)], group(), group()

    def up_to_x(dz):
        ref = up_block(dz, 0)
        first = up_first[min(abs(dz), 3)]
        plus, minus = (first, up_rest) if 0 <= dz <= 3 else (up_rest, first)
        send(ref, ref, dev(dx=1), plus)
        send(ref, ref, dev(dx=-1), minus)

    def up_pass_x(*dzs):
        got("up_x", up_first[min(abs(dzs[0]), 3)])
        for dz in dzs:
            step = 1 if 0 <= dz <= 3 else -1
            ref = up_block(dz, -step)
            send(ref, ref, dev(dx=step), up_last)

    across = group()

    def up_column(dx):
        src = wu.at[0, :, xs(dx)]
        send(src, wu.at[1, :, xs(dx)], dev(dc=1), across)

    def down_block(dz, dx):
        return wd.at[0, zi(dz), xs(dx)]

    down_far = group()
    down_at = {}

    def down_z(k, *dxs):
        for dx in dxs:
            g = down_far if k == 3 else group()
            down_at[k + 1, dx] = g
            if k < 3 or dx in (0, -1):
                ref = down_block(-k, dx)
                send(ref, ref, dev(dz=1), g)
            if k < 3 or dx in (1, 2):
                ref = down_block(k, dx)
                send(ref, ref, dev(dz=-1), g)

    def down_pass(k, *dxs):
        for dx in dxs:
            got(f"down_z{k}", down_at[k, dx])
            down_z(k, dx)

    def down_chunk(*dzs):
        for dz in dzs:
            send(wd.at[0, zi(dz)], wd.at[1, zi(dz)], dev(dc=1), across)

    @jax.named_scope("turn")
    def turn(slot, src, dst):
        @pl.loop(0, NZ)
        def _(k):
            cols = pl.ds(pl.multiple_of(k * per_z, per_z), per_z)
            dst[cols, pl.ds(slot * tok, tok)] = src[pl.ds(slot * tok, tok), cols].T

    first()
    e_a = own_tokens(r.ye, 0)
    inputs()
    c_a = own_tokens(r.yc, 0)
    tok_own = own_tokens(r.ye, 1)
    own_tokens(r.yc, 1, tok_own)
    enter_xz()
    own_down = down_block(0, 0)
    down_x1, down_x2 = group(), group()
    send(own_down, own_down, dev(dx=1), down_x1)
    send(own_down, own_down, dev(dx=-1), down_x1)
    up_to_x(0)
    up_1 = up_z(0)
    down_z(0, 0)
    turn(0, r.ye, r.et)

    got("up_z1", up_1)
    up_2 = up_z(1)
    got("down_x", down_x1)
    part = down_block(0, -1).at[pl.ds(0, rows // 2)]
    send(part, part, dev(dx=1), down_x2)
    part = down_block(0, 1).at[pl.ds(rows // 2, rows // 2)]
    send(part, part, dev(dx=-1), down_x2)
    down_z(0, -1, 1)
    up_to_x(-1)
    up_to_x(1)
    down_pass(1, 0)
    turn(0, r.yc, r.ct)
    got("up_z2", up_2)
    up_3 = up_z(2)
    up_to_x(-2)
    up_to_x(2)
    got("down_x2", down_x2)
    down_z(0, 2)
    down_chunk(0)
    up_pass_x(0)
    down_pass(1, -1, 1)
    got("up_z3", up_3)
    up_4 = up_z(3)
    up_to_x(-3)
    up_to_x(3)
    down_pass(2, 0)
    up_pass_x(-1, 1)
    down_pass(1, 2)
    down_chunk(-1, 1)
    e_f = pass_tokens(r.ye, e_a)
    down_pass(2, -1, 1)
    got("up_z4", up_4)
    up_to_x(4)
    up_column(0)
    c_f = pass_tokens(r.yc, c_a)
    free = list(done)
    l_a = own_tokens(r.yl, 0)
    tok_l = own_tokens(r.yl, 1)
    up_pass_x(-2, 2)
    down_pass(3, 0)
    down_pass(2, 2)
    down_chunk(-2, 2)
    down_pass(3, -1, 1)
    up_pass_x(-3, 3, 4)
    got("up_x_rest", up_rest)
    up_column(-1)
    up_column(1)
    down_pass(3, 2)
    down_chunk(-3, 3)
    got("up_x_last", up_last)
    up_column(2)
    got("down_z4", down_far)
    down_chunk(4)
    got("tok_own", tok_own)
    for slot in (1, 2):
        turn(slot, r.ye, r.et)
        turn(slot, r.yc, r.ct)
    got("across", across)
    spent += free

    tile = 256
    many, last = pl.ds(0, 3 * tok), pl.ds(3 * tok, tok)

    @jax.named_scope("pre_earlier")
    def pre_earlier():
        for core in range(2):

            @pl.loop(0, ff // tile)
            def _(n):
                at = pl.multiple_of(n * tile, tile)
                w_up = wu[core, :, :, pl.ds(at, tile)].reshape(d, tile)
                w_down = wd[core, :, :, pl.ds(at, tile)].reshape(d, tile)
                relu = jnp.maximum(jnp.dot(r.ye[many], w_up, preferred_element_type=F32), 0.0)
                grad = jnp.dot(r.yc[many], w_down, preferred_element_type=F32)
                out = pl.ds(pl.multiple_of(core * ff + at, tile), tile)
                r.hid[many, out] = (relu * relu).astype(BF)
                r.pg[many, out] = (2.0 * relu * grad).astype(BF)

    @jax.named_scope("pre_last_e")
    def pre_last_e():
        for core in range(2):

            @pl.loop(0, ff // tile)
            def _(n):
                at = pl.multiple_of(n * tile, tile)
                w_up = wu[core, :, :, pl.ds(at, tile)].reshape(d, tile)
                relu = jnp.maximum(jnp.dot(r.ye[last], w_up, preferred_element_type=F32), 0.0)
                out = pl.ds(pl.multiple_of(core * ff + at, tile), tile)
                r.hid[last, out] = (relu * relu).astype(BF)
                r.rel[:, out] = relu

    @jax.named_scope("pre_last_c")
    def pre_last_c():
        for core in range(2):

            @pl.loop(0, ff // tile)
            def _(n):
                at = pl.multiple_of(n * tile, tile)
                w_down = wd[core, :, :, pl.ds(at, tile)].reshape(d, tile)
                grad = jnp.dot(r.yc[last], w_down, preferred_element_type=F32)
                out = pl.ds(pl.multiple_of(core * ff + at, tile), tile)
                r.pg[last, out] = (2.0 * r.rel[:, out] * grad).astype(BF)

    @jax.named_scope("pre_later")
    def pre_later(core):
        @pl.loop(0, ff // tile)
        def _(n):
            at = pl.multiple_of(n * tile, tile)
            w_up = wu[core, :, :, pl.ds(at, tile)].reshape(d, tile)
            relu = jnp.maximum(jnp.dot(r.yl[...], w_up, preferred_element_type=F32), 0.0)
            out = pl.ds(pl.multiple_of(core * ff + at, tile), tile)
            r.hid[:, out] = (relu * relu).astype(BF)

    pre_earlier()
    got("tok_last_e", e_f)
    turn(3, r.ye, r.et)
    pre_last_e()
    got("tok_last_c", c_f)
    turn(3, r.yc, r.ct)
    pre_last_c()

    def gradient(left, right, ks, core):
        rows_at = [left[pl.ds(pl.multiple_of(k * per_z, per_z), per_z)] for k in ks]
        both = jnp.concatenate(rows_at, axis=0)
        cols = right[:, core * ff : (core + 1) * ff]
        both = jnp.dot(both, cols, preferred_element_type=F32)
        return both[:per_z], both[per_z:]

    def farthest(j):
        return zi(4 + (1 - 2 * (j % 2)) * ((j + 1) // 2))

    @jax.named_scope("cross_grad")
    def cross_grad(left, right, out, into, order):
        copies = []
        for part in range(4):
            ks = order(2 * part), order(2 * part + 1)
            for k, total in zip(ks, gradient(left, right, ks, 1)):
                out[k] = total.astype(BF)
            copies.append(group())
            for k in ks:
                send(out.at[k], into.at[k], dev(dc=1), copies[-1])
        return copies

    @jax.named_scope("own_grad")
    def own_grad(left, right, other, out, order, part):
        ks = order(2 * part), order(2 * part + 1)
        for k, total in zip(ks, gradient(left, right, ks, 0)):
            out[k] = (total + other[k].astype(F32)).astype(BF)

    su, sd = r.su, r.sd

    def z_sum(name, acc, plus, minus, size):
        order = (0, True), (1, True), (1, False), (2, True), (2, False)
        steps = {key: group() for key in order}
        steps[3, True] = steps[3, False] = end = group()

        def ways(s, first):
            for k, buf, step in ((zi(4 - s), plus, 1), (zi(s - 4), minus, -1)):
                yield k, buf, step, pl.ds(0 if first == (step == 1) else size, size)

        def start(s, first):
            for k, buf, step, part in ways(s, first):
                send(acc.at[k, part], buf.at[s, part], dev(dz=step), steps[s, first])

        def hop(s, first):
            got(f"{name}{s}", steps[s - 1, first])
            for k, buf, step, part in ways(s, first):
                total = acc[k, part].astype(F32) + buf[s - 1, part].astype(F32)
                acc[k, part] = total.astype(BF)
            start(s, first)

        def finish():
            got(f"{name}4", end)
            return acc[z].astype(F32) + plus[3].astype(F32) + minus[3].astype(F32)

        return start, hop, finish

    z_send, hop, z_end = z_sum("hop", sd, r.ra, r.rb, hz)
    uz_send, uz_hop, uz_end = z_sum("uz", r.tu, r.ua, r.ub, rows // 2)

    @jax.named_scope("back")
    def back(left, weight, out, part, begin=0, end=NZ // 2):
        @pl.loop(begin, end)
        def _(k):
            for core in range(2):
                w = weight[core, pl.ds(2 * k, 2)].reshape(2 * per_z, ff)
                acc = dot_tt(left[part, core * ff : (core + 1) * ff], w)
                total = acc if core == 0 else total + acc
            at = pl.ds(pl.multiple_of(k * 2 * per_z, per_z), 2 * per_z)
            out[part, at] = total.astype(BF)

    def start_sum(p, s):
        g = group()
        send(p.at[rows_of(3, 0)], s.at[0], dev(dy=1), g)
        send(p.at[rows_of(3, 1)], s.at[1], dev(dy=-1), g)
        return g

    def more_sum(p, m):
        g0, g1 = group(), group()
        send(p.at[rows_of(2, 1)], m.at[0, pl.ds(half, half)], dev(dy=1), g1)
        send(p.at[rows_of(1, 0)], m.at[1, pl.ds(0, half)], dev(dy=-1), g0)
        return g0, g1

    def pass_sum(p, s, m, g, groups):
        g0, g1 = groups
        got("sum_first", g)
        at = rows_of(2, 0)
        p[at] = (p[at].astype(F32) + s[0].astype(F32)).astype(BF)
        send(p.at[at], m.at[0, pl.ds(0, half)], dev(dy=1), g0)
        at = rows_of(1, 1)
        p[at] = (p[at].astype(F32) + s[1].astype(F32)).astype(BF)
        send(p.at[at], m.at[1, pl.ds(half, half)], dev(dy=-1), g1)

    def end_sum(p, m, groups, out):
        for h in range(2):
            got("sum_end", groups[h])
            own = rows_of(0, h)
            total = p[own].astype(F32) + m[0, own].astype(F32) + m[1, own].astype(F32)
            out[own] = total.astype(BF)

    pass_tokens(r.yl, l_a, tok_l)
    back(r.pg, wu, r.pe, last)
    first_e = start_sum(r.pe, r.se)
    c_down = cross_grad(r.ct, r.hid, r.god, r.xd, farthest)
    pairs = ((4, 0), (3, 5), (2, 6), (1, 7))
    c_up = cross_grad(r.et, r.pg, r.gou, r.xu, lambda j: zi(pairs[j // 2][j % 2]))
    for part in range(4):
        got("c_down", c_down[part])
        own_grad(r.ct, r.hid, r.xd, sd, farthest, part)
        if part == 0:
            z_send(0, True)
        if part == 1:
            z_send(1, False)

    x_first, x_last = [group() for _ in pairs], [group() for _ in pairs]

    def x_send(p):
        for i, step in ((0, 1), (1, -1)):
            k = zi(pairs[p][i])
            send(su.at[k, xs(2)], r.sx.at[p, i], dev(dx=step), x_first[p])

    def x_hop(p):
        got(f"x_hop{p}", x_first[p])
        for i, step in ((0, 1), (1, -1)):
            k = zi(pairs[p][i])
            total = su[k, xs(step)].astype(F32) + r.sx[p, i].astype(F32)
            su[k, xs(step)] = total.astype(BF)
            send(su.at[k, xs(step)], r.rx.at[i, 2 * p + i], dev(dx=step), x_last[p])
        for i, step in ((0, 1), (1, -1)):
            k = zi(pairs[p][1 - i])
            send(su.at[k, xs(step)], r.rx.at[i, 2 * p + 1 - i], dev(dx=step), x_last[p])

    def x_end(p):
        got(f"x_end{p}", x_last[p])
        for i in range(2):
            k, j = zi(pairs[p][i]), 2 * p + i
            total = su[k, xs(0)].astype(F32) + r.rx[0, j].astype(F32) + r.rx[1, j].astype(F32)
            r.tu[k] = total.astype(BF)

    for part in range(4):
        got("c_up", c_up[part])
        own_grad(r.et, r.pg, r.xu, su, lambda j: zi(pairs[j // 2][j % 2]), part)
        x_send(part)

    back(r.pg, wu, r.pe, many)
    more_e = more_sum(r.pe, r.re)
    hop(1, True)
    x_hop(0)
    hop(2, False)

    got("tok_l", tok_l)
    pre_later(0)
    x_hop(1)
    x_hop(2)
    x_hop(3)
    pass_sum(r.pe, r.se, r.re, first_e, more_e)
    pre_later(1)
    hop(2, True)
    back(r.hid, wd, r.po, pl.ds(0, 4 * tok))
    first_o = start_sum(r.po, r.so)
    more_o = more_sum(r.po, r.ro)
    x_end(0)
    uz_send(0, True)
    hop(3, False)
    x_end(1)
    uz_send(1, False)
    uz_hop(1, True)
    hop(3, True)
    x_end(2)
    uz_hop(2, False)
    x_end(3)
    uz_hop(2, True)
    uz_hop(3, False)

    down_sum = z_end()
    td = r.td
    td[...] = down_sum.astype(BF).reshape(NX, rows, ff)
    q0, q1 = pl.ds(0, rows // 2), pl.ds(rows // 2, rows // 2)
    dx1, dx2 = group(), group()
    send(td.at[xi(2), q0], r.xa.at[0, q0], dev(dx=1), dx1)
    send(td.at[xi(2), q1], r.xb.at[0, q1], dev(dx=-1), dx1)
    uz_hop(3, True)

    def add_on(acc, k, buf, s, part):
        acc[k, part] = (acc[k, part].astype(F32) + buf[s, part].astype(F32)).astype(BF)

    pass_sum(r.po, r.so, r.ro, first_o, more_o)
    got("dx1", dx1)
    add_on(td, xi(1), r.xa, 0, q0)
    send(td.at[xi(1)], r.xa.at[1], dev(dx=1), dx2)
    add_on(td, xi(-1), r.xb, 0, q1)
    send(td.at[xi(-1)], r.xb.at[1], dev(dx=-1), dx2)
    totals()
    o_up[...] = r.tot_u[...] + uz_end() * factor
    got("dx2", dx2)
    total = td[x].astype(F32) + r.xa[1].astype(F32) + r.xb[1].astype(F32)
    o_down[...] = r.tot_d[...] + total * factor
    end_sum(r.pe, r.re, more_e, o_earlier)
    settle()
    end_sum(r.po, r.ro, more_o, o_later)
    assert len(leaving) == N_SENT and len(arriving) == N_GOT, (len(leaving), len(arriving))


def body(later_rows, earlier_rows, cotangent, up_weight, down_weight, up_total, down_total):
    given = later_rows, earlier_rows, cotangent, up_weight, down_weight, up_total, down_total
    tok, d = later_rows.shape
    rows, ff = up_weight.shape
    total_rows = tok * lax.axis_size("fs") * lax.axis_size("tp")
    factor = 1.0 / math.sqrt(total_rows)
    scratch = scratch_of(tok, d, ff, rows)

    def run(*refs):
        kernel(list(scratch), factor, *refs)

    shapes = (
        jax.ShapeDtypeStruct((tok, d), BF),
        jax.ShapeDtypeStruct((tok, d), BF),
        jax.ShapeDtypeStruct((rows, ff), F32),
        jax.ShapeDtypeStruct((rows, ff), F32),
    )
    results = pl.pallas_call(
        run,
        out_shape=shapes,
        in_specs=[pl.BlockSpec(memory_space=pltpu.HBM)] * 7,
        out_specs=(pl.BlockSpec(memory_space=pltpu.VMEM),) * 4,
        scratch_shapes=list(scratch.values()),
        compiler_params=pltpu.CompilerParams(
            collective_id=0, has_side_effects=True, vmem_limit_bytes=50 * 2**20
        ),
        name="ffn_step",
    )(*(pltpu.with_memory_space_constraint(a, pltpu.HBM) for a in given))
    return pl.pallas_call(
        store,
        out_shape=shapes,
        in_specs=[pl.BlockSpec(memory_space=pltpu.VMEM)] * 4,
        out_specs=(pl.BlockSpec(memory_space=pl.ANY),) * 4,
        scratch_shapes=[pltpu.SemaphoreType.DMA((4,))],
        compiler_params=pltpu.CompilerParams(vmem_limit_bytes=4 * 2**20),
        name="ffn_store",
    )(*results)


def store(*refs):
    copies = [pltpu.make_async_copy(refs[i], refs[4 + i], refs[8].at[i]) for i in range(4)]
    for copy in copies:
        copy.start()
    for copy in copies:
        copy.wait()


def solution(mesh):
    tokens = P(("fs", "tp"), None)
    weight = P("fs", "tp")
    return jax.shard_map(
        body,
        mesh=mesh,
        in_specs=(tokens, tokens, tokens, weight, weight, weight, weight),
        out_specs=(tokens, tokens, weight, weight),
        check_vma=False,
    )
```
